512 devices in a mesh: sp: 64 (over z, y), tp: 8 (over x, core).
Axes of the slice: x: 4, y: 8, z: 8, core: 2. Of those that a mesh axis runs over, the one named last changes fastest.
Arguments:
- resid: bfloat16 [24576, 2048], P('sp'), may hold values from -6 to 6
- x_branch: bfloat16 [24576, 2048], P('sp', 'tp'), may hold values from -6 to 6
- gate_branch: bfloat16 [24576, 2048], P('sp', 'tp'), may hold values from -6 to 6
- conv_w: float32 [4, 2048], P(None, 'tp'), may hold values from -3 to 3
- gate_a_w: bfloat16 [32, 64, 64], P('tp'), may hold values from -0.75 to 0.75
- gate_x_w: bfloat16 [32, 64, 64], P('tp'), may hold values from -0.75 to 0.75
- decay_rate: float32 [2048], P('tp'), may hold values from 0 to 0.01, as said below
- decay_extra: float32 [24576, 2048], P('sp', 'tp'), may hold values from -3 to 0, as said below
- w_proj: bfloat16 [2048, 2048], P('tp'), may hold values from -0.125 to 0.125
- mix_gain: float32 [2048], replicated, may hold values from 0.1 to 1.9
- pre_gain: float32 [2048], replicated, may hold values from 0.1 to 1.9
- w_gate: bfloat16 [2048, 5632], P('sp', 'tp'), may hold values from -0.125 to 0.125
- w_up: bfloat16 [2048, 5632], P('sp', 'tp'), may hold values from -0.125 to 0.125
- w_down: bfloat16 [5632, 2048], P('tp', 'sp'), may hold values from -0.078125 to 0.078125
- out_gain: float32 [2048], replicated, may hold values from 0.1 to 1.9
Outputs:
- stream_out: bfloat16 [24576, 2048], P(('sp', 'tp'))
The draws below stay inside these ranges and needn't reach their ends.
Inputs may be any that keep to these rules, and one draw needn't show every extreme that they name: `decay_rate`: positive rates. `decay_extra`: non-positive values.
All inputs are finite; a program needn't handle non-finite values.
Results may differ from the reference program's by a relative error of at most 0.015.
Values may be sent and summed in bfloat16 or wider, within the bound.
A program may use at most 64 MiB of HBM per device.

```python
import math
import jax
import jax.numpy as jnp
from jax import lax

D = 2048
BLOCKS = 32
BW = 64
RECURRENCE_WIDTH = 2048
FF = 5632
CONV = 4
TOK_DEV = 384
TOKEN_SLOTS = 24576
N_TP = 8


def draw_decay_rate(key, part):
    key_pick, key_fast, key_slow = jax.random.split(key, 3)
    fast_share = 0.5
    is_fast = jax.random.uniform(key_pick, (RECURRENCE_WIDTH,), jnp.float32) < fast_share
    fast_rate = jnp.exp(jax.random.uniform(key_fast, (RECURRENCE_WIDTH,), jnp.float32, minval=math.log(1.0 / 240.0), maxval=math.log(1.0 / 120.0)))
    slow_rate = math.log(10.0) / (16.0 * TOKEN_SLOTS) * jax.random.uniform(key_slow, (RECURRENCE_WIDTH,), jnp.float32, minval=0.25, maxval=1.0)
    return jnp.where(is_fast, fast_rate, slow_rate).astype(jnp.float32)


def draw_decay_extra(key, part):
    key_level, key_location_draw, key_extent_draw = jax.random.split(key, 3)
    nblocks = TOKEN_SLOTS // TOK_DEV
    levels = jax.random.uniform(key_level, (nblocks, RECURRENCE_WIDTH), jnp.float32) * (-0.5 / TOKEN_SLOTS)
    drawn_regime = jnp.repeat(levels, TOK_DEV, axis=0)
    spike_token_rows = jax.random.randint(key_location_draw, (3,), 0, TOKEN_SLOTS)
    spike_extent = jax.random.uniform(key_extent_draw, (3, RECURRENCE_WIDTH), jnp.float32, minval=math.log(0.5), maxval=math.log(0.8))
    token_offsets = jnp.arange(TOKEN_SLOTS)
    inside_spike = (token_offsets[:, None] == spike_token_rows[None, :]).astype(jnp.float32)
    return (drawn_regime + jnp.dot(inside_spike, spike_extent)).astype(jnp.float32)


def block_scale(own_key, extent, cuts, least, largest):
    factor_of = 1.0
    for axis_at, parts in cuts:
        steps = jax.random.uniform(jax.random.fold_in(jax.random.fold_in(own_key, 6), axis_at), (parts,), jnp.float32, least / len(cuts), largest / len(cuts))
        factor_of = factor_of * jnp.repeat(jnp.exp(steps), extent[axis_at] // parts).reshape((-1,) + (1,) * (len(extent) - 1 - axis_at))
    return factor_of


def bell_draw(key, dims, width, reach, shards=(), held_as=jnp.bfloat16):
    array = width * jax.random.normal(key, dims, jnp.float32)
    if shards:
        array = array * block_scale(key, dims, shards, -0.22, 0.18)
    return jnp.clip(array, -reach, reach).astype(held_as)


def setup_inputs(seed: int = 0) -> dict:
    seeds = jax.random.split(jax.random.key(seed), 16)
    return {
        "resid": bell_draw(seeds[0], (TOKEN_SLOTS, D), 1.0, 6.0, ((0, 64),)),
        "x_branch": bell_draw(seeds[1], (TOKEN_SLOTS, RECURRENCE_WIDTH), 1.0, 6.0, ((0, 64), (1, 8))),
        "gate_branch": bell_draw(seeds[2], (TOKEN_SLOTS, RECURRENCE_WIDTH), 1.0, 6.0, ((0, 64), (1, 8))),
        "conv_w": bell_draw(seeds[3], (CONV, RECURRENCE_WIDTH), CONV ** -0.5, 3.0, ((1, 8),), jnp.float32),
        "gate_a_w": bell_draw(seeds[4], (BLOCKS, BW, BW), BW ** -0.5, 0.75, ((0, 8),)),
        "gate_x_w": bell_draw(seeds[5], (BLOCKS, BW, BW), BW ** -0.5, 0.75, ((0, 8),)),
        "decay_rate": draw_decay_rate(jax.random.fold_in(seeds[15], 71), 0),
        "decay_extra": draw_decay_extra(jax.random.fold_in(seeds[15], 71), 0),
        "w_proj": bell_draw(seeds[8], (RECURRENCE_WIDTH, D), RECURRENCE_WIDTH ** -0.5, 0.125, ((0, 8),)),
        "mix_gain": jnp.clip(1.0 + 0.18 * jax.random.normal(seeds[9], (D,), jnp.float32), 0.1, 1.9),
        "pre_gain": jnp.clip(1.0 + 0.18 * jax.random.normal(seeds[10], (D,), jnp.float32), 0.1, 1.9),
        "w_gate": bell_draw(seeds[11], (D, FF), D ** -0.5, 0.125, ((0, 64), (1, 8))),
        "w_up": bell_draw(seeds[12], (D, FF), D ** -0.5, 0.125, ((0, 64), (1, 8))),
        "w_down": bell_draw(seeds[13], (FF, D), FF ** -0.5, 0.078125, ((0, 8), (1, 64))),
        "out_gain": jnp.clip(1.0 + 0.18 * jax.random.normal(seeds[14], (D,), jnp.float32), 0.1, 1.9),
    }


LRU_SCALE = 8.0
NORM_EPS = 1e-06

def chain(earlier, later):
    return (earlier[0] * later[0], later[0] * earlier[1] + later[1])

def rms_scale(values, gains):
    return values * lax.rsqrt(lax.optimization_barrier(jnp.mean(values * values, axis=-1, keepdims=True)) + NORM_EPS) * gains

def reference(resid, x_branch, gate_branch, conv_w, gate_a_w, gate_x_w, decay_rate, decay_extra, w_proj, mix_gain, pre_gain, w_gate, w_up, w_down, out_gain):
    padded = jnp.pad(x_branch.astype(jnp.float32), ((CONV - 1, 0), (0, 0)))
    conv = padded[0:TOKEN_SLOTS] * conv_w[0]
    for tap in range(1, CONV):
        conv = conv + padded[tap:tap + TOKEN_SLOTS] * conv_w[tap]
    conv_out = conv.astype(jnp.bfloat16)
    grouped = conv_out.astype(jnp.float32).reshape(TOKEN_SLOTS, BLOCKS, BW)
    recur = jax.nn.sigmoid(jnp.einsum('rnc,ncd->rnd', grouped, gate_a_w.astype(jnp.float32)).reshape(TOKEN_SLOTS, RECURRENCE_WIDTH))
    inject = jax.nn.sigmoid(jnp.einsum('rnc,ncd->rnd', grouped, gate_x_w.astype(jnp.float32)).reshape(TOKEN_SLOTS, RECURRENCE_WIDTH))
    log_decay = -LRU_SCALE * recur * decay_rate + decay_extra
    decay = jnp.exp(log_decay)
    drive = jnp.sqrt(-jnp.expm1(2.0 * log_decay)) * inject * conv_out.astype(jnp.float32)
    _, state = lax.associative_scan(chain, (decay, drive), axis=0)
    mixer = (state * jax.nn.gelu(gate_branch.astype(jnp.float32))).astype(jnp.bfloat16)
    group_w = RECURRENCE_WIDTH // N_TP
    mixed = jnp.zeros((TOKEN_SLOTS, D), jnp.float32)
    for group in range(N_TP):
        partial_sum = jnp.dot(mixer[:, group * group_w:(group + 1) * group_w], w_proj[group * group_w:(group + 1) * group_w], preferred_element_type=jnp.float32)
        mixed = mixed + lax.optimization_barrier(partial_sum.astype(jnp.bfloat16)).astype(jnp.float32)
    stream = resid.astype(jnp.float32) + rms_scale(mixed, mix_gain)
    normed = rms_scale(stream, pre_gain).astype(jnp.bfloat16)
    group_f = FF // N_TP
    ffn = jnp.zeros((TOKEN_SLOTS, D), jnp.float32)
    for group in range(N_TP):
        gate = jnp.dot(normed, w_gate[:, group * group_f:(group + 1) * group_f], preferred_element_type=jnp.float32)
        upward = jnp.dot(normed, w_up[:, group * group_f:(group + 1) * group_f], preferred_element_type=jnp.float32)
        hidden = (jax.nn.silu(gate) * upward).astype(jnp.bfloat16)
        partial_sum = jnp.dot(hidden, w_down[group * group_f:(group + 1) * group_f], preferred_element_type=jnp.float32)
        ffn = ffn + lax.optimization_barrier(partial_sum.astype(jnp.bfloat16)).astype(jnp.float32)
    return (stream + 0.5 * rms_scale(ffn, out_gain)).astype(jnp.bfloat16)
```

```python
import functools

import jax
import jax.numpy as jnp
from jax import lax
from jax.experimental import pallas as pl
from jax.experimental.pallas import tpu as pltpu
from jax.sharding import PartitionSpec as P

LRU_SCALE = 8.0
NORM_EPS = 1e-06
MESH = pl.DeviceIdType.MESH
F32 = jnp.float32
BF16 = jnp.bfloat16

NF = 8
NX = 4
ROWS = 384
CH = 256
D = 2048
BLK = 48
HID = 704
GL = 1408
WL = 2176
S1A = 1152
NCOPY = 176


def dot(a, b):
    return jnp.dot(a, b, preferred_element_type=F32)


def dot_nt(a, b):
    return lax.dot_general(a, b, (((1,), (1,)), ((), ())), preferred_element_type=F32)


def sigmoid(v):
    return 1.0 / (1.0 + jnp.exp(-v))


def gelu(v):
    inner = 0.7978845608028654 * (v + 0.044715 * (v * v * v))
    return 0.5 * v * (1.0 + jnp.tanh(inner))


def one_minus_exp(w):
    series = 1.0 + w * (1.0 / 6.0)
    for n in (5.0, 4.0, 3.0, 2.0):
        series = 1.0 + w * (1.0 / n) * series
    return jnp.where(w > -0.25, -w * series, 1.0 - jnp.exp(w))


def rms_scale(values, gains):
    mean = jnp.sum(values * values, axis=-1, keepdims=True) * (1.0 / D)
    return values * lax.rsqrt(mean + NORM_EPS) * gains


def kernel(
    resid, x_in, g_in, conv_w, ga_in, gx_in, rate, extra, wp_in, mixg, preg, wg_in, wu_in, wd_in, outg,
    out,
    W, wp, xb, xp, gb, eb, cw, ga, gx, rt, mg, pg, og, wg, wu, wd, rs_b,
    halo, bd, cout, gates, acum, bcum, geb, tot, rowbuf, rtot, colbuf,
    mixa, mixs, mixb, parts, stream,
    sa, s1, s3, rl, rr, fl, fr, nb, hid,
    local_sem, send_sem, recv_sem,
):
    sp = lax.axis_index("sp")
    tp = lax.axis_index("tp")
    z, y = sp // NF, sp % NF
    x, c = tp // 2, tp % 2

    def at_zy(zz, yy):
        return {"sp": zz * NF + yy, "tp": tp}

    def at_x(step):
        return {"sp": sp, "tp": ((x + step) % NX) * 2 + c}

    partner = {"sp": sp, "tp": x * 2 + (1 - c)}
    behind = {"sp": (sp + NF * NF - 1) % (NF * NF), "tp": tp}
    ahead = {"sp": (sp + 1) % (NF * NF), "tp": tp}

    loads = {}

    def load(name, src, dst):
        copy = pltpu.make_async_copy(src, dst, local_sem.at[len(loads)])
        copy.start()
        loads[name] = copy

    load("wg", wg_in, wg)
    load("wu", wu_in, wu)
    load("wd", wd_in, wd)
    load("x", x_in, xb)
    load("ga", ga_in, ga)
    load("gx", gx_in, gx)
    load("g", g_in, gb)
    load("cw", conv_w, cw)
    load("rt", rate, rt)
    load("e", extra, eb)
    load("wp", wp_in, wp.at[0])
    load("rs", resid.at[pl.ds(pl.multiple_of(tp * BLK, 16), BLK), :], rs_b)
    load("mg", mixg, mg)
    load("pg", preg, pg)
    load("og", outg, og)

    barrier = pltpu.get_barrier_semaphore()
    peers = [at_zy(z, (y + k) % NF) for k in range(1, NF)]
    peers += [at_zy((z + k) % NF, y) for k in range(1, NF)]
    peers += [at_x(1), at_x(NX - 1), partner, behind, ahead]
    for peer in peers:
        pl.semaphore_signal(barrier, inc=1, device_id=peer, device_id_type=MESH)

    for name in ("wg", "wu", "wd"):
        loads[name].wait()
    eye = jnp.where(
        lax.broadcasted_iota(jnp.int32, (32, 32), 0) == lax.broadcasted_iota(jnp.int32, (32, 32), 1), 1.0, 0.0
    ).astype(BF16)
    wdt = dot_nt(eye, wd[...]).astype(BF16)
    for h in range(2):
        rows = slice(16 * h, 16 * h + 16)
        mine = W.at[c, z, y, h]
        for n in range(2):
            mine[:, 512 * n : 512 * n + 256] = wg[rows, 256 * n : 256 * n + 256]
            mine[:, 512 * n + 256 : 512 * n + 512] = wu[rows, 256 * n : 256 * n + 256]
        mine[:, 1024:1152] = wg[rows, 512:640]
        mine[:, 1152:1280] = wu[rows, 512:640]
        mine[:, 1280:1408] = jnp.concatenate([wg[rows, 640:704], wu[rows, 640:704]], axis=1)
        mine[:, 1408:2048] = wdt[rows, 0:640]
        mine[:, 2048:2176] = jnp.concatenate([wdt[rows, 640:704], jnp.zeros((16, 64), BF16)], axis=1)

    started = []

    def send(src, dst, device):
        index = len(started)
        copy = pltpu.make_async_remote_copy(
            src_ref=src,
            dst_ref=dst,
            send_sem=send_sem.at[index],
            recv_sem=recv_sem.at[index],
            device_id=device,
            device_id_type=MESH,
        )
        copy.start()
        started.append(copy)
        return copy

    def piece(h, first, second, lanes):
        if h == 0:
            return W.at[c, second, first, 0, :, lanes]
        return W.at[c, first, second, 1, :, lanes]

    def row_of(h, second, lanes, span=slice(0, NF)):
        if h == 0:
            return W.at[c, second, span, 0, :, lanes]
        return W.at[c, span, second, 1, :, lanes]

    first = (y, z)
    second = (z, y)

    def along_first(h, step):
        return at_zy(z, (y + step) % NF) if h == 0 else at_zy((z + step) % NF, y)

    def along_second(h, step):
        return along_first(1 - h, step)

    def mod(v):
        return (v + NF) % NF

    FULL, GLN, DLN = slice(0, WL), slice(0, GL), slice(GL, WL)
    HALVES = (slice(0, 4), slice(4, 8))
    s1c, s2g, s2d, d2d = {}, {}, {}, []

    def hop1(k):
        for h in range(2):
            for d, step in ((0, 1), (1, NF - 1)):
                src = mod(first[h] - (k - 1)) if d == 0 else mod(first[h] + (k - 1))
                lanes = FULL if k < 4 else (slice(0, S1A) if d == 0 else slice(S1A, WL))
                ref = piece(h, src, second[h], lanes)
                s1c[k, h, d] = send(ref, ref, along_first(h, step))

    def hop1_wait(k):
        for h in range(2):
            for d in range(2):
                s1c[k, h, d].wait_recv()

    def spread(js):
        for j in js:
            for h in range(2):
                off = (j + 1) // 2
                src = mod(first[h] - off) if j % 2 == 1 else mod(first[h] + off)
                ref = piece(h, src, second[h], GLN)
                for d, step in ((0, 1), (1, NF - 1)):
                    s2g[1, h, d, j] = send(ref, ref, along_second(h, step))

    def to_partner(h, row, lanes):
        ref = row_of(h, row, lanes)
        d2d.append((lanes, send(ref, ref, partner)))

    def src_row(h, d, t):
        return mod(second[h] - t) if d == 0 else mod(second[h] + t)

    def hop2(table, t, lanes, b):
        for h in range(2):
            for d, step in ((0, 1), (1, NF - 1)):
                if t == 4 and b != d:
                    continue
                ref = row_of(h, src_row(h, d, t - 1), lanes, HALVES[b])
                table[t, h, d, b] = send(ref, ref, along_second(h, step))

    def hop2_wait(table, t, bs):
        for b in bs:
            for h in range(2):
                for d in range(2):
                    if (t, h, d, b) in table:
                        table[t, h, d, b].wait_recv()

    def share(t, lanes):
        for h in range(2):
            for d in range(2 if t < 4 else 1):
                to_partner(h, src_row(h, d, t), lanes)

    loads["x"].wait()
    pl.semaphore_wait(barrier, len(peers))
    halo_copy = send(xb.at[pl.ds(ROWS - 16, 16), :], halo, ahead)
    hop1(1)
    spread([0])
    loads["wp"].wait()
    wp_copy = send(wp.at[0], wp.at[1], partner)

    for name in ("ga", "gx", "g", "cw", "rt", "e"):
        loads[name].wait()
    bd[...] = jnp.zeros_like(bd)
    for n in range(4):
        s = slice(64 * n, 64 * n + 64)
        bd[s, 64 * n : 64 * n + 64] = ga[n]
        bd[s, CH + 64 * n : CH + 64 * n + 64] = gx[n]
    xp[16:, :] = xb[...].astype(F32)
    geb[...] = gelu(gb[...].astype(F32))
    halo_copy.wait_recv()
    xp[0:16, :] = jnp.where(sp > 0, halo[...].astype(F32), 0.0)

    hop1_wait(1)
    hop1(2)
    spread([1, 2])

    conv = xp[13 : 13 + ROWS, :] * cw[0:1, :]
    for tap in range(1, 4):
        conv = conv + xp[13 + tap : 13 + tap + ROWS, :] * cw[tap : tap + 1, :]
    cout[...] = conv.astype(BF16)
    gates[...] = dot(cout[...], bd[...])

    in_group = lax.broadcasted_iota(jnp.int32, (4, 8, CH), 1)

    def chunk(i, carry):
        rows = pl.ds(pl.multiple_of(i * 32, 32), 32)
        recur = sigmoid(gates[rows, 0:CH])
        inject = sigmoid(gates[rows, CH:])
        log_decay = (-LRU_SCALE * recur) * rt[...] + eb[rows, :]
        decay = jnp.exp(log_decay)
        grown = one_minus_exp(2.0 * log_decay)
        root = jnp.where(grown > 0.0, grown * lax.rsqrt(jnp.maximum(grown, 1e-37)), 0.0)
        drive = root * inject * cout[rows, :].astype(F32)
        a = decay.reshape(4, 8, CH)
        b = drive.reshape(4, 8, CH)
        for step in (1, 2, 4):
            keep = in_group >= step
            a_prev = jnp.where(keep, pltpu.roll(a, step, 1), 1.0)
            b_prev = jnp.where(keep, pltpu.roll(b, step, 1), 0.0)
            b = a * b_prev + b
            a = a * a_prev
        a_in, b_in = carry
        a_all, b_all = [], []
        for n in range(4):
            a_n = a[n] * a_in
            b_n = a[n] * b_in + b[n]
            a_in, b_in = a_n[7:8, :], b_n[7:8, :]
            a_all.append(a_n)
            b_all.append(b_n)
        acum[rows, :] = jnp.concatenate(a_all, axis=0)
        bcum[rows, :] = jnp.concatenate(b_all, axis=0)
        return a_in, b_in

    a_end, b_end = lax.fori_loop(0, ROWS // 32, chunk, (jnp.ones((1, CH), F32), jnp.zeros((1, CH), F32)))
    tot[:, 0:CH] = a_end
    tot[:, CH:] = b_end

    row_copies = [send(tot, rowbuf.at[k - 1], at_zy(z, (y + k) % NF)) for k in range(1, NF)]
    hop1_wait(2)
    hop1(3)
    spread([3, 4])
    for copy in row_copies:
        copy.wait_recv()

    def composed(own, buf, me):
        pa, pb = jnp.ones((1, CH), F32), jnp.zeros((1, CH), F32)
        ea, eb_ = pa, pb
        for place in range(NF):
            slot = (me - place + NF) % NF
            got = buf[jnp.maximum(slot - 1, 0)]
            is_me = slot == 0
            va = jnp.where(is_me, own[:, 0:CH], got[:, 0:CH])
            vb = jnp.where(is_me, own[:, CH:], got[:, CH:])
            ea = jnp.where(is_me, pa, ea)
            eb_ = jnp.where(is_me, pb, eb_)
            pa, pb = pa * va, va * pb + vb
        return (pa, pb), (ea, eb_)

    (ra, rb_), (in_a, in_b) = composed(tot[...], rowbuf, y)
    rtot[:, 0:CH] = ra
    rtot[:, CH:] = rb_
    col_copies = [send(rtot, colbuf.at[k - 1], at_zy((z + k) % NF, y)) for k in range(1, NF)]
    hop1_wait(3)
    hop1(4)
    spread([5, 6])
    hop1_wait(4)
    spread([7])
    for h in range(2):
        to_partner(h, second[h], FULL)
    for copy in col_copies:
        copy.wait_recv()
    _, (col_a, col_b) = composed(rtot[...], colbuf, z)
    carried = in_a * col_b + in_b

    def mixer_block(core, rel):
        block = ((x + rel) % NX) * 2 + core
        rows = pl.ds(pl.multiple_of(block * BLK, 16), BLK)
        return ((bcum[rows, :] + acum[rows, :] * carried) * geb[rows, :]).astype(BF16)

    for rel in range(NX):
        mixs[BLK * rel : BLK * rel + BLK, :] = mixer_block(1 - c, rel)
    mix_copy = send(mixs, mixb, partner)
    for rel in range(NX):
        mixa[BLK * rel : BLK * rel + BLK, :] = mixer_block(c, rel)
    parts[...] = dot(mixa[...], wp[0])
    wp_copy.wait_recv()
    mix_copy.wait_recv()
    parts[...] += dot(mixb[...], wp[1])

    def scatter_start(u):
        for half in range(2):
            sa[u, half] = parts[2 * BLK : 3 * BLK, 1024 * half : 1024 * half + 1024].astype(BF16)
        relay_l = send(sa.at[u, 0], rl.at[u], at_x(1))
        relay_r = send(sa.at[u, 1], rr.at[u], at_x(NX - 1))
        s1[u, 1] = parts[BLK : 2 * BLK, 1024:].astype(BF16)
        far_l = send(s1.at[u, 1], fl.at[u, 1], at_x(1))
        s3[u, 0] = parts[3 * BLK :, 0:1024].astype(BF16)
        far_r = send(s3.at[u, 0], fr.at[u, 0], at_x(NX - 1))
        return relay_l, relay_r, far_l, far_r

    def scatter_relay(u, copies):
        relay_l, relay_r = copies[:2]
        relay_l.wait_recv()
        s1[u, 0] = (parts[BLK : 2 * BLK, 0:1024] + rl[u].astype(F32)).astype(BF16)
        near_l = send(s1.at[u, 0], fl.at[u, 0], at_x(1))
        relay_r.wait_recv()
        s3[u, 1] = (parts[3 * BLK :, 1024:] + rr[u].astype(F32)).astype(BF16)
        near_r = send(s3.at[u, 1], fr.at[u, 1], at_x(NX - 1))
        return copies[2:] + (near_l, near_r)

    def scatter_end(u, copies):
        for copy in copies:
            copy.wait_recv()
        halves = [
            parts[0:BLK, 1024 * half : 1024 * half + 1024] + fl[u, half].astype(F32) + fr[u, half].astype(F32)
            for half in range(2)
        ]
        return jnp.concatenate(halves, axis=1)

    copies = scatter_start(0)
    hop2_wait_list = [s2g[1, h, d, j] for j in range(NF) for h in range(2) for d in range(2)]
    for copy in hop2_wait_list:
        copy.wait_recv()
    hop2(s2g, 2, GLN, 0)
    copies = scatter_relay(0, copies)
    hop2(s2g, 2, GLN, 1)
    share(1, GLN)
    for name in ("rs", "mg", "pg", "og"):
        loads[name].wait()
    hop2_wait(s2g, 2, (0,))
    hop2(s2g, 3, GLN, 0)
    mixed = scatter_end(0, copies)
    after_mix = rs_b[...].astype(F32) + rms_scale(mixed, mg[...])
    stream[...] = after_mix
    normed = rms_scale(after_mix, pg[...]).astype(BF16)
    nb[0, 0] = normed[:, 0:1024]
    nb[1, 0] = normed[:, 1024:]

    left_a = send(nb.at[0, 0], nb.at[0, 3], at_x(1))
    right_a = send(nb.at[1, 0], nb.at[1, 1], at_x(NX - 1))
    left_b = send(nb.at[1, 0], nb.at[1, 3], at_x(1))
    right_b = send(nb.at[0, 0], nb.at[0, 1], at_x(NX - 1))
    hop2_wait(s2g, 2, (1,))
    hop2(s2g, 3, GLN, 1)
    share(2, GLN)
    left_a.wait_recv()
    left_c = send(nb.at[0, 3], nb.at[0, 2], at_x(1))
    right_a.wait_recv()
    right_c = send(nb.at[1, 1], nb.at[1, 2], at_x(NX - 1))
    hop2_wait(s2g, 3, (0, 1))
    hop2(s2g, 4, GLN, 0)
    hop2(s2g, 4, GLN, 1)
    share(3, GLN)
    for b in range(2):
        for h in range(2):
            for d, step in ((0, 1), (1, NF - 1)):
                ref = row_of(h, second[h], DLN, HALVES[b])
                s2d[1, h, d, b] = send(ref, ref, along_second(h, step))
    for copy in (left_b, right_b, left_c, right_c):
        copy.wait_recv()
    hop2_wait(s2g, 4, (0, 1))
    share(4, GLN)
    for lanes, copy in d2d:
        copy.wait_recv()
    n_shared = len(d2d)

    def gate_up(core, lanes):
        w = W[core, :, :, :, :, lanes]
        w = w.reshape(D, w.shape[-1])
        acc = dot(nb[0].reshape(NX * BLK, 1024), w[0:1024])
        return acc + dot(nb[1].reshape(NX * BLK, 1024), w[1024:])

    for core in range(2):
        for n in range(2):
            both = gate_up(core, slice(512 * n, 512 * n + 512))
            g, u = both[:, 0:256], both[:, 256:512]
            hid[core, :, 256 * n : 256 * n + 256] = (g * sigmoid(g) * u).astype(BF16)
        both = gate_up(core, slice(1024, 1408))
        g, u = both[:, 0:128], both[:, 128:256]
        hid[core, :, 512:640] = (g * sigmoid(g) * u).astype(BF16)
        last = both[:, 256:384]
        g, u = last, pltpu.roll(last, 64, 1)
        lane = lax.broadcasted_iota(jnp.int32, last.shape, 1)
        hid[core, :, 640:768] = jnp.where(lane < 64, g * sigmoid(g) * u, 0.0).astype(BF16)
        if core == 0:
            hop2_wait(s2d, 1, (0,))
            hop2(s2d, 2, DLN, 0)
            hop2_wait(s2d, 1, (1,))
            hop2(s2d, 2, DLN, 1)
            share(1, DLN)
    hop2_wait(s2d, 2, (0,))
    hop2(s2d, 3, DLN, 0)
    hop2_wait(s2d, 2, (1,))
    hop2(s2d, 3, DLN, 1)
    share(2, DLN)
    hop2_wait(s2d, 3, (0, 1))
    hop2(s2d, 4, DLN, 0)
    hop2(s2d, 4, DLN, 1)
    share(3, DLN)
    hop2_wait(s2d, 4, (0, 1))
    share(4, DLN)
    for lanes, copy in d2d[n_shared:]:
        copy.wait_recv()

    def down(n, _):
        acc = jnp.zeros((NX * BLK, 256), F32)
        for core in range(2):
            w = W[core, n, :, :, :, slice(GL, WL)]
            acc = acc + dot_nt(hid[core], w.reshape(256, WL - GL))
        parts[:, pl.ds(pl.multiple_of(n * 256, 256), 256)] = acc
        return 0

    lax.fori_loop(0, NF, down, 0)
    copies = scatter_start(1)
    copies = scatter_relay(1, copies)
    ffn = scatter_end(1, copies)
    out[...] = (stream[...] + 0.5 * rms_scale(ffn, og[...])).astype(BF16)
    for copy in started:
        copy.wait_send()


def shards(
    resid, x_branch, gate_branch, conv_w, gate_a_w, gate_x_w, decay_rate, decay_extra, w_proj, mix_gain,
    pre_gain, w_gate, w_up, w_down, out_gain,
):
    vmem = pltpu.VMEM
    half = (2, BLK, 1024)
    return pl.pallas_call(
        kernel,
        out_shape=jax.ShapeDtypeStruct((BLK, D), BF16),
        in_specs=[pl.BlockSpec(memory_space=pl.ANY)] * 15,
        out_specs=pl.BlockSpec(memory_space=pltpu.VMEM),
        scratch_shapes=[
            vmem((2, NF, NF, 2, 16, WL), BF16),
            vmem((2, CH, D), BF16),
            vmem((ROWS, CH), BF16),
            vmem((ROWS + 16, CH), F32),
            vmem((ROWS, CH), BF16),
            vmem((ROWS, CH), F32),
            vmem((4, CH), F32),
            vmem((4, 64, 64), BF16),
            vmem((4, 64, 64), BF16),
            vmem((1, CH), F32),
            vmem((1, D), F32),
            vmem((1, D), F32),
            vmem((1, D), F32),
            vmem((32, HID), BF16),
            vmem((32, HID), BF16),
            vmem((HID, 32), BF16),
            vmem((BLK, D), BF16),
            vmem((16, CH), BF16),
            vmem((CH, 2 * CH), BF16),
            vmem((ROWS, CH), BF16),
            vmem((ROWS, 2 * CH), F32),
            vmem((ROWS, CH), F32),
            vmem((ROWS, CH), F32),
            vmem((ROWS, CH), F32),
            vmem((1, 2 * CH), F32),
            vmem((NF - 1, 1, 2 * CH), F32),
            vmem((1, 2 * CH), F32),
            vmem((NF - 1, 1, 2 * CH), F32),
            vmem((NX * BLK, CH), BF16),
            vmem((NX * BLK, CH), BF16),
            vmem((NX * BLK, CH), BF16),
            vmem((NX * BLK, D), F32),
            vmem((BLK, D), F32),
            vmem((2,) + half, BF16),
            vmem((2,) + half, BF16),
            vmem((2,) + half, BF16),
            vmem(half, BF16),
            vmem(half, BF16),
            vmem((2,) + half, BF16),
            vmem((2,) + half, BF16),
            vmem((2, NX, BLK, 1024), BF16),
            vmem((2, NX * BLK, 768), BF16),
            pltpu.SemaphoreType.DMA((15,)),
            pltpu.SemaphoreType.DMA((NCOPY,)),
            pltpu.SemaphoreType.DMA((NCOPY,)),
        ],
        compiler_params=pltpu.CompilerParams(
            collective_id=0, has_side_effects=True, vmem_limit_bytes=58 * 1024 * 1024
        ),
        name="layer",
    )(
        resid, x_branch, gate_branch, conv_w, gate_a_w, gate_x_w, decay_rate.reshape(1, CH), decay_extra,
        w_proj, mix_gain.reshape(1, D), pre_gain.reshape(1, D), w_gate, w_up, w_down, out_gain.reshape(1, D),
    )


def solution(mesh):
    return jax.shard_map(
        shards,
        mesh=mesh,
        in_specs=(
            P("sp", None),
            P("sp", "tp"),
            P("sp", "tp"),
            P(None, "tp"),
            P("tp", None, None),
            P("tp", None, None),
            P("tp"),
            P("sp", "tp"),
            P("tp", None),
            P(),
            P(),
            P("sp", "tp"),
            P("sp", "tp"),
            P("tp", "sp"),
            P(),
        ),
        out_specs=P(("sp", "tp"), None),
        check_vma=False,
    )
```

```python
import functools

import jax
import jax.numpy as jnp
from jax import lax
from jax.experimental import pallas as pl
from jax.experimental.pallas import tpu as pltpu
from jax.sharding import PartitionSpec as P

LRU_SCALE = 8.0
NORM_EPS = 1e-06
MESH = pl.DeviceIdType.MESH
F32 = jnp.float32
BF16 = jnp.bfloat16

NF = 8
NX = 4
ROWS = 384
CH = 256
D = 2048
BLK = 48
HID = 704
WL = 2176
DA, GA, GB, DB = slice(0, 512), slice(512, 1152), slice(1152, 1920), slice(1920, 2176)
LA, LB, GU, ALL = slice(0, 1152), slice(1152, WL), slice(512, 1920), slice(0, WL)
LANES = {"DA": DA, "GA": GA, "GB": GB, "DB": DB}
GROUPS = ((0,), (1, 2), (3, 4), (5, 6), (7,))
NRECV = 110
NSEND = 22

ORDER = (
    ("DA", 0, 0), ("DB", 0, 0), ("scan", 0, 0), ("SB", 1, 0), ("SA", 1, 0), ("GA", 1, 0), ("GB", 1, 0),
    ("DA", 1, 0), ("DB", 1, 0), ("SB", 2, 0), ("GB", 1, 1), ("row", 0, 0), ("GA", 1, 1), ("SA", 2, 0),
    ("GA", 2, 0), ("DA", 2, 0), ("GB", 2, 0), ("DB", 2, 0), ("SB", 3, 0), ("GB", 1, 2), ("GA", 2, 1),
    ("col", 0, 0), ("mix", 0, 0), ("GB", 2, 1), ("GA", 1, 2), ("GA", 3, 0), ("SA", 3, 0), ("DA", 3, 0),
    ("mix2", 0, 0), ("GB", 3, 0), ("SB", 4, 0), ("DB", 3, 0), ("GA", 3, 1), ("GB", 1, 3), ("GA", 2, 2),
    ("relay", 0, 0), ("GA", 4, 0), ("GB", 2, 2), ("GA", 1, 3), ("DA", 4, 0), ("GB", 3, 1), ("GA", 4, 1),
    ("SA", 4, 0), ("send", 0, 0), ("GB", 4, 0), ("GA", 3, 2), ("GB", 1, 4), ("PGB", 1, 0), ("DB", 4, 0),
    ("DA", 0, 1), ("GA", 2, 3), ("GB", 2, 3), ("GA", 1, 4), ("PGA", 1, 0), ("GA", 4, 2), ("ag", 0, 0),
    ("GB", 3, 2), ("DA", 1, 1), ("GB", 4, 1), ("DA", 0, 2), ("GA", 3, 3), ("GB", 2, 4), ("PGB", 2, 0),
    ("GA", 2, 4), ("PGA", 2, 0), ("agend", 0, 0), ("DB", 0, 1), ("GB", 3, 3), ("DA", 2, 1), ("GB", 4, 2),
    ("DB", 0, 2), ("DA", 1, 2), ("DB", 0, 3), ("GB", 3, 4), ("PGB", 3, 0), ("GA", 4, 3), ("DB", 1, 1),
    ("GA", 3, 4), ("PGA", 3, 0), ("GB", 4, 3), ("DA", 0, 3), ("DB", 0, 4), ("DB", 1, 2), ("DA", 3, 1),
    ("DB", 1, 3), ("GB", 4, 4), ("PGB", 4, 0), ("DA", 0, 4), ("DA", 2, 2), ("GA", 4, 4), ("PGA", 4, 0),
    ("DB", 2, 1), ("DB", 1, 4), ("PDB", 1, 0), ("DB", 2, 2), ("DA", 1, 3), ("gw", 0, 0), ("gu0", 0, 0),
    ("DB", 2, 3), ("gu1", 0, 0), ("DA", 4, 1), ("gu2", 0, 0), ("DB", 3, 1), ("DA", 1, 4), ("PDA", 1, 0),
    ("DB", 2, 4), ("PDB", 2, 0), ("gu3", 0, 0), ("DB", 3, 2), ("gu4", 0, 0), ("DA", 3, 2), ("DB", 3, 3),
    ("gu5", 0, 0), ("DA", 2, 3), ("DB", 4, 1), ("DB", 3, 4), ("PDB", 3, 0), ("DA", 2, 4), ("PDA", 2, 0),
    ("DB", 4, 2), ("DB", 4, 3), ("DA", 4, 2), ("DB", 4, 4), ("PDB", 4, 0), ("DA", 3, 3), ("g0", 0, 0),
    ("DA", 3, 4), ("PDA", 3, 0), ("DA", 4, 3), ("g1", 0, 0), ("DA", 4, 4), ("PDA", 4, 0), ("g2", 0, 0),
    ("g0r", 0, 0),
)


def dot(a, b):
    return jnp.dot(a, b, preferred_element_type=F32)


def dot_nt(a, b):
    return lax.dot_general(a, b, (((1,), (1,)), ((), ())), preferred_element_type=F32)


def sigmoid(v):
    return 1.0 / (1.0 + jnp.exp(-v))


def gelu(v):
    inner = 0.7978845608028654 * (v + 0.044715 * (v * v * v))
    return 0.5 * v * (1.0 + jnp.tanh(inner))


def one_minus_exp(w):
    series = 1.0 + w * (1.0 / 6.0)
    for n in (5.0, 4.0, 3.0, 2.0):
        series = 1.0 + w * (1.0 / n) * series
    return jnp.where(w > -0.25, -w * series, 1.0 - jnp.exp(w))


def rms_scale(values, gains):
    mean = jnp.sum(values * values, axis=-1, keepdims=True) * (1.0 / D)
    return values * lax.rsqrt(mean + NORM_EPS) * gains


def kernel(
    resid, x_in, g_in, conv_w, ga_in, gx_in, rate, extra, wp_in, mixg, preg, wg_in, wu_in, wd_in, outg,
    out,
    W, wp, xb, xp, gb, eb, cw, ga, gx, rt, mg, pg, og, wg, wu, wd, rs_b,
    halo, bd, cout, gates, acum, bcum, geb, tot, rowbuf, rtot, colbuf,
    mixa, mixs, mixb, parts, stream, sb, rl, rr, fl, fr, nb, hid,
    parts2, sb0, rl0, rr0, fl0, fr0, sb1, rb1, sb2, rb2, ffn,
    local_sem, send_sem, recv_sem,
):
    sp = lax.axis_index("sp")
    tp = lax.axis_index("tp")
    z, y = sp // NF, sp % NF
    x, c = tp // 2, tp % 2

    def at_zy(zz, yy):
        return {"sp": zz * NF + yy, "tp": tp}

    def at_x(step):
        return {"sp": sp, "tp": ((x + step) % NX) * 2 + c}

    partner = {"sp": sp, "tp": x * 2 + (1 - c)}
    behind = {"sp": (sp + NF * NF - 1) % (NF * NF), "tp": tp}
    ahead = {"sp": (sp + 1) % (NF * NF), "tp": tp}

    loads = {}

    def load(name, src, dst):
        copy = pltpu.make_async_copy(src, dst, local_sem.at[len(loads)])
        copy.start()
        loads[name] = copy

    load("wg", wg_in, wg)
    load("wu", wu_in, wu)
    load("wd", wd_in, wd)
    load("x", x_in, xb)
    load("ga", ga_in, ga)
    load("gx", gx_in, gx)
    load("g", g_in, gb)
    load("cw", conv_w, cw)
    load("rt", rate, rt)
    load("e", extra, eb)
    load("wp", wp_in, wp.at[0])
    load("rs", resid.at[pl.ds(pl.multiple_of(tp * BLK, 16), BLK), :], rs_b)
    load("mg", mixg, mg)
    load("pg", preg, pg)
    load("og", outg, og)

    barrier = pltpu.get_barrier_semaphore()
    peers = [at_zy(z, (y + k) % NF) for k in range(1, NF)]
    peers += [at_zy((z + k) % NF, y) for k in range(1, NF)]
    peers += [at_x(1), at_x(2), at_x(NX - 1), partner, behind, ahead]
    for peer in peers:
        pl.semaphore_signal(barrier, inc=1, device_id=peer, device_id_type=MESH)

    for name in ("wg", "wu", "wd"):
        loads[name].wait()
    mine = W.at[c, z, y]
    mine[:, 0:512] = wd[:, 0:512]
    for n in range(2):
        mine[:, 512 * n + 512 : 512 * n + 768] = wg[:, 256 * n : 256 * n + 256]
        mine[:, 512 * n + 768 : 512 * n + 1024] = wu[:, 256 * n : 256 * n + 256]
    mine[:, 1536:1664] = wg[:, 512:640]
    mine[:, 1664:1792] = wu[:, 512:640]
    mine[:, 1792:1920] = jnp.concatenate([wg[:, 640:704], wu[:, 640:704]], axis=1)
    mine[:, 1920:2048] = wd[:, 512:640]
    mine[:, 2048:2176] = jnp.concatenate([wd[:, 640:704], jnp.zeros((32, 64), BF16)], axis=1)

    send_ids, recv_ids = {}, {}

    def send(src, dst, device, to, out):
        copy = pltpu.make_async_remote_copy(
            src_ref=src,
            dst_ref=dst,
            send_sem=send_sem.at[send_ids.setdefault(out, len(send_ids))],
            recv_sem=recv_sem.at[recv_ids.setdefault(to, len(recv_ids))],
            device_id=device,
            device_id_type=MESH,
        )
        copy.start()

    def arrived(to, like):
        pltpu.make_async_copy(like, like, recv_sem.at[recv_ids[to]]).wait()

    def sent(out, like):
        pltpu.make_async_copy(like, like, send_sem.at[send_ids[out]]).wait()

    def mod(v):
        return (v + NF) % NF

    def piece(fam, first, second, lanes):
        return W.at[c, second, first, :, lanes] if fam == "A" else W.at[c, first, second, :, lanes]

    def row_of(fam, second, lanes):
        return W.at[c, second, :, :, lanes] if fam == "A" else W.at[c, :, second, :, lanes]

    def some(n, lanes):
        return W.at[c, 0, 0:n, :, lanes]

    first = {"A": y, "B": z}
    second = {"A": z, "B": y}

    def along_y(step):
        return at_zy(z, (y + step) % NF)

    def along_z(step):
        return at_zy((z + step) % NF, y)

    along_first = {"A": along_y, "B": along_z}
    along_second = {"A": along_z, "B": along_y}
    WAYS = ((1, -1), (NF - 1, 1))

    def hop1(fam, k):
        whole = LA if fam == "A" else LB
        cut = whole.start + (640 if fam == "A" else 512)
        for d, (step, sign) in enumerate(WAYS):
            lanes = whole if k < 4 else (slice(whole.start, cut) if d == 0 else slice(cut, whole.stop))
            ref = piece(fam, mod(first[fam] + sign * (k - 1)), second[fam], lanes)
            send(ref, ref, along_first[fam](step), ("S" + fam, k), "S" + fam)

    def hop1_done(fam, k):
        whole = LA if fam == "A" else LB
        arrived(("S" + fam, k), some(2 if k < 4 else 1, whole))

    def offset(j):
        return (j + 1) // 2 * (-1 if j % 2 == 1 else 1)

    def hop2(name, t, q):
        fam, lanes = name[1], LANES[name]
        for d, (step, sign) in enumerate(WAYS):
            for j in GROUPS[q]:
                if t == 4 and (j < 4) != (d == 0):
                    continue
                ref = piece(fam, mod(first[fam] + offset(j)), mod(second[fam] + sign * (t - 1)), lanes)
                send(ref, ref, along_second[fam](step), (name, t, q), name)

    def hop2_done(name, t, q):
        n = len(GROUPS[q])
        arrived((name, t, q), some(2 * n if t < 4 else n, LANES[name]))

    def to_partner(name, t):
        fam = name[1]
        for sign in (-1, 1)[: 2 if t < 4 else 1]:
            ref = row_of(fam, mod(second[fam] + sign * t), LANES[name])
            to = "PG" if name[0] == "G" else ("PDB" if fam == "B" else ("PDA", max(t, 2)))
            send(ref, ref, partner, to, to)

    loads["x"].wait()
    pl.semaphore_wait(barrier, len(peers))
    hop1("A", 1)
    hop1("B", 1)
    send(xb.at[pl.ds(ROWS - 16, 16), :], halo, ahead, "halo", "halo")
    hop2("GA", 1, 0)
    hop2("GB", 1, 0)
    loads["wp"].wait()
    send(wp.at[0], wp.at[1], partner, "wp", "wp")
    for name in ("ga", "gx", "g", "cw", "rt", "e"):
        loads[name].wait()
    bd[...] = jnp.zeros_like(bd)
    for n in range(4):
        s = slice(64 * n, 64 * n + 64)
        bd[s, 64 * n : 64 * n + 64] = ga[n]
        bd[s, CH + 64 * n : CH + 64 * n + 64] = gx[n]
    xp[16:, :] = xb[...].astype(F32)
    geb[...] = gelu(gb[...].astype(F32))

    def scan():
        arrived("halo", halo)
        xp[0:16, :] = jnp.where(sp > 0, halo[...].astype(F32), 0.0)
        conv = xp[13 : 13 + ROWS, :] * cw[0:1, :]
        for tap in range(1, 4):
            conv = conv + xp[13 + tap : 13 + tap + ROWS, :] * cw[tap : tap + 1, :]
        cout[...] = conv.astype(BF16)
        gates[...] = dot(cout[...], bd[...])
        in_group = lax.broadcasted_iota(jnp.int32, (4, 8, CH), 1)

        def chunk(i, carry):
            rows = pl.ds(pl.multiple_of(i * 32, 32), 32)
            recur = sigmoid(gates[rows, 0:CH])
            inject = sigmoid(gates[rows, CH:])
            log_decay = (-LRU_SCALE * recur) * rt[...] + eb[rows, :]
            decay = jnp.exp(log_decay)
            grown = one_minus_exp(2.0 * log_decay)
            root = jnp.where(grown > 0.0, grown * lax.rsqrt(jnp.maximum(grown, 1e-37)), 0.0)
            drive = root * inject * cout[rows, :].astype(F32)
            a = decay.reshape(4, 8, CH)
            b = drive.reshape(4, 8, CH)
            for step in (1, 2, 4):
                keep = in_group >= step
                a_prev = jnp.where(keep, pltpu.roll(a, step, 1), 1.0)
                b_prev = jnp.where(keep, pltpu.roll(b, step, 1), 0.0)
                b = a * b_prev + b
                a = a * a_prev
            a_in, b_in = carry
            a_all, b_all = [], []
            for n in range(4):
                a_n = a[n] * a_in
                b_n = a[n] * b_in + b[n]
                a_in, b_in = a_n[7:8, :], b_n[7:8, :]
                a_all.append(a_n)
                b_all.append(b_n)
            acum[rows, :] = jnp.concatenate(a_all, axis=0)
            bcum[rows, :] = jnp.concatenate(b_all, axis=0)
            return a_in, b_in

        start = (jnp.ones((1, CH), F32), jnp.zeros((1, CH), F32))
        a_end, b_end = lax.fori_loop(0, ROWS // 32, chunk, start)
        tot[:, 0:CH] = a_end
        tot[:, CH:] = b_end
        for k in range(1, NF):
            send(tot, rowbuf.at[k - 1], along_y(k), "row", "row")

    def composed(own, buf, me):
        pa, pb = jnp.ones((1, CH), F32), jnp.zeros((1, CH), F32)
        ea, eb_ = pa, pb
        for place in range(NF):
            slot = (me - place + NF) % NF
            got = buf[jnp.maximum(slot - 1, 0)]
            is_me = slot == 0
            va = jnp.where(is_me, own[:, 0:CH], got[:, 0:CH])
            vb = jnp.where(is_me, own[:, CH:], got[:, CH:])
            ea = jnp.where(is_me, pa, ea)
            eb_ = jnp.where(is_me, pb, eb_)
            pa, pb = pa * va, va * pb + vb
        return (pa, pb), (ea, eb_)

    held = {}

    def row():
        arrived("row", rowbuf)
        (ra, rb_), held["in"] = composed(tot[...], rowbuf, y)
        rtot[:, 0:CH] = ra
        rtot[:, CH:] = rb_
        for k in range(1, NF):
            send(rtot, colbuf.at[k - 1], along_z(k), "col", "col")

    def col():
        arrived("col", colbuf)
        _, (col_a, col_b) = composed(rtot[...], colbuf, z)
        in_a, in_b = held["in"]
        held["carried"] = in_a * col_b + in_b

    def mixer_block(core, rel):
        block = ((x + rel) % NX) * 2 + core
        rows = pl.ds(pl.multiple_of(block * BLK, 16), BLK)
        return ((bcum[rows, :] + acum[rows, :] * held["carried"]) * geb[rows, :]).astype(BF16)

    def mix():
        for rel in range(NX):
            mixs[BLK * rel : BLK * rel + BLK, :] = mixer_block(1 - c, rel)
        send(mixs, mixb, partner, "mix", "mix")
        for rel in range(NX):
            mixa[BLK * rel : BLK * rel + BLK, :] = mixer_block(c, rel)
        arrived("wp", wp.at[1])
        parts[...] = dot(mixa[...], wp[0])

    def scatter_start(u, take, sbuf, bufs):
        rl_, rr_, fl_, fr_ = bufs
        for half in range(2):
            sbuf[half] = take(2, half).astype(BF16)
        send(sbuf.at[0], rl_, at_x(1), ("rl", u), ("sb", u))
        send(sbuf.at[1], rr_, at_x(NX - 1), ("rr", u), ("sb", u))
        sbuf[2] = take(1, 1).astype(BF16)
        send(sbuf.at[2], fl_.at[1], at_x(1), ("f", u), ("sb", u))
        sbuf[3] = take(3, 0).astype(BF16)
        send(sbuf.at[3], fr_.at[0], at_x(NX - 1), ("f", u), ("sb", u))

    def scatter_relay(u, take, sbuf, bufs):
        rl_, rr_, fl_, fr_ = bufs
        arrived(("rl", u), rl_)
        sbuf[4] = (take(1, 0) + rl_[...].astype(F32)).astype(BF16)
        send(sbuf.at[4], fl_.at[0], at_x(1), ("f", u), ("sb", u))
        arrived(("rr", u), rr_)
        sbuf[5] = (take(3, 1) + rr_[...].astype(F32)).astype(BF16)
        send(sbuf.at[5], fr_.at[1], at_x(NX - 1), ("f", u), ("sb", u))

    bufs = (rl, rr, fl, fr)

    def take(rel, half):
        return parts[BLK * rel : BLK * rel + BLK, 1024 * half : 1024 * half + 1024]

    def mix2():
        arrived("mix", mixb)
        parts[...] += dot(mixb[...], wp[1])
        scatter_start(0, take, sb, bufs)

    def relay():
        scatter_relay(0, take, sb, bufs)

    def norm_and_send():
        arrived(("f", 0), sb.at[0:4])
        for name in ("rs", "mg", "pg", "og"):
            loads[name].wait()
        halves = [take(0, half) + fl[half].astype(F32) + fr[half].astype(F32) for half in range(2)]
        mixed = jnp.concatenate(halves, axis=1)
        after_mix = rs_b[...].astype(F32) + rms_scale(mixed, mg[...])
        stream[...] = after_mix
        normed = rms_scale(after_mix, pg[...]).astype(BF16)
        nb[0, 0] = normed[:, 0:1024]
        nb[1, 0] = normed[:, 1024:]
        send(nb.at[0, 0], nb.at[0, 3], at_x(1), "al", "nb")
        send(nb.at[1, 0], nb.at[1, 1], at_x(NX - 1), "ar", "nb")
        send(nb.at[1, 0], nb.at[1, 3], at_x(1), "ab", "nb")
        send(nb.at[0, 0], nb.at[0, 1], at_x(NX - 1), "ab", "nb")

    def ag():
        arrived("al", nb.at[0, 3])
        send(nb.at[0, 3], nb.at[0, 2], at_x(1), "ab", "nb")
        arrived("ar", nb.at[1, 1])
        send(nb.at[1, 1], nb.at[1, 2], at_x(NX - 1), "ab", "nb")

    def agend():
        arrived("ab", nb.at[0])

    def gw():
        arrived("P0", W.at[c, 0, :, :, ALL])
        arrived("PG", W.at[c, 0:7, :, :, GU])

    def gate_up(core, lanes):
        w = W[core, :, :, :, lanes]
        w = w.reshape(D, w.shape[-1])
        acc = dot(nb[0].reshape(NX * BLK, 1024), w[0:1024])
        return acc + dot(nb[1].reshape(NX * BLK, 1024), w[1024:])

    def gu(i):
        core, n = i // 3, i % 3
        if n < 2:
            both = gate_up(core, slice(512 * n + 512, 512 * n + 1024))
            g, u = both[:, 0:256], both[:, 256:512]
            hid[core, :, 256 * n : 256 * n + 256] = (g * sigmoid(g) * u).astype(BF16)
        else:
            both = gate_up(core, slice(1536, 1920))
            g, u = both[:, 0:128], both[:, 128:256]
            hid[core, :, 512:640] = (g * sigmoid(g) * u).astype(BF16)
            g = both[:, 256:384]
            u = pltpu.roll(g, 64, 1)
            lane = lax.broadcasted_iota(jnp.int32, g.shape, 1)
            hid[core, :, 640:768] = jnp.where(lane < 64, g * sigmoid(g) * u, 0.0).astype(BF16)

    def place(i):
        return (z + NF + (i + 1) // 2 * (1 - 2 * (i % 2))) % NF

    def down(i, _):
        acc = jnp.zeros((NX * BLK, 256), F32)
        for core in range(2):
            wa = W[core, place(i), :, :, DA].reshape(256, 512)
            wb = W[core, place(i), :, :, DB].reshape(256, 256)
            acc = acc + dot_nt(hid[core, :, 0:512], wa) + dot_nt(hid[core, :, 512:768], wb)
        parts2[i] = acc
        return 0

    bufs0 = (rl0, rr0, fl0, fr0)

    def take0(rel, half):
        return parts2[0:5, BLK * rel : BLK * rel + BLK, 128 * half : 128 * half + 128]

    def g0():
        arrived("PDB", W.at[c, 0:7, :, :, DB])
        arrived(("PDA", 2), W.at[c, 0:4, :, :, DA])
        lax.fori_loop(0, 5, down, 0)
        scatter_start(1, take0, sb0, bufs0)

    def g0r():
        scatter_relay(1, take0, sb0, bufs0)

    def direct(u, lo, hi, sbuf, rbuf):
        for k, (rel, step) in enumerate(((2, 2), (1, 1), (3, NX - 1))):
            sbuf[k] = parts2[lo:hi, BLK * rel : BLK * rel + BLK, :].astype(BF16)
            send(sbuf.at[k], rbuf.at[k], at_x(step), ("d", u), ("d", u))

    def g1():
        arrived(("PDA", 3), W.at[c, 0:2, :, :, DA])
        lax.fori_loop(5, 7, down, 0)
        direct(1, 5, 7, sb1, rb1)

    def g2():
        arrived(("PDA", 4), W.at[c, 0, :, :, DA])
        down(7, 0)
        direct(2, 7, 8, sb2, rb2)

    steps = {
        "scan": scan, "row": row, "col": col, "mix": mix, "mix2": mix2, "relay": relay, "send": norm_and_send,
        "ag": ag, "agend": agend, "gw": gw, "g0": g0, "g0r": g0r, "g1": g1, "g2": g2,
    }
    for i in range(6):
        steps["gu%d" % i] = functools.partial(gu, i)

    for name, t, q in ORDER:
        if name in steps:
            steps[name]()
        elif name[0] == "S":
            fam = name[1]
            hop1_done(fam, t)
            if t < 4:
                hop1(fam, t + 1)
            else:
                ref = row_of(fam, second[fam], LA if fam == "A" else LB)
                send(ref, ref, partner, "P0", "P0")
            hop2("G" + fam, 1, t)
        elif name[0] == "P":
            to_partner(name[1:], t)
        else:
            if t > 0:
                hop2_done(name, t, q)
            if t < 4:
                hop2(name, t + 1, q)

    arrived(("f", 1), sb0.at[0:4])
    arrived(("d", 1), rb1)
    arrived(("d", 2), rb2)

    def put(i, lane, value):
        ffn[:, pl.ds(pl.multiple_of(place(i) * 256 + lane, 128), value.shape[-1])] = value

    for half in range(2):
        got = take0(0, half) + fl0[half].astype(F32) + fr0[half].astype(F32)
        for i in range(5):
            put(i, 128 * half, got[i])
    for lo, hi, rbuf in ((5, 7, rb1), (7, 8, rb2)):
        for i in range(lo, hi):
            put(i, 0, parts2[i, 0:BLK, :] + sum(rbuf[k, i - lo].astype(F32) for k in range(3)))
    out[...] = (stream[...] + 0.5 * rms_scale(ffn[...], og[...])).astype(BF16)

    for fam, lanes in (("A", LA), ("B", LB)):
        sent("S" + fam, W.at[c, 0, 0:7, :, lanes])
    for name in LANES:
        sent(name, W.at[c, 0:7, :, :, LANES[name]])
    sent("P0", W.at[c, 0, :, :, ALL])
    sent("PG", W.at[c, 0:7, :, :, GU])
    sent("PDB", W.at[c, 0:7, :, :, DB])
    for t, n in ((2, 4), (3, 2), (4, 1)):
        sent(("PDA", t), W.at[c, 0:n, :, :, DA])
    for out_, ref in (
        ("halo", halo), ("wp", wp.at[1]), ("row", rowbuf), ("col", colbuf), ("mix", mixb), (("sb", 0), sb),
        ("nb", sb), (("sb", 1), sb0), (("d", 1), sb1), (("d", 2), sb2),
    ):
        sent(out_, ref)
    assert len(recv_ids) <= NRECV and len(send_ids) <= NSEND, (len(recv_ids), len(send_ids))


def shards(
    resid, x_branch, gate_branch, conv_w, gate_a_w, gate_x_w, decay_rate, decay_extra, w_proj, mix_gain,
    pre_gain, w_gate, w_up, w_down, out_gain,
):
    vmem = pltpu.VMEM
    return pl.pallas_call(
        kernel,
        out_shape=jax.ShapeDtypeStruct((BLK, D), BF16),
        in_specs=[pl.BlockSpec(memory_space=pl.ANY)] * 15,
        out_specs=pl.BlockSpec(memory_space=pltpu.VMEM),
        scratch_shapes=[
            vmem((2, NF, NF, 32, WL), BF16),
            vmem((2, CH, D), BF16),
            vmem((ROWS, CH), BF16),
            vmem((ROWS + 16, CH), F32),
            vmem((ROWS, CH), BF16),
            vmem((ROWS, CH), F32),
            vmem((4, CH), F32),
            vmem((4, 64, 64), BF16),
            vmem((4, 64, 64), BF16),
            vmem((1, CH), F32),
            vmem((1, D), F32),
            vmem((1, D), F32),
            vmem((1, D), F32),
            vmem((32, HID), BF16),
            vmem((32, HID), BF16),
            vmem((32, HID), BF16),
            vmem((BLK, D), BF16),
            vmem((16, CH), BF16),
            vmem((CH, 2 * CH), BF16),
            vmem((ROWS, CH), BF16),
            vmem((ROWS, 2 * CH), F32),
            vmem((ROWS, CH), F32),
            vmem((ROWS, CH), F32),
            vmem((ROWS, CH), F32),
            vmem((1, 2 * CH), F32),
            vmem((NF - 1, 1, 2 * CH), F32),
            vmem((1, 2 * CH), F32),
            vmem((NF - 1, 1, 2 * CH), F32),
            vmem((NX * BLK, CH), BF16),
            vmem((NX * BLK, CH), BF16),
            vmem((NX * BLK, CH), BF16),
            vmem((NX * BLK, D), F32),
            vmem((BLK, D), F32),
            vmem((6, BLK, 1024), BF16),
            vmem((BLK, 1024), BF16),
            vmem((BLK, 1024), BF16),
            vmem((2, BLK, 1024), BF16),
            vmem((2, BLK, 1024), BF16),
            vmem((2, NX, BLK, 1024), BF16),
            vmem((2, NX * BLK, 768), BF16),
            vmem((NF, NX * BLK, 256), F32),
            vmem((6, 5, BLK, 128), BF16),
            vmem((5, BLK, 128), BF16),
            vmem((5, BLK, 128), BF16),
            vmem((2, 5, BLK, 128), BF16),
            vmem((2, 5, BLK, 128), BF16),
            vmem((3, 2, BLK, 256), BF16),
            vmem((3, 2, BLK, 256), BF16),
            vmem((3, 1, BLK, 256), BF16),
            vmem((3, 1, BLK, 256), BF16),
            vmem((BLK, D), F32),
            pltpu.SemaphoreType.DMA((15,)),
            pltpu.SemaphoreType.DMA((NSEND,)),
            pltpu.SemaphoreType.DMA((NRECV,)),
        ],
        compiler_params=pltpu.CompilerParams(
            collective_id=0, has_side_effects=True, vmem_limit_bytes=58 * 1024 * 1024
        ),
        name="layer",
    )(
        resid, x_branch, gate_branch, conv_w, gate_a_w, gate_x_w, decay_rate.reshape(1, CH), decay_extra,
        w_proj, mix_gain.reshape(1, D), pre_gain.reshape(1, D), w_gate, w_up, w_down.T, out_gain.reshape(1, D),
    )


def solution(mesh):
    return jax.shard_map(
        shards,
        mesh=mesh,
        in_specs=(
            P("sp", None),
            P("sp", "tp"),
            P("sp", "tp"),
            P(None, "tp"),
            P("tp", None, None),
            P("tp", None, None),
            P("tp"),
            P("sp", "tp"),
            P("tp", None),
            P(),
            P(),
            P("sp", "tp"),
            P("sp", "tp"),
            P("tp", "sp"),
            P(),
        ),
        out_specs=P(("sp", "tp"), None),
        check_vma=False,
    )
```

```python
import functools

import jax
import jax.numpy as jnp
from jax import lax
from jax.experimental import pallas as pl
from jax.experimental.pallas import tpu as pltpu
from jax.sharding import PartitionSpec as P

LRU_SCALE = 8.0
NORM_EPS = 1e-06
MESH = pl.DeviceIdType.MESH
F32 = jnp.float32
BF16 = jnp.bfloat16

NF = 8
NX = 4
ROWS = 384
CH = 256
D = 2048
BLK = 48
HID = 704
WL = 2176
LANES = {"DA": slice(0, 768), "GA": slice(768, 1152), "GB1": slice(1152, 1664), "GB2": slice(1664, 2176)}
LA, LB, ALL = slice(0, 1152), slice(1152, WL), slice(0, WL)
GROUPS = ((0,), (1, 2), (3, 4), (5, 6), (7,))
NRECV = 114
NSEND = 24

ORDER = (
    ("GB2", 0, 0), ("DA", 0, 0), ("scan1", 0, 0), ("SB", 1, 0), ("GB2", 0, 1), ("SA", 1, 0), ("scan2", 0, 0),
    ("GA", 1, 0), ("GB1", 1, 0), ("scan3", 0, 0), ("DA", 1, 0), ("GB2", 1, 0), ("SB", 2, 0), ("GB1", 1, 1),
    ("GA", 1, 1), ("GB2", 1, 1), ("GA", 2, 0), ("DA", 2, 0), ("SA", 2, 0), ("GB1", 2, 0), ("SB", 3, 0),
    ("GB2", 2, 0), ("GA", 2, 1), ("GA", 3, 0), ("QGA", 3, 0), ("GB1", 1, 2), ("DA", 3, 0), ("QDA", 3, 0),
    ("row", 0, 0), ("GB1", 2, 1), ("GA", 1, 2), ("SB", 4, 0), ("GB2", 2, 1), ("DA", 0, 1), ("GA", 3, 1),
    ("QGA", 3, 1), ("GA", 4, 0), ("QGA", 4, 0), ("DA", 4, 0), ("QDA", 4, 0), ("SA", 3, 0), ("GB1", 3, 0),
    ("QGB1", 3, 0), ("GA", 2, 2), ("GB1", 1, 3), ("GB2", 3, 0), ("QGB2", 3, 0), ("col", 0, 0), ("mix", 0, 0),
    ("DA", 0, 2), ("DA", 1, 1), ("GA", 4, 1), ("QGA", 4, 1), ("GB1", 2, 2), ("GA", 1, 3), ("mix2", 0, 0),
    ("GB1", 3, 1), ("QGB1", 3, 1), ("GA", 3, 2), ("QGA", 3, 2), ("GB1", 1, 4), ("PGB1", 1, 0), ("GB2", 3, 1),
    ("QGB2", 3, 1), ("DA", 1, 2), ("SA", 4, 0), ("GB1", 4, 0), ("QGB1", 4, 0), ("relay", 0, 0), ("DA", 2, 1),
    ("GB1", 2, 3), ("GB2", 4, 0), ("QGB2", 4, 0), ("GA", 2, 3), ("GA", 4, 2), ("QGA", 4, 2), ("GB2", 0, 2),
    ("GB1", 3, 2), ("QGB1", 3, 2), ("GB1", 4, 1), ("QGB1", 4, 1), ("GB1", 2, 4), ("PGB1", 2, 0), ("send", 0, 0),
    ("DA", 2, 2), ("GB2", 4, 1), ("QGB2", 4, 1), ("GA", 1, 4), ("PGA", 1, 0), ("GB2", 0, 3), ("GB1", 3, 3),
    ("QGB1", 3, 3), ("DA", 3, 1), ("QDA", 3, 1), ("GB2", 0, 4), ("GB2", 1, 2), ("GA", 3, 3), ("QGA", 3, 3),
    ("GB1", 4, 2), ("QGB1", 4, 2), ("ag", 0, 0), ("GB1", 3, 4), ("QGB1", 3, 4), ("DA", 0, 3), ("DA", 3, 2),
    ("QDA", 3, 2), ("GB2", 1, 3), ("GA", 2, 4), ("PGA", 2, 0), ("GB1", 4, 3), ("QGB1", 4, 3), ("DA", 4, 1),
    ("QDA", 4, 1), ("GB2", 1, 4), ("PGB2", 1, 0), ("GA", 4, 3), ("QGA", 4, 3), ("agend", 0, 0), ("GB2", 2, 2),
    ("DA", 0, 4), ("GB1", 4, 4), ("QGB1", 4, 4), ("DA", 1, 3), ("GB2", 2, 3), ("DA", 4, 2), ("QDA", 4, 2),
    ("GB2", 2, 4), ("PGB2", 2, 0), ("GA", 3, 4), ("QGA", 3, 4), ("u1c0", 0, 0), ("DA", 1, 4), ("PDA", 1, 0),
    ("GB2", 3, 2), ("QGB2", 3, 2), ("u1c1", 0, 0), ("GB2", 3, 3), ("QGB2", 3, 3), ("DA", 2, 3), ("GB2", 3, 4),
    ("QGB2", 3, 4), ("GA", 4, 4), ("QGA", 4, 4), ("GB2", 4, 2), ("QGB2", 4, 2), ("DA", 2, 4), ("PDA", 2, 0),
    ("GB2", 4, 3), ("QGB2", 4, 3), ("GB2", 4, 4), ("QGB2", 4, 4), ("u0c0", 0, 0), ("DA", 3, 3), ("QDA", 3, 3),
    ("u0c1", 0, 0), ("e0", 0, 0), ("DA", 3, 4), ("QDA", 3, 4), ("e1", 0, 0), ("e2", 0, 0), ("u2c0", 0, 0),
    ("e3", 0, 0), ("u2c1", 0, 0), ("DA", 4, 3), ("QDA", 4, 3), ("DA", 4, 4), ("QDA", 4, 4), ("e4", 0, 0),
    ("f0", 0, 0), ("e5", 0, 0), ("f1", 0, 0), ("e6", 0, 0), ("f2", 0, 0), ("f3", 0, 0), ("g0s", 0, 0),
    ("f4", 0, 0), ("f5", 0, 0), ("e7", 0, 0), ("f6", 0, 0), ("f7", 0, 0), ("g1s", 0, 0), ("g2s", 0, 0),
    ("g0r", 0, 0), ("g1r", 0, 0),
)


def dot(a, b):
    return jnp.dot(a, b, preferred_element_type=F32)


def dot_nt(a, b):
    return lax.dot_general(a, b, (((1,), (1,)), ((), ())), preferred_element_type=F32)


def sigmoid(v):
    return 1.0 / (1.0 + jnp.exp(-v))


def gelu(v):
    inner = 0.7978845608028654 * (v + 0.044715 * (v * v * v))
    return 0.5 * v * (1.0 + jnp.tanh(inner))


def one_minus_exp(w):
    series = 1.0 + w * (1.0 / 6.0)
    for n in (5.0, 4.0, 3.0, 2.0):
        series = 1.0 + w * (1.0 / n) * series
    return jnp.where(w > -0.25, -w * series, 1.0 - jnp.exp(w))


def rms_scale(values, gains):
    mean = jnp.sum(values * values, axis=-1, keepdims=True) * (1.0 / D)
    return values * lax.rsqrt(mean + NORM_EPS) * gains


def kernel(
    resid, x_in, g_in, conv_w, ga_in, gx_in, rate, extra, wp_in, mixg, preg, wg_in, wu_in, wd_in, outg,
    out,
    W, wp, xb, xp, gb, eb, cw, ga, gx, rt, mg, pg, og, wg, wu, wd, rs_b,
    halo, bd, cout, gates, acum, bcum, geb, tot, rowbuf, rtot, colbuf,
    mixa, mixs, mixb, parts, stream, sb, rl, rr, fl, fr, nb, hid,
    parts2, sb0, rl0, rr0, fl0, fr0, sb1, rl1, rr1, fl1, fr1, sb2, rb2, ffn,
    local_sem, send_sem, recv_sem,
):
    sp = lax.axis_index("sp")
    tp = lax.axis_index("tp")
    z, y = sp // NF, sp % NF
    x, c = tp // 2, tp % 2

    def at_zy(zz, yy):
        return {"sp": zz * NF + yy, "tp": tp}

    def at_x(step):
        return {"sp": sp, "tp": ((x + step) % NX) * 2 + c}

    partner = {"sp": sp, "tp": x * 2 + (1 - c)}
    behind = {"sp": (sp + NF * NF - 1) % (NF * NF), "tp": tp}
    ahead = {"sp": (sp + 1) % (NF * NF), "tp": tp}

    loads = {}

    def load(name, src, dst):
        copy = pltpu.make_async_copy(src, dst, local_sem.at[len(loads)])
        copy.start()
        loads[name] = copy

    load("wg", wg_in, wg)
    load("wu", wu_in, wu)
    load("wd", wd_in, wd)
    load("x", x_in, xb)
    load("ga", ga_in, ga)
    load("gx", gx_in, gx)
    load("g", g_in, gb)
    load("cw", conv_w, cw)
    load("rt", rate, rt)
    load("e", extra, eb)
    load("wp", wp_in, wp.at[0])
    load("rs", resid.at[pl.ds(pl.multiple_of(tp * BLK, 16), BLK), :], rs_b)
    load("mg", mixg, mg)
    load("pg", preg, pg)
    load("og", outg, og)

    barrier = pltpu.get_barrier_semaphore()
    peers = [at_zy(z, (y + k) % NF) for k in range(1, NF)]
    peers += [at_zy((z + k) % NF, y) for k in range(1, NF)]
    peers += [at_x(1), at_x(2), at_x(NX - 1), partner, behind, ahead]
    for peer in peers:
        pl.semaphore_signal(barrier, inc=1, device_id=peer, device_id_type=MESH)

    for name in ("wg", "wu", "wd"):
        loads[name].wait()
    mine = W.at[c, z, y]
    mine[:, 0:640] = wd[:, 0:640]
    mine[:, 640:768] = jnp.concatenate([wd[:, 640:704], jnp.zeros((32, 64), BF16)], axis=1)
    mine[:, 768:896] = wg[:, 512:640]
    mine[:, 896:1024] = wu[:, 512:640]
    mine[:, 1024:1152] = jnp.concatenate([wg[:, 640:704], wu[:, 640:704]], axis=1)
    for n in range(2):
        mine[:, 512 * n + 1152 : 512 * n + 1408] = wg[:, 256 * n : 256 * n + 256]
        mine[:, 512 * n + 1408 : 512 * n + 1664] = wu[:, 256 * n : 256 * n + 256]

    send_ids, recv_ids = {}, {}

    def send(src, dst, device, to, out):
        copy = pltpu.make_async_remote_copy(
            src_ref=src,
            dst_ref=dst,
            send_sem=send_sem.at[send_ids.setdefault(out, len(send_ids))],
            recv_sem=recv_sem.at[recv_ids.setdefault(to, len(recv_ids))],
            device_id=device,
            device_id_type=MESH,
        )
        copy.start()

    def arrived(to, like):
        pltpu.make_async_copy(like, like, recv_sem.at[recv_ids[to]]).wait()

    def sent(out, like):
        pltpu.make_async_copy(like, like, send_sem.at[send_ids[out]]).wait()

    def mod(v):
        return (v + NF) % NF

    def piece(fam, first, second, lanes):
        return W.at[c, second, first, :, lanes] if fam == "A" else W.at[c, first, second, :, lanes]

    def row_of(fam, second, lanes):
        return W.at[c, second, :, :, lanes] if fam == "A" else W.at[c, :, second, :, lanes]

    def some(n, lanes):
        return W.at[c, 0, 0:n, :, lanes]

    first = {"A": y, "B": z}
    second = {"A": z, "B": y}

    def along_y(step):
        return at_zy(z, (y + step) % NF)

    def along_z(step):
        return at_zy((z + step) % NF, y)

    along_first = {"A": along_y, "B": along_z}
    along_second = {"A": along_z, "B": along_y}
    WAYS = ((1, -1), (NF - 1, 1))

    def hop1(fam, k):
        whole = LA if fam == "A" else LB
        cut = whole.start + (640 if fam == "A" else 512)
        for d, (step, sign) in enumerate(WAYS):
            lanes = whole if k < 4 else (slice(whole.start, cut) if d == 0 else slice(cut, whole.stop))
            ref = piece(fam, mod(first[fam] + sign * (k - 1)), second[fam], lanes)
            send(ref, ref, along_first[fam](step), ("S" + fam, k), "S" + fam)

    def hop1_done(fam, k):
        whole = LA if fam == "A" else LB
        arrived(("S" + fam, k), some(2 if k < 4 else 1, whole))

    def offset(j):
        return (j + 1) // 2 * (-1 if j % 2 == 1 else 1)

    def hop2(name, t, q):
        fam, lanes = name[1], LANES[name]
        for d, (step, sign) in enumerate(WAYS):
            for j in GROUPS[q]:
                if t == 4 and (j < 4) != (d == 0):
                    continue
                ref = piece(fam, mod(first[fam] + offset(j)), mod(second[fam] + sign * (t - 1)), lanes)
                send(ref, ref, along_second[fam](step), (name, t, q), name)

    def hop2_done(name, t, q):
        n = len(GROUPS[q])
        arrived((name, t, q), some(2 * n if t < 4 else n, LANES[name]))

    def partner_ids(name, t):
        to = ("PDA", t) if name == "DA" else "P" + name
        return to, to

    def to_partner(name, t):
        fam = name[1]
        for sign in (-1, 1)[: 2 if t < 4 else 1]:
            ref = row_of(fam, mod(second[fam] + sign * t), LANES[name])
            send(ref, ref, partner, *partner_ids(name, t))

    def group_to_partner(name, t, q):
        fam = name[1]
        for sign in (-1, 1)[: 2 if t < 4 else 1]:
            for j in GROUPS[q]:
                ref = piece(fam, mod(first[fam] + offset(j)), mod(second[fam] + sign * t), LANES[name])
                send(ref, ref, partner, *partner_ids(name, t))

    loads["x"].wait()
    pl.semaphore_wait(barrier, len(peers))
    send(xb.at[pl.ds(ROWS - 16, 16), :], halo, ahead, "halo", "halo")
    hop1("A", 1)
    hop1("B", 1)
    hop2("GA", 1, 0)
    hop2("GB1", 1, 0)
    loads["wp"].wait()
    send(wp.at[0], wp.at[1], partner, "wp", "wp")
    for name in ("ga", "gx", "g", "cw", "rt", "e"):
        loads[name].wait()
    bd[...] = jnp.zeros_like(bd)
    for n in range(4):
        s = slice(64 * n, 64 * n + 64)
        bd[s, 64 * n : 64 * n + 64] = ga[n]
        bd[s, CH + 64 * n : CH + 64 * n + 64] = gx[n]
    xp[16:, :] = xb[...].astype(F32)
    geb[...] = gelu(gb[...].astype(F32))

    def scan1():
        arrived("halo", halo)
        xp[0:16, :] = jnp.where(sp > 0, halo[...].astype(F32), 0.0)
        conv = xp[13 : 13 + ROWS, :] * cw[0:1, :]
        for tap in range(1, 4):
            conv = conv + xp[13 + tap : 13 + tap + ROWS, :] * cw[tap : tap + 1, :]
        cout[...] = conv.astype(BF16)
        gates[...] = dot(cout[...], bd[...])

    held = {}

    def scan_rows(lo, hi, start):
        in_group = lax.broadcasted_iota(jnp.int32, (4, 8, CH), 1)

        def chunk(i, carry):
            rows = pl.ds(pl.multiple_of(i * 32, 32), 32)
            recur = sigmoid(gates[rows, 0:CH])
            inject = sigmoid(gates[rows, CH:])
            log_decay = (-LRU_SCALE * recur) * rt[...] + eb[rows, :]
            decay = jnp.exp(log_decay)
            grown = one_minus_exp(2.0 * log_decay)
            root = jnp.where(grown > 0.0, grown * lax.rsqrt(jnp.maximum(grown, 1e-37)), 0.0)
            drive = root * inject * cout[rows, :].astype(F32)
            a = decay.reshape(4, 8, CH)
            b = drive.reshape(4, 8, CH)
            for step in (1, 2, 4):
                keep = in_group >= step
                a_prev = jnp.where(keep, pltpu.roll(a, step, 1), 1.0)
                b_prev = jnp.where(keep, pltpu.roll(b, step, 1), 0.0)
                b = a * b_prev + b
                a = a * a_prev
            a_in, b_in = carry
            a_all, b_all = [], []
            for n in range(4):
                a_n = a[n] * a_in
                b_n = a[n] * b_in + b[n]
                a_in, b_in = a_n[7:8, :], b_n[7:8, :]
                a_all.append(a_n)
                b_all.append(b_n)
            acum[rows, :] = jnp.concatenate(a_all, axis=0)
            bcum[rows, :] = jnp.concatenate(b_all, axis=0)
            return a_in, b_in

        return lax.fori_loop(lo, hi, chunk, start)

    def scan2():
        held["half"] = scan_rows(0, 6, (jnp.ones((1, CH), F32), jnp.zeros((1, CH), F32)))

    def scan3():
        a_end, b_end = scan_rows(6, ROWS // 32, held["half"])
        tot[:, 0:CH] = a_end
        tot[:, CH:] = b_end
        for k in range(1, NF):
            send(tot, rowbuf.at[k - 1], along_y(k), "row", "row")

    def composed(own, buf, me):
        pa, pb = jnp.ones((1, CH), F32), jnp.zeros((1, CH), F32)
        ea, eb_ = pa, pb
        for place in range(NF):
            slot = (me - place + NF) % NF
            got = buf[jnp.maximum(slot - 1, 0)]
            is_me = slot == 0
            va = jnp.where(is_me, own[:, 0:CH], got[:, 0:CH])
            vb = jnp.where(is_me, own[:, CH:], got[:, CH:])
            ea = jnp.where(is_me, pa, ea)
            eb_ = jnp.where(is_me, pb, eb_)
            pa, pb = pa * va, va * pb + vb
        return (pa, pb), (ea, eb_)

    def row():
        arrived("row", rowbuf)
        (ra, rb_), held["in"] = composed(tot[...], rowbuf, y)
        rtot[:, 0:CH] = ra
        rtot[:, CH:] = rb_
        for k in range(1, NF):
            send(rtot, colbuf.at[k - 1], along_z(k), "col", "col")

    def col():
        arrived("col", colbuf)
        _, (col_a, col_b) = composed(rtot[...], colbuf, z)
        in_a, in_b = held["in"]
        held["carried"] = in_a * col_b + in_b

    def mixer_block(core, rel):
        block = ((x + rel) % NX) * 2 + core
        rows = pl.ds(pl.multiple_of(block * BLK, 16), BLK)
        return ((bcum[rows, :] + acum[rows, :] * held["carried"]) * geb[rows, :]).astype(BF16)

    def mix():
        for rel in range(NX):
            mixs[BLK * rel : BLK * rel + BLK, :] = mixer_block(1 - c, rel)
        send(mixs, mixb, partner, "mix", "mix")
        for rel in range(NX):
            mixa[BLK * rel : BLK * rel + BLK, :] = mixer_block(c, rel)
        arrived("wp", wp.at[1])
        parts[...] = dot(mixa[...], wp[0])

    def scatter_start(u, take, sbuf, bufs):
        rl_, rr_, fl_, fr_ = bufs
        for half in range(2):
            sbuf[half] = take(2, half).astype(BF16)
        send(sbuf.at[0], rl_, at_x(1), ("rl", u), ("sb", u))
        send(sbuf.at[1], rr_, at_x(NX - 1), ("rr", u), ("sb", u))
        sbuf[2] = take(1, 1).astype(BF16)
        send(sbuf.at[2], fl_.at[1], at_x(1), ("f", u), ("sb", u))
        sbuf[3] = take(3, 0).astype(BF16)
        send(sbuf.at[3], fr_.at[0], at_x(NX - 1), ("f", u), ("sb", u))

    def scatter_relay(u, take, sbuf, bufs):
        rl_, rr_, fl_, fr_ = bufs
        arrived(("rl", u), rl_)
        sbuf[4] = (take(1, 0) + rl_[...].astype(F32)).astype(BF16)
        send(sbuf.at[4], fl_.at[0], at_x(1), ("f", u), ("sb", u))
        arrived(("rr", u), rr_)
        sbuf[5] = (take(3, 1) + rr_[...].astype(F32)).astype(BF16)
        send(sbuf.at[5], fr_.at[1], at_x(NX - 1), ("f", u), ("sb", u))

    bufs = (rl, rr, fl, fr)

    def take(rel, half):
        return parts[BLK * rel : BLK * rel + BLK, 1024 * half : 1024 * half + 1024]

    def mix2():
        arrived("mix", mixb)
        parts[...] += dot(mixb[...], wp[1])
        scatter_start(0, take, sb, bufs)

    def relay():
        scatter_relay(0, take, sb, bufs)

    def norm_and_send():
        arrived(("f", 0), sb.at[0:4])
        for name in ("rs", "mg", "pg", "og"):
            loads[name].wait()
        halves = [take(0, half) + fl[half].astype(F32) + fr[half].astype(F32) for half in range(2)]
        mixed = jnp.concatenate(halves, axis=1)
        after_mix = rs_b[...].astype(F32) + rms_scale(mixed, mg[...])
        stream[...] = after_mix
        normed = rms_scale(after_mix, pg[...]).astype(BF16)
        nb[0, 0] = normed[:, 0:1024]
        nb[1, 0] = normed[:, 1024:]
        send(nb.at[0, 0], nb.at[0, 3], at_x(1), "al", "nb")
        send(nb.at[1, 0], nb.at[1, 1], at_x(NX - 1), "ar", "nb")
        send(nb.at[1, 0], nb.at[1, 3], at_x(1), "ab", "nb")
        send(nb.at[0, 0], nb.at[0, 1], at_x(NX - 1), "ab", "nb")

    def ag():
        arrived("al", nb.at[0, 3])
        send(nb.at[0, 3], nb.at[0, 2], at_x(1), "ab", "nb")
        arrived("ar", nb.at[1, 1])
        send(nb.at[1, 1], nb.at[1, 2], at_x(NX - 1), "ab", "nb")

    def agend():
        arrived("ab", nb.at[0])

    def gate_up(core, lanes):
        w = W[core, :, :, :, lanes]
        w = w.reshape(D, w.shape[-1])
        acc = dot(nb[0].reshape(NX * BLK, 1024), w[0:1024])
        return acc + dot(nb[1].reshape(NX * BLK, 1024), w[1024:])

    came = set()

    def came_from_partner(to, like):
        if to not in came:
            came.add(to)
            arrived(to, like)

    def gate_and_up(n, core):
        name = ("GA", "GB1", "GB2")[n]
        came_from_partner("P0", W.at[c, 0, :, :, ALL])
        came_from_partner("P" + name, W.at[c, 0:7, :, :, LANES[name]])
        both = gate_up(core, LANES[name])
        if n > 0:
            g, u = both[:, 0:256], both[:, 256:512]
            hid[core, :, 256 * n - 256 : 256 * n] = (g * sigmoid(g) * u).astype(BF16)
        else:
            g, u = both[:, 0:128], both[:, 128:256]
            hid[core, :, 512:640] = (g * sigmoid(g) * u).astype(BF16)
            g = both[:, 256:384]
            u = pltpu.roll(g, 64, 1)
            lane = lax.broadcasted_iota(jnp.int32, g.shape, 1)
            hid[core, :, 640:768] = jnp.where(lane < 64, g * sigmoid(g) * u, 0.0).astype(BF16)

    def place(i):
        return (z + NF + (i + 1) // 2 * (1 - 2 * (i % 2))) % NF

    def down(i, parts_of_k):
        acc = jnp.zeros((NX * BLK, 256), F32)
        for core in range(2):
            for lanes in parts_of_k:
                w = W[core, place(i), :, :, lanes]
                acc = acc + dot_nt(hid[core, :, lanes], w.reshape(256, lanes.stop - lanes.start))
        return acc

    def down_first(i):
        if i > 0:
            came_from_partner(("PDA", (i + 1) // 2), W.at[c, 0 : 2 if i < 7 else 1, :, :, LANES["DA"]])
        parts2[i] = down(i, (slice(0, 256), slice(512, 768)))

    def down_last(i):
        parts2[i] += down(i, (slice(256, 512),))

    bufs0 = (rl0, rr0, fl0, fr0)
    bufs1 = (rl1, rr1, fl1, fr1)

    def take0(rel, half):
        return parts2[0:3, BLK * rel : BLK * rel + BLK, 128 * half : 128 * half + 128]

    def take1(rel, half):
        return parts2[3:7, BLK * rel : BLK * rel + BLK, 128 * half : 128 * half + 128]

    def g0s():
        scatter_start(1, take0, sb0, bufs0)

    def g0r():
        scatter_relay(1, take0, sb0, bufs0)

    def g1s():
        scatter_start(2, take1, sb1, bufs1)

    def g1r():
        scatter_relay(2, take1, sb1, bufs1)

    def g2s():
        for k, (rel, step) in enumerate(((2, 2), (1, 1), (3, NX - 1))):
            sb2[k] = parts2[7, BLK * rel : BLK * rel + BLK, :].astype(BF16)
            send(sb2.at[k], rb2.at[k], at_x(step), "d", "d")

    steps = {
        "scan1": scan1, "scan2": scan2, "scan3": scan3, "row": row, "col": col, "mix": mix, "mix2": mix2,
        "relay": relay, "send": norm_and_send, "ag": ag, "agend": agend, "g0s": g0s, "g0r": g0r, "g1s": g1s,
        "g1r": g1r, "g2s": g2s,
    }
    for n in range(3):
        for core in range(2):
            steps["u%dc%d" % (n, core)] = functools.partial(gate_and_up, n, core)
    for i in range(NF):
        steps["e%d" % i] = functools.partial(down_first, i)
        steps["f%d" % i] = functools.partial(down_last, i)

    for name, t, q in ORDER:
        if name in steps:
            steps[name]()
        elif name[0] == "S":
            fam = name[1]
            hop1_done(fam, t)
            if t < 4:
                hop1(fam, t + 1)
            else:
                ref = row_of(fam, second[fam], LA if fam == "A" else LB)
                send(ref, ref, partner, "P0", "P0")
            hop2("GA" if fam == "A" else "GB1", 1, t)
        elif name[0] == "P":
            to_partner(name[1:], t)
        elif name[0] == "Q":
            group_to_partner(name[1:], t, q)
        else:
            if t > 0:
                hop2_done(name, t, q)
            if t < 4:
                hop2(name, t + 1, q)

    def put(i, lane, value):
        ffn[:, pl.ds(pl.multiple_of(place(i) * 256 + lane, 128), value.shape[-1])] = value

    for u, lo, hi, take_, sbuf, (_, _, fl_, fr_) in ((1, 0, 3, take0, sb0, bufs0), (2, 3, 7, take1, sb1, bufs1)):
        arrived(("f", u), sbuf.at[0:4])
        for half in range(2):
            got = take_(0, half) + fl_[half].astype(F32) + fr_[half].astype(F32)
            for i in range(lo, hi):
                put(i, 128 * half, got[i - lo])
    arrived("d", rb2)
    put(7, 0, parts2[7, 0:BLK, :] + sum(rb2[k].astype(F32) for k in range(3)))
    out[...] = (stream[...] + 0.5 * rms_scale(ffn[...], og[...])).astype(BF16)

    for fam, lanes in (("A", LA), ("B", LB)):
        sent("S" + fam, W.at[c, 0, 0:7, :, lanes])
    for name in LANES:
        sent(name, W.at[c, 0:7, :, :, LANES[name]])
    sent("P0", W.at[c, 0, :, :, ALL])
    for name in ("GA", "GB1", "GB2"):
        sent("P" + name, W.at[c, 0:7, :, :, LANES[name]])
    for t, n in ((1, 2), (2, 2), (3, 2), (4, 1)):
        sent(("PDA", t), W.at[c, 0:n, :, :, LANES["DA"]])
    for out_, ref in (
        ("halo", halo), ("wp", wp.at[1]), ("row", rowbuf), ("col", colbuf), ("mix", mixb), (("sb", 0), sb),
        ("nb", sb), (("sb", 1), sb0), (("sb", 2), sb1), ("d", sb2),
    ):
        sent(out_, ref)
    assert len(recv_ids) <= NRECV and len(send_ids) <= NSEND, (len(recv_ids), len(send_ids))


def shards(
    resid, x_branch, gate_branch, conv_w, gate_a_w, gate_x_w, decay_rate, decay_extra, w_proj, mix_gain,
    pre_gain, w_gate, w_up, w_down, out_gain,
):
    vmem = pltpu.VMEM
    return pl.pallas_call(
        kernel,
        out_shape=jax.ShapeDtypeStruct((BLK, D), BF16),
        in_specs=[pl.BlockSpec(memory_space=pl.ANY)] * 15,
        out_specs=pl.BlockSpec(memory_space=pltpu.VMEM),
        scratch_shapes=[
            vmem((2, NF, NF, 32, WL), BF16),
            vmem((2, CH, D), BF16),
            vmem((ROWS, CH), BF16),
            vmem((ROWS + 16, CH), F32),
            vmem((ROWS, CH), BF16),
            vmem((ROWS, CH), F32),
            vmem((4, CH), F32),
            vmem((4, 64, 64), BF16),
            vmem((4, 64, 64), BF16),
            vmem((1, CH), F32),
            vmem((1, D), F32),
            vmem((1, D), F32),
            vmem((1, D), F32),
            vmem((32, HID), BF16),
            vmem((32, HID), BF16),
            vmem((32, HID), BF16),
            vmem((BLK, D), BF16),
            vmem((16, CH), BF16),
            vmem((CH, 2 * CH), BF16),
            vmem((ROWS, CH), BF16),
            vmem((ROWS, 2 * CH), F32),
            vmem((ROWS, CH), F32),
            vmem((ROWS, CH), F32),
            vmem((ROWS, CH), F32),
            vmem((1, 2 * CH), F32),
            vmem((NF - 1, 1, 2 * CH), F32),
            vmem((1, 2 * CH), F32),
            vmem((NF - 1, 1, 2 * CH), F32),
            vmem((NX * BLK, CH), BF16),
            vmem((NX * BLK, CH), BF16),
            vmem((NX * BLK, CH), BF16),
            vmem((NX * BLK, D), F32),
            vmem((BLK, D), F32),
            vmem((6, BLK, 1024), BF16),
            vmem((BLK, 1024), BF16),
            vmem((BLK, 1024), BF16),
            vmem((2, BLK, 1024), BF16),
            vmem((2, BLK, 1024), BF16),
            vmem((2, NX, BLK, 1024), BF16),
            vmem((2, NX * BLK, 768), BF16),
            vmem((NF, NX * BLK, 256), F32),
            vmem((6, 3, BLK, 128), BF16),
            vmem((3, BLK, 128), BF16),
            vmem((3, BLK, 128), BF16),
            vmem((2, 3, BLK, 128), BF16),
            vmem((2, 3, BLK, 128), BF16),
            vmem((6, 4, BLK, 128), BF16),
            vmem((4, BLK, 128), BF16),
            vmem((4, BLK, 128), BF16),
            vmem((2, 4, BLK, 128), BF16),
            vmem((2, 4, BLK, 128), BF16),
            vmem((3, BLK, 256), BF16),
            vmem((3, BLK, 256), BF16),
            vmem((BLK, D), F32),
            pltpu.SemaphoreType.DMA((15,)),
            pltpu.SemaphoreType.DMA((NSEND,)),
            pltpu.SemaphoreType.DMA((NRECV,)),
        ],
        compiler_params=pltpu.CompilerParams(
            collective_id=0, has_side_effects=True, vmem_limit_bytes=58 * 1024 * 1024
        ),
        name="layer",
    )(
        resid, x_branch, gate_branch, conv_w, gate_a_w, gate_x_w, decay_rate.reshape(1, CH), decay_extra,
        w_proj, mix_gain.reshape(1, D), pre_gain.reshape(1, D), w_gate, w_up, w_down.T, out_gain.reshape(1, D),
    )


def solution(mesh):
    return jax.shard_map(
        shards,
        mesh=mesh,
        in_specs=(
            P("sp", None),
            P("sp", "tp"),
            P("sp", "tp"),
            P(None, "tp"),
            P("tp", None, None),
            P("tp", None, None),
            P("tp"),
            P("sp", "tp"),
            P("tp", None),
            P(),
            P(),
            P("sp", "tp"),
            P("sp", "tp"),
            P("tp", "sp"),
            P(),
        ),
        out_specs=P(("sp", "tp"), None),
        check_vma=False,
    )
```

```python
import functools

import jax
import jax.numpy as jnp
from jax import lax
from jax.experimental import pallas as pl
from jax.experimental.pallas import tpu as pltpu
from jax.sharding import PartitionSpec as P

LRU_SCALE = 8.0
NORM_EPS = 1e-06
MESH = pl.DeviceIdType.MESH
F32 = jnp.float32
BF16 = jnp.bfloat16

NF = 8
NX = 4
ROWS = 384
CH = 256
D = 2048
BLK = 48
HID = 704
WL = 2176
LANES = {"DA": slice(0, 768), "GA": slice(768, 1152), "GB1": slice(1152, 1664), "GB2": slice(1664, 2176)}
LA, LB = slice(0, 1152), slice(1152, WL)
GROUPS = ((0,), (1, 2), (3, 4), (5, 6), (7,))
NRECV = 111
NSEND = 21

ORDER = (
    ("GB1", 0, 0), ("GA", 0, 0), ("GB2", 0, 0), ("DA", 0, 0), ("scan1", 0, 0), ("SB", 1, 0), ("GB1", 0, 1),
    ("SA", 1, 0), ("scan2", 0, 0), ("GA", 0, 1), ("scan3", 0, 0), ("GB1", 1, 0), ("GA", 1, 0), ("DA", 0, 1),
    ("GB2", 0, 1), ("SB", 2, 0), ("GB1", 0, 2), ("GB1", 1, 1), ("SA", 2, 0), ("GA", 1, 1), ("GA", 2, 0),
    ("GA", 0, 2), ("GB1", 2, 0), ("row", 0, 0), ("DA", 1, 0), ("SB", 3, 0), ("GB1", 0, 3), ("GA", 2, 1),
    ("GB1", 1, 2), ("GA", 3, 0), ("GB1", 2, 1), ("GA", 1, 2), ("SA", 3, 0), ("GA", 0, 3), ("DA", 0, 2),
    ("SB", 4, 0), ("GB1", 3, 0), ("GB1", 0, 4), ("col", 0, 0), ("GB1", 1, 3), ("GA", 3, 1), ("GA", 4, 0),
    ("mix", 0, 0), ("GA", 2, 2), ("GB1", 2, 2), ("GA", 1, 3), ("mix2", 0, 0), ("GB1", 3, 1), ("SA", 4, 0),
    ("GA", 0, 4), ("GB1", 4, 0), ("DA", 1, 1), ("GB1", 1, 4), ("GA", 4, 1), ("GB2", 1, 0), ("GB1", 2, 3),
    ("GA", 3, 2), ("DA", 0, 3), ("GB1", 3, 2), ("relay", 0, 0), ("GB1", 4, 1), ("GB2", 0, 2), ("GA", 2, 3),
    ("GB1", 2, 4), ("GA", 1, 4), ("GB2", 1, 1), ("GA", 4, 2), ("DA", 2, 0), ("GB1", 3, 3), ("GB1", 4, 2),
    ("DA", 0, 4), ("send", 0, 0), ("GB2", 0, 3), ("DA", 1, 2), ("GB1", 3, 4), ("GA", 3, 3), ("GB2", 0, 4),
    ("GA", 2, 4), ("GB2", 2, 0), ("GB2", 1, 2), ("GB1", 4, 3), ("DA", 2, 1), ("ag", 0, 0), ("GB2", 2, 1),
    ("GB1", 4, 4), ("DA", 1, 3), ("GB2", 1, 3), ("GA", 4, 3), ("ag2", 0, 0), ("GA", 3, 4), ("GB2", 1, 4),
    ("GB2", 3, 0), ("DA", 3, 0), ("GB2", 2, 2), ("DA", 1, 4), ("agend", 0, 0), ("DA", 2, 2), ("GB2", 3, 1),
    ("GB2", 2, 3), ("agp", 0, 0), ("u1", 0, 0), ("DA", 3, 1), ("GB2", 2, 4), ("GA", 4, 4), ("GB2", 4, 0),
    ("DA", 4, 0), ("u0", 0, 0), ("DA", 2, 3), ("GB2", 3, 2), ("GB2", 4, 1), ("DA", 2, 4), ("e0", 0, 0),
    ("DA", 3, 2), ("GB2", 3, 3), ("GB2", 3, 4), ("DA", 4, 1), ("GB2", 4, 2), ("DA", 3, 3), ("GB2", 4, 3),
    ("GB2", 4, 4), ("u2p", 0, 0), ("DA", 3, 4), ("f0p", 0, 0), ("e1", 0, 0), ("DA", 4, 2), ("h0", 0, 0),
    ("f1p", 0, 0), ("h1", 0, 0), ("u2o", 0, 0), ("DA", 4, 3), ("f0o", 0, 0), ("DA", 4, 4), ("f1o", 0, 0),
    ("g0s", 0, 0), ("e2", 0, 0), ("g1s", 0, 0), ("f2p", 0, 0), ("h2", 0, 0), ("f2o", 0, 0), ("g2s", 0, 0),
    ("g0r", 0, 0), ("g1r", 0, 0),
)


def dot(a, b):
    return jnp.dot(a, b, preferred_element_type=F32)


def dot_nt(a, b):
    return lax.dot_general(a, b, (((1,), (1,)), ((), ())), preferred_element_type=F32)


def sigmoid(v):
    return 1.0 / (1.0 + jnp.exp(-v))


def gelu(v):
    inner = 0.7978845608028654 * (v + 0.044715 * (v * v * v))
    return 0.5 * v * (1.0 + jnp.tanh(inner))


def one_minus_exp(w):
    series = 1.0 + w * (1.0 / 6.0)
    for n in (5.0, 4.0, 3.0, 2.0):
        series = 1.0 + w * (1.0 / n) * series
    return jnp.where(w > -0.25, -w * series, 1.0 - jnp.exp(w))


def rms_scale(values, gains):
    mean = jnp.sum(values * values, axis=-1, keepdims=True) * (1.0 / D)
    return values * lax.rsqrt(mean + NORM_EPS) * gains


def kernel(
    resid, x_in, g_in, conv_w, ga_in, gx_in, rate, extra, wp_in, mixg, preg, wg_in, wu_in, wd_in, outg,
    out,
    W, wp, xb, xp, gb, eb, cw, ga, gx, rt, mg, pg, og, wg, wu, wd, rs_b,
    halo, bd, cout, gates, acum, bcum, geb, tot, rowbuf, rtot, colbuf,
    mixa, mixs, mixb, parts, stream, sb, rl, rr, fl, fr, nb, hid,
    parts2, psend, pbuf, sb0, rl0, rr0, fl0, fr0, sb1, rl1, rr1, fl1, fr1, sb2, rb2, ffn,
    local_sem, send_sem, recv_sem,
):
    sp = lax.axis_index("sp")
    tp = lax.axis_index("tp")
    z, y = sp // NF, sp % NF
    x, c = tp // 2, tp % 2

    def at_zy(zz, yy):
        return {"sp": zz * NF + yy, "tp": tp}

    def at_x(step):
        return {"sp": sp, "tp": ((x + step) % NX) * 2 + c}

    partner = {"sp": sp, "tp": x * 2 + (1 - c)}
    behind = {"sp": (sp + NF * NF - 1) % (NF * NF), "tp": tp}
    ahead = {"sp": (sp + 1) % (NF * NF), "tp": tp}

    loads = {}

    def load(name, src, dst):
        copy = pltpu.make_async_copy(src, dst, local_sem.at[len(loads)])
        copy.start()
        loads[name] = copy

    load("wg", wg_in, wg)
    load("wu", wu_in, wu)
    load("wd", wd_in, wd)
    load("x", x_in, xb)
    load("ga", ga_in, ga)
    load("gx", gx_in, gx)
    load("g", g_in, gb)
    load("cw", conv_w, cw)
    load("rt", rate, rt)
    load("e", extra, eb)
    load("wp", wp_in, wp.at[0])
    load("rs", resid.at[pl.ds(pl.multiple_of(tp * BLK, 16), BLK), :], rs_b)
    load("mg", mixg, mg)
    load("pg", preg, pg)
    load("og", outg, og)

    barrier = pltpu.get_barrier_semaphore()
    peers = [at_zy(z, (y + k) % NF) for k in range(1, NF)]
    peers += [at_zy((z + k) % NF, y) for k in range(1, NF)]
    peers += [at_x(1), at_x(2), at_x(NX - 1), partner, behind, ahead]
    for peer in peers:
        pl.semaphore_signal(barrier, inc=1, device_id=peer, device_id_type=MESH)

    for name in ("wg", "wu", "wd"):
        loads[name].wait()
    mine = W.at[z, y]
    mine[:, 0:640] = wd[:, 0:640]
    mine[:, 640:768] = jnp.concatenate([wd[:, 640:704], jnp.zeros((32, 64), BF16)], axis=1)
    mine[:, 768:896] = wg[:, 512:640]
    mine[:, 896:1024] = wu[:, 512:640]
    mine[:, 1024:1152] = jnp.concatenate([wg[:, 640:704], wu[:, 640:704]], axis=1)
    for n in range(2):
        mine[:, 512 * n + 1152 : 512 * n + 1408] = wg[:, 256 * n : 256 * n + 256]
        mine[:, 512 * n + 1408 : 512 * n + 1664] = wu[:, 256 * n : 256 * n + 256]

    send_ids, recv_ids = {}, {}

    def send(src, dst, device, to, out):
        copy = pltpu.make_async_remote_copy(
            src_ref=src,
            dst_ref=dst,
            send_sem=send_sem.at[send_ids.setdefault(out, len(send_ids))],
            recv_sem=recv_sem.at[recv_ids.setdefault(to, len(recv_ids))],
            device_id=device,
            device_id_type=MESH,
        )
        copy.start()

    def arrived(to, like):
        pltpu.make_async_copy(like, like, recv_sem.at[recv_ids[to]]).wait()

    def sent(out, like):
        pltpu.make_async_copy(like, like, send_sem.at[send_ids[out]]).wait()

    def mod(v):
        return (v + NF) % NF

    def piece(fam, first, second, lanes):
        return W.at[second, first, :, lanes] if fam == "A" else W.at[first, second, :, lanes]

    def some(n, lanes):
        return W.at[0, 0:n, :, lanes]

    first = {"A": y, "B": z}
    second = {"A": z, "B": y}

    def along_y(step):
        return at_zy(z, (y + step) % NF)

    def along_z(step):
        return at_zy((z + step) % NF, y)

    along_first = {"A": along_y, "B": along_z}
    along_second = {"A": along_z, "B": along_y}
    WAYS = ((1, -1), (NF - 1, 1))

    def hop1(fam, k):
        whole = LA if fam == "A" else LB
        cut = whole.start + (640 if fam == "A" else 512)
        for d, (step, sign) in enumerate(WAYS):
            lanes = whole if k < 4 else (slice(whole.start, cut) if d == 0 else slice(cut, whole.stop))
            ref = piece(fam, mod(first[fam] + sign * (k - 1)), second[fam], lanes)
            send(ref, ref, along_first[fam](step), ("S" + fam, k), "S" + fam)

    def hop1_done(fam, k):
        whole = LA if fam == "A" else LB
        arrived(("S" + fam, k), some(2 if k < 4 else 1, whole))

    def offset(j):
        return (j + 1) // 2 * (-1 if j % 2 == 1 else 1)

    def hop2(name, t, q):
        fam, lanes = name[1], LANES[name]
        for d, (step, sign) in enumerate(WAYS):
            for j in GROUPS[q]:
                if t == 4 and (j < 4) != (d == 0):
                    continue
                ref = piece(fam, mod(first[fam] + offset(j)), mod(second[fam] + sign * (t - 1)), lanes)
                send(ref, ref, along_second[fam](step), (name, t, q), name)

    def hop2_done(name, t, q):
        n = len(GROUPS[q])
        arrived((name, t, q), some(2 * n if t < 4 else n, LANES[name]))

    loads["x"].wait()
    pl.semaphore_wait(barrier, len(peers))
    send(xb.at[pl.ds(ROWS - 16, 16), :], halo, ahead, "halo", "halo")
    hop1("A", 1)
    hop1("B", 1)
    loads["wp"].wait()
    send(wp.at[0], wp.at[1], partner, "wp", "wp")
    for name in ("ga", "gx", "g", "cw", "rt", "e"):
        loads[name].wait()
    bd[...] = jnp.zeros_like(bd)
    for n in range(4):
        s = slice(64 * n, 64 * n + 64)
        bd[s, 64 * n : 64 * n + 64] = ga[n]
        bd[s, CH + 64 * n : CH + 64 * n + 64] = gx[n]
    xp[16:, :] = xb[...].astype(F32)
    geb[...] = gelu(gb[...].astype(F32))

    def scan1():
        arrived("halo", halo)
        xp[0:16, :] = jnp.where(sp > 0, halo[...].astype(F32), 0.0)
        conv = xp[13 : 13 + ROWS, :] * cw[0:1, :]
        for tap in range(1, 4):
            conv = conv + xp[13 + tap : 13 + tap + ROWS, :] * cw[tap : tap + 1, :]
        cout[...] = conv.astype(BF16)
        gates[...] = dot(cout[...], bd[...])

    held = {}

    def scan_rows(lo, hi, start):
        in_group = lax.broadcasted_iota(jnp.int32, (4, 8, CH), 1)

        def chunk(i, carry):
            rows = pl.ds(pl.multiple_of(i * 32, 32), 32)
            recur = sigmoid(gates[rows, 0:CH])
            inject = sigmoid(gates[rows, CH:])
            log_decay = (-LRU_SCALE * recur) * rt[...] + eb[rows, :]
            decay = jnp.exp(log_decay)
            grown = one_minus_exp(2.0 * log_decay)
            root = jnp.where(grown > 0.0, grown * lax.rsqrt(jnp.maximum(grown, 1e-37)), 0.0)
            drive = root * inject * cout[rows, :].astype(F32)
            a = decay.reshape(4, 8, CH)
            b = drive.reshape(4, 8, CH)
            for step in (1, 2, 4):
                keep = in_group >= step
                a_prev = jnp.where(keep, pltpu.roll(a, step, 1), 1.0)
                b_prev = jnp.where(keep, pltpu.roll(b, step, 1), 0.0)
                b = a * b_prev + b
                a = a * a_prev
            a_in, b_in = carry
            a_all, b_all = [], []
            for n in range(4):
                a_n = a[n] * a_in
                b_n = a[n] * b_in + b[n]
                a_in, b_in = a_n[7:8, :], b_n[7:8, :]
                a_all.append(a_n)
                b_all.append(b_n)
            acum[rows, :] = jnp.concatenate(a_all, axis=0)
            bcum[rows, :] = jnp.concatenate(b_all, axis=0)
            return a_in, b_in

        return lax.fori_loop(lo, hi, chunk, start)

    def scan2():
        held["half"] = scan_rows(0, 6, (jnp.ones((1, CH), F32), jnp.zeros((1, CH), F32)))

    def scan3():
        a_end, b_end = scan_rows(6, ROWS // 32, held["half"])
        tot[:, 0:CH] = a_end
        tot[:, CH:] = b_end
        for k in range(1, NF):
            send(tot, rowbuf.at[k - 1], along_y(k), "row", "row")

    def composed(own, buf, me):
        pa, pb = jnp.ones((1, CH), F32), jnp.zeros((1, CH), F32)
        ea, eb_ = pa, pb
        for place in range(NF):
            slot = (me - place + NF) % NF
            got = buf[jnp.maximum(slot - 1, 0)]
            is_me = slot == 0
            va = jnp.where(is_me, own[:, 0:CH], got[:, 0:CH])
            vb = jnp.where(is_me, own[:, CH:], got[:, CH:])
            ea = jnp.where(is_me, pa, ea)
            eb_ = jnp.where(is_me, pb, eb_)
            pa, pb = pa * va, va * pb + vb
        return (pa, pb), (ea, eb_)

    def row():
        arrived("row", rowbuf)
        (ra, rb_), held["in"] = composed(tot[...], rowbuf, y)
        rtot[:, 0:CH] = ra
        rtot[:, CH:] = rb_
        for k in range(1, NF):
            send(rtot, colbuf.at[k - 1], along_z(k), "col", "col")

    def col():
        arrived("col", colbuf)
        _, (col_a, col_b) = composed(rtot[...], colbuf, z)
        in_a, in_b = held["in"]
        held["carried"] = in_a * col_b + in_b

    def mixer_block(core, rel):
        block = ((x + rel) % NX) * 2 + core
        rows = pl.ds(pl.multiple_of(block * BLK, 16), BLK)
        return ((bcum[rows, :] + acum[rows, :] * held["carried"]) * geb[rows, :]).astype(BF16)

    def mix():
        for rel in range(NX):
            mixs[BLK * rel : BLK * rel + BLK, :] = mixer_block(1 - c, rel)
        send(mixs, mixb, partner, "mix", "mix")
        for rel in range(NX):
            mixa[BLK * rel : BLK * rel + BLK, :] = mixer_block(c, rel)
        arrived("wp", wp.at[1])
        parts[...] = dot(mixa[...], wp[0])

    def scatter_start(u, take, sbuf, bufs):
        rl_, rr_, fl_, fr_ = bufs
        for half in range(2):
            sbuf[half] = take(2, half).astype(BF16)
        send(sbuf.at[0], rl_, at_x(1), ("rl", u), ("sb", u))
        send(sbuf.at[1], rr_, at_x(NX - 1), ("rr", u), ("sb", u))
        sbuf[2] = take(1, 1).astype(BF16)
        send(sbuf.at[2], fl_.at[1], at_x(1), ("f", u), ("sb", u))
        sbuf[3] = take(3, 0).astype(BF16)
        send(sbuf.at[3], fr_.at[0], at_x(NX - 1), ("f", u), ("sb", u))

    def scatter_relay(u, take, sbuf, bufs):
        rl_, rr_, fl_, fr_ = bufs
        arrived(("rl", u), rl_)
        sbuf[4] = (take(1, 0) + rl_[...].astype(F32)).astype(BF16)
        send(sbuf.at[4], fl_.at[0], at_x(1), ("f", u), ("sb", u))
        arrived(("rr", u), rr_)
        sbuf[5] = (take(3, 1) + rr_[...].astype(F32)).astype(BF16)
        send(sbuf.at[5], fr_.at[1], at_x(NX - 1), ("f", u), ("sb", u))

    bufs = (rl, rr, fl, fr)

    def take(rel, half):
        return parts[BLK * rel : BLK * rel + BLK, 1024 * half : 1024 * half + 1024]

    def mix2():
        arrived("mix", mixb)
        parts[...] += dot(mixb[...], wp[1])
        scatter_start(0, take, sb, bufs)

    def relay():
        scatter_relay(0, take, sb, bufs)

    def norm_and_send():
        arrived(("f", 0), sb.at[0:4])
        for name in ("rs", "mg", "pg", "og"):
            loads[name].wait()
        halves = [take(0, half) + fl[half].astype(F32) + fr[half].astype(F32) for half in range(2)]
        mixed = jnp.concatenate(halves, axis=1)
        after_mix = rs_b[...].astype(F32) + rms_scale(mixed, mg[...])
        stream[...] = after_mix
        normed = rms_scale(after_mix, pg[...]).astype(BF16)
        nb[0, 0] = normed[:, 0:1024]
        nb[1, 0] = normed[:, 1024:]
        send(nb.at[0, 0], nb.at[0, 3], at_x(1), "al", "nb")
        send(nb.at[1, 0], nb.at[1, 1], at_x(NX - 1), "ar", "nb")
        send(nb.at[1, 0], nb.at[1, 3], at_x(1), "an", "nb")
        send(nb.at[0, 0], nb.at[0, 1], at_x(NX - 1), "an", "nb")
        for half in range(2):
            to_partner(half, 0)

    def to_partner(half, rel):
        send(nb.at[half, rel], nb.at[half, NX + rel], partner, "nbp", "nbp")

    def ag():
        arrived("al", nb.at[0, 3])
        send(nb.at[0, 3], nb.at[0, 2], at_x(1), "ab", "nb")
        to_partner(0, 3)
        arrived("ar", nb.at[1, 1])
        send(nb.at[1, 1], nb.at[1, 2], at_x(NX - 1), "ab", "nb")
        to_partner(1, 1)

    def ag2():
        arrived("an", nb.at[0, 0:2])
        to_partner(1, 3)
        to_partner(0, 1)

    def agend():
        arrived("ab", nb.at[0, 0:2])
        to_partner(0, 2)
        to_partner(1, 2)

    def agp():
        arrived("nbp", nb.at[0])

    HALF = NX * BLK
    mine_rows, other_rows, all_rows = slice(0, HALF), slice(HALF, 2 * HALF), slice(0, 2 * HALF)

    def gate_up(n, span):
        w = W[:, :, :, LANES[("GA", "GB1", "GB2")[n]]]
        w = w.reshape(D, w.shape[-1])
        rows = span.stop - span.start
        at = slice(span.start // BLK, span.stop // BLK)
        both = dot(nb[0, at].reshape(rows, 1024), w[0:1024]) + dot(nb[1, at].reshape(rows, 1024), w[1024:])
        if n > 0:
            g, u = both[:, 0:256], both[:, 256:512]
            hid[span, 256 * n - 256 : 256 * n] = (g * sigmoid(g) * u).astype(BF16)
        else:
            g, u = both[:, 0:128], both[:, 128:256]
            hid[span, 512:640] = (g * sigmoid(g) * u).astype(BF16)
            g = both[:, 256:384]
            u = pltpu.roll(g, 64, 1)
            lane = lax.broadcasted_iota(jnp.int32, g.shape, 1)
            hid[span, 640:768] = jnp.where(lane < 64, g * sigmoid(g) * u, 0.0).astype(BF16)

    def place(i):
        return (z + NF + (i + 1) // 2 * (1 - 2 * (i % 2))) % NF

    def down(i, rows, lanes):
        w = W[place(i), :, :, lanes]
        return dot_nt(hid[rows, lanes], w.reshape(256, lanes.stop - lanes.start))

    def down_first(lo, hi):
        for i in range(lo, hi):
            parts2[i] = down(i, all_rows, slice(0, 256)) + down(i, all_rows, slice(512, 768))

    def down_last(u, rows):
        for i in range(*SPANS[u]):
            parts2[i, rows] += down(i, rows, slice(256, 512))

    SPANS = ((0, 4), (4, 7), (7, 8))

    def pair_start(u):
        span = slice(*SPANS[u])
        psend[span] = parts2[span, other_rows, :].astype(BF16)
        send(psend.at[span], pbuf.at[span], partner, ("h", u), ("h", u))

    def pair_end(u):
        span = slice(*SPANS[u])
        arrived(("h", u), pbuf.at[span])
        parts2[span, mine_rows, :] += pbuf[span].astype(F32)

    bufs0 = (rl0, rr0, fl0, fr0)
    bufs1 = (rl1, rr1, fl1, fr1)

    def take0(rel, half):
        return parts2[0:4, BLK * rel : BLK * rel + BLK, 128 * half : 128 * half + 128]

    def take1(rel, half):
        return parts2[4:7, BLK * rel : BLK * rel + BLK, 128 * half : 128 * half + 128]

    def g0s():
        pair_end(0)
        scatter_start(1, take0, sb0, bufs0)

    def g0r():
        scatter_relay(1, take0, sb0, bufs0)

    def g1s():
        pair_end(1)
        scatter_start(2, take1, sb1, bufs1)

    def g1r():
        scatter_relay(2, take1, sb1, bufs1)

    def g2s():
        pair_end(2)
        for k, (rel, step) in enumerate(((2, 2), (1, 1), (3, NX - 1))):
            sb2[k] = parts2[7, BLK * rel : BLK * rel + BLK, :].astype(BF16)
            send(sb2.at[k], rb2.at[k], at_x(step), "d", "d")

    steps = {
        "scan1": scan1, "scan2": scan2, "scan3": scan3, "row": row, "col": col, "mix": mix, "mix2": mix2,
        "relay": relay, "send": norm_and_send, "ag": ag, "agend": agend, "g0s": g0s, "g0r": g0r, "g1s": g1s,
        "g1r": g1r, "g2s": g2s, "agp": agp, "ag2": ag2,
    }
    for n in range(2):
        steps["u%d" % n] = functools.partial(gate_up, n, all_rows)
    for n, span in enumerate(((0, 5), (5, 7), (7, 8))):
        steps["e%d" % n] = functools.partial(down_first, *span)
        steps["h%d" % n] = functools.partial(pair_start, n)
    for name, rows in (("p", other_rows), ("o", mine_rows)):
        steps["u2" + name] = functools.partial(gate_up, 2, rows)
        for n in range(3):
            steps["f%d" % n + name] = functools.partial(down_last, n, rows)

    for name, t, q in ORDER:
        if name in steps:
            steps[name]()
        elif name[0] == "S":
            fam = name[1]
            hop1_done(fam, t)
            if t < 4:
                hop1(fam, t + 1)
        else:
            if t > 0:
                hop2_done(name, t, q)
            if t < 4:
                hop2(name, t + 1, q)

    def put(i, lane, value):
        ffn[:, pl.ds(pl.multiple_of(place(i) * 256 + lane, 128), value.shape[-1])] = value

    for u, lo, hi, take_, sbuf, (_, _, fl_, fr_) in ((1, 0, 4, take0, sb0, bufs0), (2, 4, 7, take1, sb1, bufs1)):
        arrived(("f", u), sbuf.at[0:4])
        for half in range(2):
            got = take_(0, half) + fl_[half].astype(F32) + fr_[half].astype(F32)
            for i in range(lo, hi):
                put(i, 128 * half, got[i - lo])
    arrived("d", rb2)
    put(7, 0, parts2[7, 0:BLK, :] + sum(rb2[k].astype(F32) for k in range(3)))
    out[...] = (stream[...] + 0.5 * rms_scale(ffn[...], og[...])).astype(BF16)

    for fam, lanes in (("A", LA), ("B", LB)):
        sent("S" + fam, W.at[0, 0:7, :, lanes])
    for name in LANES:
        sent(name, W.at[0:7, :, :, LANES[name]])
    for u, span in enumerate(SPANS):
        sent(("h", u), psend.at[slice(*span)])
    for out_, ref in (
        ("halo", halo), ("wp", wp.at[1]), ("row", rowbuf), ("col", colbuf), ("mix", mixb), (("sb", 0), sb),
        ("nb", sb), ("nbp", nb.at[0]), (("sb", 1), sb0), (("sb", 2), sb1), ("d", sb2),
    ):
        sent(out_, ref)
    assert len(recv_ids) <= NRECV and len(send_ids) <= NSEND, (len(recv_ids), len(send_ids))


def shards(
    resid, x_branch, gate_branch, conv_w, gate_a_w, gate_x_w, decay_rate, decay_extra, w_proj, mix_gain,
    pre_gain, w_gate, w_up, w_down, out_gain,
):
    vmem = pltpu.VMEM
    return pl.pallas_call(
        kernel,
        out_shape=jax.ShapeDtypeStruct((BLK, D), BF16),
        in_specs=[pl.BlockSpec(memory_space=pl.ANY)] * 15,
        out_specs=pl.BlockSpec(memory_space=pltpu.VMEM),
        scratch_shapes=[
            vmem((NF, NF, 32, WL), BF16),
            vmem((2, CH, D), BF16),
            vmem((ROWS, CH), BF16),
            vmem((ROWS + 16, CH), F32),
            vmem((ROWS, CH), BF16),
            vmem((ROWS, CH), F32),
            vmem((4, CH), F32),
            vmem((4, 64, 64), BF16),
            vmem((4, 64, 64), BF16),
            vmem((1, CH), F32),
            vmem((1, D), F32),
            vmem((1, D), F32),
            vmem((1, D), F32),
            vmem((32, HID), BF16),
            vmem((32, HID), BF16),
            vmem((32, HID), BF16),
            vmem((BLK, D), BF16),
            vmem((16, CH), BF16),
            vmem((CH, 2 * CH), BF16),
            vmem((ROWS, CH), BF16),
            vmem((ROWS, 2 * CH), F32),
            vmem((ROWS, CH), F32),
            vmem((ROWS, CH), F32),
            vmem((ROWS, CH), F32),
            vmem((1, 2 * CH), F32),
            vmem((NF - 1, 1, 2 * CH), F32),
            vmem((1, 2 * CH), F32),
            vmem((NF - 1, 1, 2 * CH), F32),
            vmem((NX * BLK, CH), BF16),
            vmem((NX * BLK, CH), BF16),
            vmem((NX * BLK, CH), BF16),
            vmem((NX * BLK, D), F32),
            vmem((BLK, D), F32),
            vmem((6, BLK, 1024), BF16),
            vmem((BLK, 1024), BF16),
            vmem((BLK, 1024), BF16),
            vmem((2, BLK, 1024), BF16),
            vmem((2, BLK, 1024), BF16),
            vmem((2, 2 * NX, BLK, 1024), BF16),
            vmem((2 * NX * BLK, 768), BF16),
            vmem((NF, 2 * NX * BLK, 256), F32),
            vmem((NF, NX * BLK, 256), BF16),
            vmem((NF, NX * BLK, 256), BF16),
            vmem((6, 4, BLK, 128), BF16),
            vmem((4, BLK, 128), BF16),
            vmem((4, BLK, 128), BF16),
            vmem((2, 4, BLK, 128), BF16),
            vmem((2, 4, BLK, 128), BF16),
            vmem((6, 3, BLK, 128), BF16),
            vmem((3, BLK, 128), BF16),
            vmem((3, BLK, 128), BF16),
            vmem((2, 3, BLK, 128), BF16),
            vmem((2, 3, BLK, 128), BF16),
            vmem((3, BLK, 256), BF16),
            vmem((3, BLK, 256), BF16),
            vmem((BLK, D), F32),
            pltpu.SemaphoreType.DMA((15,)),
            pltpu.SemaphoreType.DMA((NSEND,)),
            pltpu.SemaphoreType.DMA((NRECV,)),
        ],
        compiler_params=pltpu.CompilerParams(
            collective_id=0, has_side_effects=True, vmem_limit_bytes=58 * 1024 * 1024
        ),
        name="layer",
    )(
        resid, x_branch, gate_branch, conv_w, gate_a_w, gate_x_w, decay_rate.reshape(1, CH), decay_extra,
        w_proj, mix_gain.reshape(1, D), pre_gain.reshape(1, D), w_gate, w_up, w_down.T, out_gain.reshape(1, D),
    )


def solution(mesh):
    return jax.shard_map(
        shards,
        mesh=mesh,
        in_specs=(
            P("sp", None),
            P("sp", "tp"),
            P("sp", "tp"),
            P(None, "tp"),
            P("tp", None, None),
            P("tp", None, None),
            P("tp"),
            P("sp", "tp"),
            P("tp", None),
            P(),
            P(),
            P("sp", "tp"),
            P("sp", "tp"),
            P("tp", "sp"),
            P(),
        ),
        out_specs=P(("sp", "tp"), None),
        check_vma=False,
    )
```

```python
import functools

import jax
import jax.numpy as jnp
from jax import lax
from jax.experimental import pallas as pl
from jax.experimental.pallas import tpu as pltpu
from jax.sharding import PartitionSpec as P

LRU_SCALE = 8.0
NORM_EPS = 1e-06
MESH = pl.DeviceIdType.MESH
F32 = jnp.float32
BF16 = jnp.bfloat16

NF = 8
NX = 4
ROWS = 384
CH = 256
D = 2048
BLK = 48
HID = 704
WL = 2176
LANES = {"DA": slice(0, 768), "GA": slice(768, 1152), "GB1": slice(1152, 1664), "GB2": slice(1664, 2176)}
LA, LB = slice(0, 1152), slice(1152, WL)
GROUPS = ((0,), (1, 2), (3, 4), (5, 6), (7,))
NRECV = 111
NSEND = 21

ORDER = (
    ("GB1", 0, 0), ("GA", 0, 0), ("GB2", 0, 0), ("DA", 0, 0), ("scan1", 0, 0), ("SB", 1, 0), ("GB1", 0, 1),
    ("SA", 1, 0), ("scan2", 0, 0), ("GA", 0, 1), ("scan3", 0, 0), ("GB1", 1, 0), ("GB2", 0, 1), ("GA", 1, 0),
    ("DA", 0, 1), ("GB2", 1, 0), ("SB", 2, 0), ("GB1", 0, 2), ("SA", 2, 0), ("GA", 0, 2), ("GB1", 1, 1),
    ("GA", 1, 1), ("GA", 2, 0), ("GB1", 2, 0), ("row", 0, 0), ("DA", 0, 2), ("SB", 3, 0), ("GB1", 0, 3),
    ("GA", 1, 2), ("GB1", 1, 2), ("GA", 2, 1), ("SA", 3, 0), ("GA", 0, 3), ("GB1", 2, 1), ("GA", 3, 0),
    ("DA", 0, 3), ("GB1", 3, 0), ("SB", 4, 0), ("GB1", 0, 4), ("col", 0, 0), ("mix", 0, 0), ("GB1", 1, 3),
    ("GA", 2, 2), ("GB1", 2, 2), ("GA", 3, 1), ("SA", 4, 0), ("GA", 0, 4), ("mix2", 0, 0), ("DA", 0, 4),
    ("GB2", 0, 2), ("GA", 1, 3), ("GB1", 3, 1), ("DA", 1, 0), ("GB1", 1, 4), ("GB2", 0, 3), ("DA", 1, 1),
    ("relay", 0, 0), ("GB1", 2, 3), ("GA", 1, 4), ("GA", 3, 2), ("GB1", 3, 2), ("DA", 1, 2), ("GB2", 0, 4),
    ("GB2", 1, 1), ("GA", 2, 3), ("GB1", 2, 4), ("send", 0, 0), ("GB2", 1, 2), ("DA", 1, 3), ("GB1", 3, 3),
    ("GB2", 1, 3), ("GA", 2, 4), ("DA", 1, 4), ("GB2", 1, 4), ("DA", 2, 0), ("ag", 0, 0), ("GB2", 2, 0),
    ("GA", 3, 3), ("GB1", 3, 4), ("GB2", 2, 1), ("DA", 2, 1), ("ag2", 0, 0), ("GB2", 2, 2), ("GA", 3, 4),
    ("DA", 2, 2), ("GB2", 2, 3), ("agend", 0, 0), ("GB2", 2, 4), ("DA", 2, 3), ("GB2", 3, 0), ("agp", 0, 0),
    ("GB1", 4, 0), ("GB1", 4, 1), ("GB1", 4, 2), ("GB1", 4, 3), ("GB1", 4, 4), ("u1", 0, 0), ("GB2", 3, 1),
    ("DA", 2, 4), ("GA", 4, 0), ("GA", 4, 1), ("GA", 4, 2), ("GA", 4, 3), ("GA", 4, 4), ("u0", 0, 0), ("DA", 3, 0),
    ("GB2", 3, 2), ("e0", 0, 0), ("DA", 3, 1), ("GB2", 3, 3), ("GB2", 3, 4), ("DA", 3, 2), ("DA", 3, 3),
    ("DA", 3, 4), ("GB2", 4, 0), ("GB2", 4, 1), ("GB2", 4, 2), ("GB2", 4, 3), ("GB2", 4, 4), ("u2p", 0, 0),
    ("f0p", 0, 0), ("h0", 0, 0), ("u2o", 0, 0), ("f0o", 0, 0), ("e1", 0, 0), ("f1p", 0, 0), ("h1", 0, 0),
    ("g0s", 0, 0), ("f1o", 0, 0), ("DA", 4, 0), ("DA", 4, 1), ("DA", 4, 2), ("DA", 4, 3), ("DA", 4, 4),
    ("e2", 0, 0), ("f2p", 0, 0), ("h2", 0, 0), ("g1s", 0, 0), ("f2o", 0, 0), ("g0r", 0, 0), ("g2s", 0, 0),
    ("g1r", 0, 0),
)


def dot(a, b):
    return jnp.dot(a, b, preferred_element_type=F32)


def dot_nt(a, b):
    return lax.dot_general(a, b, (((1,), (1,)), ((), ())), preferred_element_type=F32)


def sigmoid(v):
    return 1.0 / (1.0 + jnp.exp(-v))


def gelu(v):
    inner = 0.7978845608028654 * (v + 0.044715 * (v * v * v))
    return 0.5 * v * (1.0 + jnp.tanh(inner))


def one_minus_exp(w):
    series = 1.0 + w * (1.0 / 6.0)
    for n in (5.0, 4.0, 3.0, 2.0):
        series = 1.0 + w * (1.0 / n) * series
    return jnp.where(w > -0.25, -w * series, 1.0 - jnp.exp(w))


def rms_scale(values, gains):
    mean = jnp.sum(values * values, axis=-1, keepdims=True) * (1.0 / D)
    return values * lax.rsqrt(mean + NORM_EPS) * gains


def kernel(
    resid, x_in, g_in, conv_w, ga_in, gx_in, rate, extra, wp_in, mixg, preg, wg_in, wu_in, wd_in, outg,
    out,
    W, wp, xb, xp, gb, eb, cw, ga, gx, rt, mg, pg, og, wg, wu, wd, rs_b,
    halo, bd, cout, gates, acum, bcum, geb, tot, rowbuf, rtot, colbuf,
    mixa, mixs, mixb, parts, stream, sb, rl, rr, fl, fr, nb, hid,
    parts2, psend, pbuf, sb0, rl0, rr0, fl0, fr0, sb1, rl1, rr1, fl1, fr1, sb2, rb2, ffn,
    local_sem, send_sem, recv_sem,
):
    sp = lax.axis_index("sp")
    tp = lax.axis_index("tp")
    z, y = sp // NF, sp % NF
    x, c = tp // 2, tp % 2

    def at_zy(zz, yy):
        return {"sp": zz * NF + yy, "tp": tp}

    def at_x(step):
        return {"sp": sp, "tp": ((x + step) % NX) * 2 + c}

    partner = {"sp": sp, "tp": x * 2 + (1 - c)}
    behind = {"sp": (sp + NF * NF - 1) % (NF * NF), "tp": tp}
    ahead = {"sp": (sp + 1) % (NF * NF), "tp": tp}

    barrier = pltpu.get_barrier_semaphore()
    peers = [at_zy(z, (y + k) % NF) for k in range(1, NF)]
    peers += [at_zy((z + k) % NF, y) for k in range(1, NF)]
    peers += [at_x(1), at_x(2), at_x(NX - 1), partner, behind, ahead]
    for peer in peers:
        pl.semaphore_signal(barrier, inc=1, device_id=peer, device_id_type=MESH)

    loads = {}

    def load(name, src, dst):
        copy = pltpu.make_async_copy(src, dst, local_sem.at[len(loads)])
        copy.start()
        loads[name] = copy

    load("wg", wg_in, wg)
    load("wu", wu_in, wu)
    load("wd", wd_in, wd)
    load("x", x_in, xb)
    load("ga", ga_in, ga)
    load("gx", gx_in, gx)
    load("g", g_in, gb)
    load("cw", conv_w, cw)
    load("rt", rate, rt)
    load("e", extra, eb)
    load("wp", wp_in, wp.at[0])
    load("rs", resid.at[pl.ds(pl.multiple_of(tp * BLK, 16), BLK), :], rs_b)
    load("mg", mixg, mg)
    load("pg", preg, pg)
    load("og", outg, og)

    for name in ("wg", "wu", "wd"):
        loads[name].wait()
    mine = W.at[z, y]
    mine[:, 0:640] = wd[:, 0:640]
    mine[:, 640:768] = jnp.concatenate([wd[:, 640:704], jnp.zeros((32, 64), BF16)], axis=1)
    mine[:, 768:896] = wg[:, 512:640]
    mine[:, 896:1024] = wu[:, 512:640]
    mine[:, 1024:1152] = jnp.concatenate([wg[:, 640:704], wu[:, 640:704]], axis=1)
    for n in range(2):
        mine[:, 512 * n + 1152 : 512 * n + 1408] = wg[:, 256 * n : 256 * n + 256]
        mine[:, 512 * n + 1408 : 512 * n + 1664] = wu[:, 256 * n : 256 * n + 256]

    send_ids, recv_ids = {}, {}

    def send(src, dst, device, to, out):
        copy = pltpu.make_async_remote_copy(
            src_ref=src,
            dst_ref=dst,
            send_sem=send_sem.at[send_ids.setdefault(out, len(send_ids))],
            recv_sem=recv_sem.at[recv_ids.setdefault(to, len(recv_ids))],
            device_id=device,
            device_id_type=MESH,
        )
        copy.start()

    def arrived(to, like):
        pltpu.make_async_copy(like, like, recv_sem.at[recv_ids[to]]).wait()

    def sent(out, like):
        pltpu.make_async_copy(like, like, send_sem.at[send_ids[out]]).wait()

    def mod(v):
        return (v + NF) % NF

    def piece(fam, first, second, lanes):
        return W.at[second, first, :, lanes] if fam == "A" else W.at[first, second, :, lanes]

    def some(n, lanes):
        return W.at[0, 0:n, :, lanes]

    first = {"A": y, "B": z}
    second = {"A": z, "B": y}

    def along_y(step):
        return at_zy(z, (y + step) % NF)

    def along_z(step):
        return at_zy((z + step) % NF, y)

    along_first = {"A": along_y, "B": along_z}
    along_second = {"A": along_z, "B": along_y}
    WAYS = ((1, -1), (NF - 1, 1))

    def hop1(fam, k):
        whole = LA if fam == "A" else LB
        cut = whole.start + (640 if fam == "A" else 512)
        for d, (step, sign) in enumerate(WAYS):
            lanes = whole if k < 4 else (slice(whole.start, cut) if d == 0 else slice(cut, whole.stop))
            ref = piece(fam, mod(first[fam] + sign * (k - 1)), second[fam], lanes)
            send(ref, ref, along_first[fam](step), ("S" + fam, k), "S" + fam)

    def hop1_done(fam, k):
        whole = LA if fam == "A" else LB
        arrived(("S" + fam, k), some(2 if k < 4 else 1, whole))

    def offset(j):
        return (j + 1) // 2 * (-1 if j % 2 == 1 else 1)

    def hop2(name, t, q):
        fam, lanes = name[1], LANES[name]
        for d, (step, sign) in enumerate(WAYS):
            for j in GROUPS[q]:
                if t == 4 and (j < 4) != (d == 0):
                    continue
                ref = piece(fam, mod(first[fam] + offset(j)), mod(second[fam] + sign * (t - 1)), lanes)
                send(ref, ref, along_second[fam](step), (name, t, q), name)

    def hop2_done(name, t, q):
        n = len(GROUPS[q])
        arrived((name, t, q), some(2 * n if t < 4 else n, LANES[name]))

    loads["x"].wait()
    pl.semaphore_wait(barrier, len(peers))
    send(xb.at[pl.ds(ROWS - 16, 16), :], halo, ahead, "halo", "halo")
    hop1("A", 1)
    hop1("B", 1)
    loads["wp"].wait()
    send(wp.at[0], wp.at[1], partner, "wp", "wp")
    for name in ("ga", "gx", "g", "cw", "rt", "e"):
        loads[name].wait()
    bd[...] = jnp.zeros_like(bd)
    for n in range(4):
        s = slice(64 * n, 64 * n + 64)
        bd[s, 64 * n : 64 * n + 64] = ga[n]
        bd[s, CH + 64 * n : CH + 64 * n + 64] = gx[n]
    xp[16:, :] = xb[...].astype(F32)
    geb[...] = gelu(gb[...].astype(F32))

    def scan1():
        arrived("halo", halo)
        xp[0:16, :] = jnp.where(sp > 0, halo[...].astype(F32), 0.0)
        conv = xp[13 : 13 + ROWS, :] * cw[0:1, :]
        for tap in range(1, 4):
            conv = conv + xp[13 + tap : 13 + tap + ROWS, :] * cw[tap : tap + 1, :]
        cout[...] = conv.astype(BF16)
        gates[...] = dot(cout[...], bd[...])

    held = {}

    def scan_rows(lo, hi, start):
        in_group = lax.broadcasted_iota(jnp.int32, (4, 8, CH), 1)

        def chunk(i, carry):
            rows = pl.ds(pl.multiple_of(i * 32, 32), 32)
            recur = sigmoid(gates[rows, 0:CH])
            inject = sigmoid(gates[rows, CH:])
            log_decay = (-LRU_SCALE * recur) * rt[...] + eb[rows, :]
            decay = jnp.exp(log_decay)
            grown = one_minus_exp(2.0 * log_decay)
            root = jnp.where(grown > 0.0, grown * lax.rsqrt(jnp.maximum(grown, 1e-37)), 0.0)
            drive = root * inject * cout[rows, :].astype(F32)
            a = decay.reshape(4, 8, CH)
            b = drive.reshape(4, 8, CH)
            for step in (1, 2, 4):
                keep = in_group >= step
                a_prev = jnp.where(keep, pltpu.roll(a, step, 1), 1.0)
                b_prev = jnp.where(keep, pltpu.roll(b, step, 1), 0.0)
                b = a * b_prev + b
                a = a * a_prev
            a_in, b_in = carry
            a_all, b_all = [], []
            for n in range(4):
                a_n = a[n] * a_in
                b_n = a[n] * b_in + b[n]
                a_in, b_in = a_n[7:8, :], b_n[7:8, :]
                a_all.append(a_n)
                b_all.append(b_n)
            acum[rows, :] = jnp.concatenate(a_all, axis=0)
            bcum[rows, :] = jnp.concatenate(b_all, axis=0)
            return a_in, b_in

        return lax.fori_loop(lo, hi, chunk, start)

    def scan2():
        held["half"] = scan_rows(0, 6, (jnp.ones((1, CH), F32), jnp.zeros((1, CH), F32)))

    def scan3():
        a_end, b_end = scan_rows(6, ROWS // 32, held["half"])
        tot[:, 0:CH] = a_end
        tot[:, CH:] = b_end
        for k in range(1, NF):
            send(tot, rowbuf.at[k - 1], along_y(k), "row", "row")

    def composed(own, buf, me):
        pa, pb = jnp.ones((1, CH), F32), jnp.zeros((1, CH), F32)
        ea, eb_ = pa, pb
        for place in range(NF):
            slot = (me - place + NF) % NF
            got = buf[jnp.maximum(slot - 1, 0)]
            is_me = slot == 0
            va = jnp.where(is_me, own[:, 0:CH], got[:, 0:CH])
            vb = jnp.where(is_me, own[:, CH:], got[:, CH:])
            ea = jnp.where(is_me, pa, ea)
            eb_ = jnp.where(is_me, pb, eb_)
            pa, pb = pa * va, va * pb + vb
        return (pa, pb), (ea, eb_)

    def row():
        arrived("row", rowbuf)
        (ra, rb_), held["in"] = composed(tot[...], rowbuf, y)
        rtot[:, 0:CH] = ra
        rtot[:, CH:] = rb_
        for k in range(1, NF):
            send(rtot, colbuf.at[k - 1], along_z(k), "col", "col")

    def col():
        arrived("col", colbuf)
        _, (col_a, col_b) = composed(rtot[...], colbuf, z)
        in_a, in_b = held["in"]
        held["carried"] = in_a * col_b + in_b

    def mixer_block(core, rel):
        block = ((x + rel) % NX) * 2 + core
        rows = pl.ds(pl.multiple_of(block * BLK, 16), BLK)
        return ((bcum[rows, :] + acum[rows, :] * held["carried"]) * geb[rows, :]).astype(BF16)

    def mix():
        for rel in range(NX):
            mixs[BLK * rel : BLK * rel + BLK, :] = mixer_block(1 - c, rel)
        send(mixs, mixb, partner, "mix", "mix")
        for rel in range(NX):
            mixa[BLK * rel : BLK * rel + BLK, :] = mixer_block(c, rel)
        arrived("wp", wp.at[1])
        parts[...] = dot(mixa[...], wp[0])

    def scatter_start(u, take, sbuf, bufs):
        rl_, rr_, fl_, fr_ = bufs
        for half in range(2):
            sbuf[half] = take(2, half).astype(BF16)
        send(sbuf.at[0], rl_, at_x(1), ("rl", u), ("sb", u))
        send(sbuf.at[1], rr_, at_x(NX - 1), ("rr", u), ("sb", u))
        sbuf[2] = take(1, 1).astype(BF16)
        send(sbuf.at[2], fl_.at[1], at_x(1), ("f", u), ("sb", u))
        sbuf[3] = take(3, 0).astype(BF16)
        send(sbuf.at[3], fr_.at[0], at_x(NX - 1), ("f", u), ("sb", u))

    def scatter_relay(u, take, sbuf, bufs):
        rl_, rr_, fl_, fr_ = bufs
        arrived(("rl", u), rl_)
        sbuf[4] = (take(1, 0) + rl_[...].astype(F32)).astype(BF16)
        send(sbuf.at[4], fl_.at[0], at_x(1), ("f", u), ("sb", u))
        arrived(("rr", u), rr_)
        sbuf[5] = (take(3, 1) + rr_[...].astype(F32)).astype(BF16)
        send(sbuf.at[5], fr_.at[1], at_x(NX - 1), ("f", u), ("sb", u))

    bufs = (rl, rr, fl, fr)

    def take(rel, half):
        return parts[BLK * rel : BLK * rel + BLK, 1024 * half : 1024 * half + 1024]

    def mix2():
        arrived("mix", mixb)
        parts[...] += dot(mixb[...], wp[1])
        scatter_start(0, take, sb, bufs)

    def relay():
        scatter_relay(0, take, sb, bufs)

    def norm_and_send():
        arrived(("f", 0), sb.at[0:4])
        for name in ("rs", "mg", "pg", "og"):
            loads[name].wait()
        halves = [take(0, half) + fl[half].astype(F32) + fr[half].astype(F32) for half in range(2)]
        mixed = jnp.concatenate(halves, axis=1)
        after_mix = rs_b[...].astype(F32) + rms_scale(mixed, mg[...])
        stream[...] = after_mix
        normed = rms_scale(after_mix, pg[...]).astype(BF16)
        nb[0, 0] = normed[:, 0:1024]
        nb[1, 0] = normed[:, 1024:]
        send(nb.at[0, 0], nb.at[0, 3], at_x(1), "al", "nb")
        send(nb.at[1, 0], nb.at[1, 1], at_x(NX - 1), "ar", "nb")
        send(nb.at[1, 0], nb.at[1, 3], at_x(1), "an", "nb")
        send(nb.at[0, 0], nb.at[0, 1], at_x(NX - 1), "an", "nb")
        for half in range(2):
            to_partner(half, 0)

    def to_partner(half, rel):
        send(nb.at[half, rel], nb.at[half, NX + rel], partner, "nbp", "nbp")

    def ag():
        arrived("al", nb.at[0, 3])
        send(nb.at[0, 3], nb.at[0, 2], at_x(1), "ab", "nb")
        to_partner(0, 3)
        arrived("ar", nb.at[1, 1])
        send(nb.at[1, 1], nb.at[1, 2], at_x(NX - 1), "ab", "nb")
        to_partner(1, 1)

    def ag2():
        arrived("an", nb.at[0, 0:2])
        to_partner(1, 3)
        to_partner(0, 1)

    def agend():
        arrived("ab", nb.at[0, 0:2])
        to_partner(0, 2)
        to_partner(1, 2)

    def agp():
        arrived("nbp", nb.at[0])

    HALF = NX * BLK
    mine_rows, other_rows, all_rows = slice(0, HALF), slice(HALF, 2 * HALF), slice(0, 2 * HALF)

    def gate_up(n, span):
        w = W[:, :, :, LANES[("GA", "GB1", "GB2")[n]]]
        w = w.reshape(D, w.shape[-1])
        rows = span.stop - span.start
        at = slice(span.start // BLK, span.stop // BLK)
        both = dot(nb[0, at].reshape(rows, 1024), w[0:1024]) + dot(nb[1, at].reshape(rows, 1024), w[1024:])
        if n > 0:
            g, u = both[:, 0:256], both[:, 256:512]
            hid[span, 256 * n - 256 : 256 * n] = (g * sigmoid(g) * u).astype(BF16)
        else:
            g, u = both[:, 0:128], both[:, 128:256]
            hid[span, 512:640] = (g * sigmoid(g) * u).astype(BF16)
            g = both[:, 256:384]
            u = pltpu.roll(g, 64, 1)
            lane = lax.broadcasted_iota(jnp.int32, g.shape, 1)
            hid[span, 640:768] = jnp.where(lane < 64, g * sigmoid(g) * u, 0.0).astype(BF16)

    def place(i):
        return (z + NF + (i + 1) // 2 * (1 - 2 * (i % 2))) % NF

    def down(i, rows, lanes):
        w = W[place(i), :, :, lanes]
        return dot_nt(hid[rows, lanes], w.reshape(256, lanes.stop - lanes.start))

    def down_first(lo, hi):
        for i in range(lo, hi):
            parts2[i] = down(i, all_rows, slice(0, 256)) + down(i, all_rows, slice(512, 768))

    def down_last(u, rows):
        for i in range(*SPANS[u]):
            parts2[i, rows] += down(i, rows, slice(256, 512))

    SPANS = ((0, 4), (4, 7), (7, 8))

    def pair_start(u):
        span = slice(*SPANS[u])
        psend[span] = parts2[span, other_rows, :].astype(BF16)
        send(psend.at[span], pbuf.at[span], partner, ("h", u), ("h", u))

    def pair_end(u):
        span = slice(*SPANS[u])
        arrived(("h", u), pbuf.at[span])
        parts2[span, mine_rows, :] += pbuf[span].astype(F32)

    bufs0 = (rl0, rr0, fl0, fr0)
    bufs1 = (rl1, rr1, fl1, fr1)

    def take0(rel, half):
        return parts2[0:4, BLK * rel : BLK * rel + BLK, 128 * half : 128 * half + 128]

    def take1(rel, half):
        return parts2[4:7, BLK * rel : BLK * rel + BLK, 128 * half : 128 * half + 128]

    def g0s():
        pair_end(0)
        scatter_start(1, take0, sb0, bufs0)

    def g0r():
        scatter_relay(1, take0, sb0, bufs0)

    def g1s():
        pair_end(1)
        scatter_start(2, take1, sb1, bufs1)

    def g1r():
        scatter_relay(2, take1, sb1, bufs1)

    def g2s():
        pair_end(2)
        for k, (rel, step) in enumerate(((2, 2), (1, 1), (3, NX - 1))):
            sb2[k] = parts2[7, BLK * rel : BLK * rel + BLK, :].astype(BF16)
            send(sb2.at[k], rb2.at[k], at_x(step), "d", "d")

    steps = {
        "scan1": scan1, "scan2": scan2, "scan3": scan3, "row": row, "col": col, "mix": mix, "mix2": mix2,
        "relay": relay, "send": norm_and_send, "ag": ag, "agend": agend, "g0s": g0s, "g0r": g0r, "g1s": g1s,
        "g1r": g1r, "g2s": g2s, "agp": agp, "ag2": ag2,
    }
    for n in range(2):
        steps["u%d" % n] = functools.partial(gate_up, n, all_rows)
    for n, span in enumerate(((0, 5), (5, 7), (7, 8))):
        steps["e%d" % n] = functools.partial(down_first, *span)
        steps["h%d" % n] = functools.partial(pair_start, n)
    for name, rows in (("p", other_rows), ("o", mine_rows)):
        steps["u2" + name] = functools.partial(gate_up, 2, rows)
        for n in range(3):
            steps["f%d" % n + name] = functools.partial(down_last, n, rows)

    for name, t, q in ORDER:
        if name in steps:
            steps[name]()
        elif name[0] == "S":
            fam = name[1]
            hop1_done(fam, t)
            if t < 4:
                hop1(fam, t + 1)
        else:
            if t > 0:
                hop2_done(name, t, q)
            if t < 4:
                hop2(name, t + 1, q)

    def put(i, lane, value):
        ffn[:, pl.ds(pl.multiple_of(place(i) * 256 + lane, 128), value.shape[-1])] = value

    for u, lo, hi, take_, sbuf, (_, _, fl_, fr_) in ((1, 0, 4, take0, sb0, bufs0), (2, 4, 7, take1, sb1, bufs1)):
        arrived(("f", u), sbuf.at[0:4])
        for half in range(2):
            got = take_(0, half) + fl_[half].astype(F32) + fr_[half].astype(F32)
            for i in range(lo, hi):
                put(i, 128 * half, got[i - lo])
    arrived("d", rb2)
    put(7, 0, parts2[7, 0:BLK, :] + sum(rb2[k].astype(F32) for k in range(3)))
    out[...] = (stream[...] + 0.5 * rms_scale(ffn[...], og[...])).astype(BF16)

    for fam, lanes in (("A", LA), ("B", LB)):
        sent("S" + fam, W.at[0, 0:7, :, lanes])
    for name in LANES:
        sent(name, W.at[0:7, :, :, LANES[name]])
    for u, span in enumerate(SPANS):
        sent(("h", u), psend.at[slice(*span)])
    for out_, ref in (
        ("halo", halo), ("wp", wp.at[1]), ("row", rowbuf), ("col", colbuf), ("mix", mixb), (("sb", 0), sb),
        ("nb", sb), ("nbp", nb.at[0]), (("sb", 1), sb0), (("sb", 2), sb1), ("d", sb2),
    ):
        sent(out_, ref)
    assert len(recv_ids) <= NRECV and len(send_ids) <= NSEND, (len(recv_ids), len(send_ids))


def shards(
    resid, x_branch, gate_branch, conv_w, gate_a_w, gate_x_w, decay_rate, decay_extra, w_proj, mix_gain,
    pre_gain, w_gate, w_up, w_down, out_gain,
):
    vmem = pltpu.VMEM
    return pl.pallas_call(
        kernel,
        out_shape=jax.ShapeDtypeStruct((BLK, D), BF16),
        in_specs=[pl.BlockSpec(memory_space=pl.ANY)] * 15,
        out_specs=pl.BlockSpec(memory_space=pltpu.VMEM),
        scratch_shapes=[
            vmem((NF, NF, 32, WL), BF16),
            vmem((2, CH, D), BF16),
            vmem((ROWS, CH), BF16),
            vmem((ROWS + 16, CH), F32),
            vmem((ROWS, CH), BF16),
            vmem((ROWS, CH), F32),
            vmem((4, CH), F32),
            vmem((4, 64, 64), BF16),
            vmem((4, 64, 64), BF16),
            vmem((1, CH), F32),
            vmem((1, D), F32),
            vmem((1, D), F32),
            vmem((1, D), F32),
            vmem((32, HID), BF16),
            vmem((32, HID), BF16),
            vmem((32, HID), BF16),
            vmem((BLK, D), BF16),
            vmem((16, CH), BF16),
            vmem((CH, 2 * CH), BF16),
            vmem((ROWS, CH), BF16),
            vmem((ROWS, 2 * CH), F32),
            vmem((ROWS, CH), F32),
            vmem((ROWS, CH), F32),
            vmem((ROWS, CH), F32),
            vmem((1, 2 * CH), F32),
            vmem((NF - 1, 1, 2 * CH), F32),
            vmem((1, 2 * CH), F32),
            vmem((NF - 1, 1, 2 * CH), F32),
            vmem((NX * BLK, CH), BF16),
            vmem((NX * BLK, CH), BF16),
            vmem((NX * BLK, CH), BF16),
            vmem((NX * BLK, D), F32),
            vmem((BLK, D), F32),
            vmem((6, BLK, 1024), BF16),
            vmem((BLK, 1024), BF16),
            vmem((BLK, 1024), BF16),
            vmem((2, BLK, 1024), BF16),
            vmem((2, BLK, 1024), BF16),
            vmem((2, 2 * NX, BLK, 1024), BF16),
            vmem((2 * NX * BLK, 768), BF16),
            vmem((NF, 2 * NX * BLK, 256), F32),
            vmem((NF, NX * BLK, 256), BF16),
            vmem((NF, NX * BLK, 256), BF16),
            vmem((6, 4, BLK, 128), BF16),
            vmem((4, BLK, 128), BF16),
            vmem((4, BLK, 128), BF16),
            vmem((2, 4, BLK, 128), BF16),
            vmem((2, 4, BLK, 128), BF16),
            vmem((6, 3, BLK, 128), BF16),
            vmem((3, BLK, 128), BF16),
            vmem((3, BLK, 128), BF16),
            vmem((2, 3, BLK, 128), BF16),
            vmem((2, 3, BLK, 128), BF16),
            vmem((3, BLK, 256), BF16),
            vmem((3, BLK, 256), BF16),
            vmem((BLK, D), F32),
            pltpu.SemaphoreType.DMA((15,)),
            pltpu.SemaphoreType.DMA((NSEND,)),
            pltpu.SemaphoreType.DMA((NRECV,)),
        ],
        compiler_params=pltpu.CompilerParams(
            collective_id=0, has_side_effects=True, vmem_limit_bytes=58 * 1024 * 1024
        ),
        name="layer",
    )(
        resid, x_branch, gate_branch, conv_w, gate_a_w, gate_x_w, decay_rate.reshape(1, CH), decay_extra,
        w_proj, mix_gain.reshape(1, D), pre_gain.reshape(1, D), w_gate, w_up, w_down.T, out_gain.reshape(1, D),
    )


def solution(mesh):
    return jax.shard_map(
        shards,
        mesh=mesh,
        in_specs=(
            P("sp", None),
            P("sp", "tp"),
            P("sp", "tp"),
            P(None, "tp"),
            P("tp", None, None),
            P("tp", None, None),
            P("tp"),
            P("sp", "tp"),
            P("tp", None),
            P(),
            P(),
            P("sp", "tp"),
            P("sp", "tp"),
            P("tp", "sp"),
            P(),
        ),
        out_specs=P(("sp", "tp"), None),
        check_vma=False,
    )
```

```python
import functools

import jax
import jax.numpy as jnp
from jax import lax
from jax.experimental import pallas as pl
from jax.experimental.pallas import tpu as pltpu
from jax.sharding import PartitionSpec as P

LRU_SCALE = 8.0
NORM_EPS = 1e-06
MESH = pl.DeviceIdType.MESH
F32 = jnp.float32
BF16 = jnp.bfloat16

NF = 8
NX = 4
ROWS = 384
CH = 256
D = 2048
BLK = 48
HID = 704
WL = 2176
LANES = {"DA": slice(0, 768), "GA": slice(768, 1152), "GB1": slice(1152, 1664), "GB2": slice(1664, 2176)}
LA, LB = slice(0, 1152), slice(1152, WL)
GROUPS = ((0,), (1, 2), (3, 4), (5, 6), (7,))
NRECV = 111
NSEND = 21

ORDER = (
    ("GB1", 0, 0), ("GA", 0, 0), ("GB2", 0, 0), ("DA", 0, 0), ("scan1", 0, 0), ("SB", 1, 0), ("GB1", 0, 1),
    ("SA", 1, 0), ("scan2", 0, 0), ("GA", 0, 1), ("scan3", 0, 0), ("GB1", 1, 0), ("GB2", 0, 1), ("GA", 1, 0),
    ("DA", 0, 1), ("GB2", 1, 0), ("SB", 2, 0), ("GB1", 0, 2), ("SA", 2, 0), ("GA", 0, 2), ("GB1", 1, 1),
    ("GA", 1, 1), ("GA", 2, 0), ("GB1", 2, 0), ("row", 0, 0), ("DA", 0, 2), ("SB", 3, 0), ("GB1", 0, 3),
    ("GA", 1, 2), ("GB1", 1, 2), ("GA", 2, 1), ("SA", 3, 0), ("GA", 0, 3), ("GB1", 2, 1), ("GA", 3, 0),
    ("DA", 0, 3), ("GB1", 3, 0), ("SB", 4, 0), ("GB1", 0, 4), ("col", 0, 0), ("mix", 0, 0), ("GB1", 1, 3),
    ("GA", 2, 2), ("GB1", 2, 2), ("GA", 3, 1), ("SA", 4, 0), ("GA", 0, 4), ("mix2", 0, 0), ("DA", 0, 4),
    ("GB2", 0, 2), ("GA", 1, 3), ("GB1", 3, 1), ("DA", 1, 0), ("GB1", 1, 4), ("GB2", 0, 3), ("DA", 1, 1),
    ("relay", 0, 0), ("GB1", 2, 3), ("GA", 1, 4), ("GA", 3, 2), ("GB1", 3, 2), ("DA", 1, 2), ("GB2", 0, 4),
    ("GB2", 1, 1), ("GA", 2, 3), ("GB1", 2, 4), ("send", 0, 0), ("GB2", 1, 2), ("DA", 1, 3), ("GB1", 3, 3),
    ("GB2", 1, 3), ("GA", 2, 4), ("DA", 1, 4), ("GB2", 1, 4), ("DA", 2, 0), ("ag", 0, 0), ("GB2", 2, 0),
    ("GA", 3, 3), ("GB1", 3, 4), ("GB2", 2, 1), ("DA", 2, 1), ("ag2", 0, 0), ("GB2", 2, 2), ("GA", 3, 4),
    ("DA", 2, 2), ("GB2", 2, 3), ("agend", 0, 0), ("GB2", 2, 4), ("DA", 2, 3), ("GB2", 3, 0), ("agp", 0, 0),
    ("GB1", 4, 0), ("GB1", 4, 1), ("GB1", 4, 2), ("GB1", 4, 3), ("GB1", 4, 4), ("u1", 0, 0), ("GB2", 3, 1),
    ("DA", 2, 4), ("GA", 4, 0), ("GA", 4, 1), ("GA", 4, 2), ("GA", 4, 3), ("GA", 4, 4), ("u0", 0, 0), ("DA", 3, 0),
    ("GB2", 3, 2), ("e0", 0, 0), ("DA", 3, 1), ("GB2", 3, 3), ("GB2", 3, 4), ("DA", 3, 2), ("DA", 3, 3),
    ("DA", 3, 4), ("GB2", 4, 0), ("GB2", 4, 1), ("GB2", 4, 2), ("GB2", 4, 3), ("GB2", 4, 4), ("u2p", 0, 0),
    ("f0p", 0, 0), ("h0", 0, 0), ("e1", 0, 0), ("f1p", 0, 0), ("h1", 0, 0), ("u2o", 0, 0), ("f0o", 0, 0),
    ("f1o", 0, 0), ("g0s", 0, 0), ("DA", 4, 0), ("DA", 4, 1), ("DA", 4, 2), ("DA", 4, 3), ("DA", 4, 4),
    ("e2", 0, 0), ("f2p", 0, 0), ("h2", 0, 0), ("g1s", 0, 0), ("f2o", 0, 0), ("g0r", 0, 0), ("g2s", 0, 0),
    ("g1r", 0, 0),
)


def dot(a, b):
    return jnp.dot(a, b, preferred_element_type=F32)


def dot_nt(a, b):
    return lax.dot_general(a, b, (((1,), (1,)), ((), ())), preferred_element_type=F32)


def sigmoid(v):
    return 1.0 / (1.0 + jnp.exp(-v))


def gelu(v):
    inner = 0.7978845608028654 * (v + 0.044715 * (v * v * v))
    return 0.5 * v * (1.0 + jnp.tanh(inner))


def one_minus_exp(w):
    series = 1.0 + w * (1.0 / 6.0)
    for n in (5.0, 4.0, 3.0, 2.0):
        series = 1.0 + w * (1.0 / n) * series
    return jnp.where(w > -0.25, -w * series, 1.0 - jnp.exp(w))


def rms_scale(values, gains):
    mean = jnp.sum(values * values, axis=-1, keepdims=True) * (1.0 / D)
    return values * lax.rsqrt(mean + NORM_EPS) * gains


def kernel(
    resid, x_in, g_in, conv_w, ga_in, gx_in, rate, extra, wp_in, mixg, preg, wg_in, wu_in, wd_in, outg,
    out,
    W, wp, xb, xp, gb, eb, cw, ga, gx, rt, mg, pg, og, wg, wu, wd, rs_b,
    halo, bd, cout, gates, acum, bcum, geb, tot, rowbuf, rtot, colbuf,
    mixa, mixs, mixb, parts, stream, sb, rl, rr, fl, fr, nb, hid,
    parts2, psend, pbuf, sb0, rl0, rr0, fl0, fr0, sb1, rl1, rr1, fl1, fr1, sb2, rb2, ffn,
    local_sem, send_sem, recv_sem,
):
    sp = lax.axis_index("sp")
    tp = lax.axis_index("tp")
    z, y = sp // NF, sp % NF
    x, c = tp // 2, tp % 2

    def at_zy(zz, yy):
        return {"sp": zz * NF + yy, "tp": tp}

    def at_x(step):
        return {"sp": sp, "tp": ((x + step) % NX) * 2 + c}

    partner = {"sp": sp, "tp": x * 2 + (1 - c)}
    behind = {"sp": (sp + NF * NF - 1) % (NF * NF), "tp": tp}
    ahead = {"sp": (sp + 1) % (NF * NF), "tp": tp}

    barrier = pltpu.get_barrier_semaphore()
    peers = [at_zy(z, (y + k) % NF) for k in range(1, NF)]
    peers += [at_zy((z + k) % NF, y) for k in range(1, NF)]
    peers += [at_x(1), at_x(2), at_x(NX - 1), partner, behind, ahead]
    for peer in peers:
        pl.semaphore_signal(barrier, inc=1, device_id=peer, device_id_type=MESH)

    loads = {}

    def load(name, src, dst):
        copy = pltpu.make_async_copy(src, dst, local_sem.at[len(loads)])
        copy.start()
        loads[name] = copy

    load("wg", wg_in, wg)
    load("wu", wu_in, wu)
    load("wd", wd_in, wd)
    load("x", x_in, xb)
    load("ga", ga_in, ga)
    load("gx", gx_in, gx)
    load("g", g_in, gb)
    load("cw", conv_w, cw)
    load("rt", rate, rt)
    load("e", extra, eb)
    load("wp", wp_in, wp.at[0])
    load("rs", resid.at[pl.ds(pl.multiple_of(tp * BLK, 16), BLK), :], rs_b)
    load("mg", mixg, mg)
    load("pg", preg, pg)
    load("og", outg, og)

    for name in ("wg", "wu", "wd"):
        loads[name].wait()
    mine = W.at[z, y]
    mine[:, 0:640] = wd[:, 0:640]
    mine[:, 640:768] = jnp.concatenate([wd[:, 640:704], jnp.zeros((32, 64), BF16)], axis=1)
    mine[:, 768:896] = wg[:, 512:640]
    mine[:, 896:1024] = wu[:, 512:640]
    mine[:, 1024:1152] = jnp.concatenate([wg[:, 640:704], wu[:, 640:704]], axis=1)
    for n in range(2):
        mine[:, 512 * n + 1152 : 512 * n + 1408] = wg[:, 256 * n : 256 * n + 256]
        mine[:, 512 * n + 1408 : 512 * n + 1664] = wu[:, 256 * n : 256 * n + 256]

    send_ids, recv_ids = {}, {}

    def send(src, dst, device, to, out):
        copy = pltpu.make_async_remote_copy(
            src_ref=src,
            dst_ref=dst,
            send_sem=send_sem.at[send_ids.setdefault(out, len(send_ids))],
            recv_sem=recv_sem.at[recv_ids.setdefault(to, len(recv_ids))],
            device_id=device,
            device_id_type=MESH,
        )
        copy.start()

    def arrived(to, like):
        pltpu.make_async_copy(like, like, recv_sem.at[recv_ids[to]]).wait()

    def sent(out, like):
        pltpu.make_async_copy(like, like, send_sem.at[send_ids[out]]).wait()

    def mod(v):
        return (v + NF) % NF

    def piece(fam, first, second, lanes):
        return W.at[second, first, :, lanes] if fam == "A" else W.at[first, second, :, lanes]

    def some(n, lanes):
        return W.at[0, 0:n, :, lanes]

    first = {"A": y, "B": z}
    second = {"A": z, "B": y}

    def along_y(step):
        return at_zy(z, (y + step) % NF)

    def along_z(step):
        return at_zy((z + step) % NF, y)

    along_first = {"A": along_y, "B": along_z}
    along_second = {"A": along_z, "B": along_y}
    WAYS = ((1, -1), (NF - 1, 1))

    def hop1(fam, k):
        whole = LA if fam == "A" else LB
        cut = whole.start + (640 if fam == "A" else 512)
        for d, (step, sign) in enumerate(WAYS):
            lanes = whole if k < 4 else (slice(whole.start, cut) if d == 0 else slice(cut, whole.stop))
            ref = piece(fam, mod(first[fam] + sign * (k - 1)), second[fam], lanes)
            send(ref, ref, along_first[fam](step), ("S" + fam, k), "S" + fam)

    def hop1_done(fam, k):
        whole = LA if fam == "A" else LB
        arrived(("S" + fam, k), some(2 if k < 4 else 1, whole))

    def offset(j):
        return (j + 1) // 2 * (-1 if j % 2 == 1 else 1)

    def hop2(name, t, q):
        fam, lanes = name[1], LANES[name]
        for d, (step, sign) in enumerate(WAYS):
            for j in GROUPS[q]:
                if t == 4 and (j < 4) != (d == 0):
                    continue
                ref = piece(fam, mod(first[fam] + offset(j)), mod(second[fam] + sign * (t - 1)), lanes)
                send(ref, ref, along_second[fam](step), (name, t, q), name)

    def hop2_done(name, t, q):
        n = len(GROUPS[q])
        arrived((name, t, q), some(2 * n if t < 4 else n, LANES[name]))

    loads["x"].wait()
    pl.semaphore_wait(barrier, len(peers))
    send(xb.at[pl.ds(ROWS - 16, 16), :], halo, ahead, "halo", "halo")
    hop1("A", 1)
    hop1("B", 1)
    loads["wp"].wait()
    send(wp.at[0], wp.at[1], partner, "wp", "wp")
    for name in ("ga", "gx", "g", "cw", "rt", "e"):
        loads[name].wait()
    bd[...] = jnp.zeros_like(bd)
    for n in range(4):
        s = slice(64 * n, 64 * n + 64)
        bd[s, 64 * n : 64 * n + 64] = ga[n]
        bd[s, CH + 64 * n : CH + 64 * n + 64] = gx[n]
    xp[16:, :] = xb[...].astype(F32)
    geb[...] = gelu(gb[...].astype(F32))

    def scan1():
        arrived("halo", halo)
        xp[0:16, :] = jnp.where(sp > 0, halo[...].astype(F32), 0.0)
        conv = xp[13 : 13 + ROWS, :] * cw[0:1, :]
        for tap in range(1, 4):
            conv = conv + xp[13 + tap : 13 + tap + ROWS, :] * cw[tap : tap + 1, :]
        cout[...] = conv.astype(BF16)
        gates[...] = dot(cout[...], bd[...])

    held = {}

    def scan_rows(lo, hi, start):
        in_group = lax.broadcasted_iota(jnp.int32, (4, 8, CH), 1)

        def chunk(i, carry):
            rows = pl.ds(pl.multiple_of(i * 32, 32), 32)
            recur = sigmoid(gates[rows, 0:CH])
            inject = sigmoid(gates[rows, CH:])
            log_decay = (-LRU_SCALE * recur) * rt[...] + eb[rows, :]
            decay = jnp.exp(log_decay)
            grown = one_minus_exp(2.0 * log_decay)
            root = jnp.where(grown > 0.0, grown * lax.rsqrt(jnp.maximum(grown, 1e-37)), 0.0)
            drive = root * inject * cout[rows, :].astype(F32)
            a = decay.reshape(4, 8, CH)
            b = drive.reshape(4, 8, CH)
            for step in (1, 2, 4):
                keep = in_group >= step
                a_prev = jnp.where(keep, pltpu.roll(a, step, 1), 1.0)
                b_prev = jnp.where(keep, pltpu.roll(b, step, 1), 0.0)
                b = a * b_prev + b
                a = a * a_prev
            a_in, b_in = carry
            a_all, b_all = [], []
            for n in range(4):
                a_n = a[n] * a_in
                b_n = a[n] * b_in + b[n]
                a_in, b_in = a_n[7:8, :], b_n[7:8, :]
                a_all.append(a_n)
                b_all.append(b_n)
            acum[rows, :] = jnp.concatenate(a_all, axis=0)
            bcum[rows, :] = jnp.concatenate(b_all, axis=0)
            return a_in, b_in

        return lax.fori_loop(lo, hi, chunk, start)

    def scan2():
        held["half"] = scan_rows(0, 6, (jnp.ones((1, CH), F32), jnp.zeros((1, CH), F32)))

    def scan3():
        a_end, b_end = scan_rows(6, ROWS // 32, held["half"])
        tot[:, 0:CH] = a_end
        tot[:, CH:] = b_end
        for k in range(1, NF):
            send(tot, rowbuf.at[k - 1], along_y(k), "row", "row")

    def composed(own, buf, me):
        pa, pb = jnp.ones((1, CH), F32), jnp.zeros((1, CH), F32)
        ea, eb_ = pa, pb
        for place in range(NF):
            slot = (me - place + NF) % NF
            got = buf[jnp.maximum(slot - 1, 0)]
            is_me = slot == 0
            va = jnp.where(is_me, own[:, 0:CH], got[:, 0:CH])
            vb = jnp.where(is_me, own[:, CH:], got[:, CH:])
            ea = jnp.where(is_me, pa, ea)
            eb_ = jnp.where(is_me, pb, eb_)
            pa, pb = pa * va, va * pb + vb
        return (pa, pb), (ea, eb_)

    def row():
        arrived("row", rowbuf)
        (ra, rb_), held["in"] = composed(tot[...], rowbuf, y)
        rtot[:, 0:CH] = ra
        rtot[:, CH:] = rb_
        for k in range(1, NF):
            send(rtot, colbuf.at[k - 1], along_z(k), "col", "col")

    def col():
        arrived("col", colbuf)
        _, (col_a, col_b) = composed(rtot[...], colbuf, z)
        in_a, in_b = held["in"]
        held["carried"] = in_a * col_b + in_b

    def mixer_block(core, rel):
        block = ((x + rel) % NX) * 2 + core
        rows = pl.ds(pl.multiple_of(block * BLK, 16), BLK)
        return ((bcum[rows, :] + acum[rows, :] * held["carried"]) * geb[rows, :]).astype(BF16)

    def mix():
        for rel in range(NX):
            mixs[BLK * rel : BLK * rel + BLK, :] = mixer_block(1 - c, rel)
        send(mixs, mixb, partner, "mix", "mix")
        for rel in range(NX):
            mixa[BLK * rel : BLK * rel + BLK, :] = mixer_block(c, rel)
        arrived("wp", wp.at[1])
        parts[...] = dot(mixa[...], wp[0])

    def scatter_start(u, take, sbuf, bufs):
        rl_, rr_, fl_, fr_ = bufs
        for half in range(2):
            sbuf[half] = take(2, half).astype(BF16)
        send(sbuf.at[0], rl_, at_x(1), ("rl", u), ("sb", u))
        send(sbuf.at[1], rr_, at_x(NX - 1), ("rr", u), ("sb", u))
        sbuf[2] = take(1, 1).astype(BF16)
        send(sbuf.at[2], fl_.at[1], at_x(1), ("f", u), ("sb", u))
        sbuf[3] = take(3, 0).astype(BF16)
        send(sbuf.at[3], fr_.at[0], at_x(NX - 1), ("f", u), ("sb", u))

    def scatter_relay(u, take, sbuf, bufs):
        rl_, rr_, fl_, fr_ = bufs
        arrived(("rl", u), rl_)
        sbuf[4] = (take(1, 0) + rl_[...].astype(F32)).astype(BF16)
        send(sbuf.at[4], fl_.at[0], at_x(1), ("f", u), ("sb", u))
        arrived(("rr", u), rr_)
        sbuf[5] = (take(3, 1) + rr_[...].astype(F32)).astype(BF16)
        send(sbuf.at[5], fr_.at[1], at_x(NX - 1), ("f", u), ("sb", u))

    bufs = (rl, rr, fl, fr)

    def take(rel, half):
        return parts[BLK * rel : BLK * rel + BLK, 1024 * half : 1024 * half + 1024]

    def mix2():
        arrived("mix", mixb)
        parts[...] += dot(mixb[...], wp[1])
        scatter_start(0, take, sb, bufs)

    def relay():
        scatter_relay(0, take, sb, bufs)

    def norm_and_send():
        arrived(("f", 0), sb.at[0:4])
        for name in ("rs", "mg", "pg", "og"):
            loads[name].wait()
        halves = [take(0, half) + fl[half].astype(F32) + fr[half].astype(F32) for half in range(2)]
        mixed = jnp.concatenate(halves, axis=1)
        after_mix = rs_b[...].astype(F32) + rms_scale(mixed, mg[...])
        stream[...] = after_mix
        normed = rms_scale(after_mix, pg[...]).astype(BF16)
        nb[0, 0] = normed[:, 0:1024]
        nb[1, 0] = normed[:, 1024:]
        send(nb.at[0, 0], nb.at[0, 3], at_x(1), "al", "nb")
        send(nb.at[1, 0], nb.at[1, 1], at_x(NX - 1), "ar", "nb")
        send(nb.at[1, 0], nb.at[1, 3], at_x(1), "an", "nb")
        send(nb.at[0, 0], nb.at[0, 1], at_x(NX - 1), "an", "nb")
        for half in range(2):
            to_partner(half, 0)

    def to_partner(half, rel):
        send(nb.at[half, rel], nb.at[half, NX + rel], partner, "nbp", "nbp")

    def ag():
        arrived("al", nb.at[0, 3])
        send(nb.at[0, 3], nb.at[0, 2], at_x(1), "ab", "nb")
        to_partner(0, 3)
        arrived("ar", nb.at[1, 1])
        send(nb.at[1, 1], nb.at[1, 2], at_x(NX - 1), "ab", "nb")
        to_partner(1, 1)

    def ag2():
        arrived("an", nb.at[0, 0:2])
        to_partner(1, 3)
        to_partner(0, 1)

    def agend():
        arrived("ab", nb.at[0, 0:2])
        to_partner(0, 2)
        to_partner(1, 2)

    def agp():
        arrived("nbp", nb.at[0])

    HALF = NX * BLK
    mine_rows, other_rows, all_rows = slice(0, HALF), slice(HALF, 2 * HALF), slice(0, 2 * HALF)

    def gate_up(n, span):
        w = W[:, :, :, LANES[("GA", "GB1", "GB2")[n]]]
        w = w.reshape(D, w.shape[-1])
        rows = span.stop - span.start
        at = slice(span.start // BLK, span.stop // BLK)
        both = dot(nb[0, at].reshape(rows, 1024), w[0:1024]) + dot(nb[1, at].reshape(rows, 1024), w[1024:])
        if n > 0:
            g, u = both[:, 0:256], both[:, 256:512]
            hid[span, 256 * n - 256 : 256 * n] = (g * sigmoid(g) * u).astype(BF16)
        else:
            g, u = both[:, 0:128], both[:, 128:256]
            hid[span, 512:640] = (g * sigmoid(g) * u).astype(BF16)
            g = both[:, 256:384]
            u = pltpu.roll(g, 64, 1)
            lane = lax.broadcasted_iota(jnp.int32, g.shape, 1)
            hid[span, 640:768] = jnp.where(lane < 64, g * sigmoid(g) * u, 0.0).astype(BF16)

    def place(i):
        return (z + NF + (i + 1) // 2 * (1 - 2 * (i % 2))) % NF

    def down(i, rows, lanes):
        w = W[place(i), :, :, lanes]
        return dot_nt(hid[rows, lanes], w.reshape(256, lanes.stop - lanes.start))

    def down_first(lo, hi):
        for i in range(lo, hi):
            parts2[i] = down(i, all_rows, slice(0, 256)) + down(i, all_rows, slice(512, 768))

    def down_last(u, rows):
        for i in range(*SPANS[u]):
            parts2[i, rows] += down(i, rows, slice(256, 512))

    SPANS = ((0, 4), (4, 7), (7, 8))

    def pair_start(u):
        span = slice(*SPANS[u])
        psend[span] = parts2[span, other_rows, :].astype(BF16)
        send(psend.at[span], pbuf.at[span], partner, ("h", u), ("h", u))

    def pair_end(u):
        span = slice(*SPANS[u])
        arrived(("h", u), pbuf.at[span])
        parts2[span, mine_rows, :] += pbuf[span].astype(F32)

    bufs0 = (rl0, rr0, fl0, fr0)
    bufs1 = (rl1, rr1, fl1, fr1)

    def take0(rel, half):
        return parts2[0:4, BLK * rel : BLK * rel + BLK, 128 * half : 128 * half + 128]

    def take1(rel, half):
        return parts2[4:7, BLK * rel : BLK * rel + BLK, 128 * half : 128 * half + 128]

    def g0s():
        pair_end(0)
        scatter_start(1, take0, sb0, bufs0)

    def g0r():
        scatter_relay(1, take0, sb0, bufs0)

    def g1s():
        pair_end(1)
        scatter_start(2, take1, sb1, bufs1)

    def g1r():
        scatter_relay(2, take1, sb1, bufs1)

    def g2s():
        pair_end(2)
        for k, (rel, step) in enumerate(((2, 2), (1, 1), (3, NX - 1))):
            sb2[k] = parts2[7, BLK * rel : BLK * rel + BLK, :].astype(BF16)
            send(sb2.at[k], rb2.at[k], at_x(step), "d", "d")

    steps = {
        "scan1": scan1, "scan2": scan2, "scan3": scan3, "row": row, "col": col, "mix": mix, "mix2": mix2,
        "relay": relay, "send": norm_and_send, "ag": ag, "agend": agend, "g0s": g0s, "g0r": g0r, "g1s": g1s,
        "g1r": g1r, "g2s": g2s, "agp": agp, "ag2": ag2,
    }
    for n in range(2):
        steps["u%d" % n] = functools.partial(gate_up, n, all_rows)
    for n, span in enumerate(((0, 5), (5, 7), (7, 8))):
        steps["e%d" % n] = functools.partial(down_first, *span)
        steps["h%d" % n] = functools.partial(pair_start, n)
    for name, rows in (("p", other_rows), ("o", mine_rows)):
        steps["u2" + name] = functools.partial(gate_up, 2, rows)
        for n in range(3):
            steps["f%d" % n + name] = functools.partial(down_last, n, rows)

    for name, t, q in ORDER:
        if name in steps:
            steps[name]()
        elif name[0] == "S":
            fam = name[1]
            hop1_done(fam, t)
            if t < 4:
                hop1(fam, t + 1)
        else:
            if t > 0:
                hop2_done(name, t, q)
            if t < 4:
                hop2(name, t + 1, q)

    def put(i, lane, value):
        ffn[:, pl.ds(pl.multiple_of(place(i) * 256 + lane, 128), value.shape[-1])] = value

    for u, lo, hi, take_, sbuf, (_, _, fl_, fr_) in ((1, 0, 4, take0, sb0, bufs0), (2, 4, 7, take1, sb1, bufs1)):
        arrived(("f", u), sbuf.at[0:4])
        for half in range(2):
            got = take_(0, half) + fl_[half].astype(F32) + fr_[half].astype(F32)
            for i in range(lo, hi):
                put(i, 128 * half, got[i - lo])
    arrived("d", rb2)
    put(7, 0, parts2[7, 0:BLK, :] + sum(rb2[k].astype(F32) for k in range(3)))
    out[...] = (stream[...] + 0.5 * rms_scale(ffn[...], og[...])).astype(BF16)

    for fam, lanes in (("A", LA), ("B", LB)):
        sent("S" + fam, W.at[0, 0:7, :, lanes])
    for name in LANES:
        sent(name, W.at[0:7, :, :, LANES[name]])
    for u, span in enumerate(SPANS):
        sent(("h", u), psend.at[slice(*span)])
    for out_, ref in (
        ("halo", halo), ("wp", wp.at[1]), ("row", rowbuf), ("col", colbuf), ("mix", mixb), (("sb", 0), sb),
        ("nb", sb), ("nbp", nb.at[0]), (("sb", 1), sb0), (("sb", 2), sb1), ("d", sb2),
    ):
        sent(out_, ref)
    assert len(recv_ids) <= NRECV and len(send_ids) <= NSEND, (len(recv_ids), len(send_ids))


def shards(
    resid, x_branch, gate_branch, conv_w, gate_a_w, gate_x_w, decay_rate, decay_extra, w_proj, mix_gain,
    pre_gain, w_gate, w_up, w_down, out_gain,
):
    vmem = pltpu.VMEM
    return pl.pallas_call(
        kernel,
        out_shape=jax.ShapeDtypeStruct((BLK, D), BF16),
        in_specs=[pl.BlockSpec(memory_space=pl.ANY)] * 15,
        out_specs=pl.BlockSpec(memory_space=pltpu.VMEM),
        scratch_shapes=[
            vmem((NF, NF, 32, WL), BF16),
            vmem((2, CH, D), BF16),
            vmem((ROWS, CH), BF16),
            vmem((ROWS + 16, CH), F32),
            vmem((ROWS, CH), BF16),
            vmem((ROWS, CH), F32),
            vmem((4, CH), F32),
            vmem((4, 64, 64), BF16),
            vmem((4, 64, 64), BF16),
            vmem((1, CH), F32),
            vmem((1, D), F32),
            vmem((1, D), F32),
            vmem((1, D), F32),
            vmem((32, HID), BF16),
            vmem((32, HID), BF16),
            vmem((32, HID), BF16),
            vmem((BLK, D), BF16),
            vmem((16, CH), BF16),
            vmem((CH, 2 * CH), BF16),
            vmem((ROWS, CH), BF16),
            vmem((ROWS, 2 * CH), F32),
            vmem((ROWS, CH), F32),
            vmem((ROWS, CH), F32),
            vmem((ROWS, CH), F32),
            vmem((1, 2 * CH), F32),
            vmem((NF - 1, 1, 2 * CH), F32),
            vmem((1, 2 * CH), F32),
            vmem((NF - 1, 1, 2 * CH), F32),
            vmem((NX * BLK, CH), BF16),
            vmem((NX * BLK, CH), BF16),
            vmem((NX * BLK, CH), BF16),
            vmem((NX * BLK, D), F32),
            vmem((BLK, D), F32),
            vmem((6, BLK, 1024), BF16),
            vmem((BLK, 1024), BF16),
            vmem((BLK, 1024), BF16),
            vmem((2, BLK, 1024), BF16),
            vmem((2, BLK, 1024), BF16),
            vmem((2, 2 * NX, BLK, 1024), BF16),
            vmem((2 * NX * BLK, 768), BF16),
            vmem((NF, 2 * NX * BLK, 256), F32),
            vmem((NF, NX * BLK, 256), BF16),
            vmem((NF, NX * BLK, 256), BF16),
            vmem((6, 4, BLK, 128), BF16),
            vmem((4, BLK, 128), BF16),
            vmem((4, BLK, 128), BF16),
            vmem((2, 4, BLK, 128), BF16),
            vmem((2, 4, BLK, 128), BF16),
            vmem((6, 3, BLK, 128), BF16),
            vmem((3, BLK, 128), BF16),
            vmem((3, BLK, 128), BF16),
            vmem((2, 3, BLK, 128), BF16),
            vmem((2, 3, BLK, 128), BF16),
            vmem((3, BLK, 256), BF16),
            vmem((3, BLK, 256), BF16),
            vmem((BLK, D), F32),
            pltpu.SemaphoreType.DMA((15,)),
            pltpu.SemaphoreType.DMA((NSEND,)),
            pltpu.SemaphoreType.DMA((NRECV,)),
        ],
        compiler_params=pltpu.CompilerParams(
            collective_id=0, has_side_effects=True, vmem_limit_bytes=58 * 1024 * 1024
        ),
        name="layer",
    )(
        resid, x_branch, gate_branch, conv_w, gate_a_w, gate_x_w, decay_rate.reshape(1, CH), decay_extra,
        w_proj, mix_gain.reshape(1, D), pre_gain.reshape(1, D), w_gate, w_up, w_down.T, out_gain.reshape(1, D),
    )


def solution(mesh):
    return jax.shard_map(
        shards,
        mesh=mesh,
        in_specs=(
            P("sp", None),
            P("sp", "tp"),
            P("sp", "tp"),
            P(None, "tp"),
            P("tp", None, None),
            P("tp", None, None),
            P("tp"),
            P("sp", "tp"),
            P("tp", None),
            P(),
            P(),
            P("sp", "tp"),
            P("sp", "tp"),
            P("tp", "sp"),
            P(),
        ),
        out_specs=P(("sp", "tp"), None),
        check_vma=False,
    )
```

```python
import functools

import jax
import jax.numpy as jnp
from jax import lax
from jax.experimental import pallas as pl
from jax.experimental.pallas import tpu as pltpu
from jax.sharding import PartitionSpec as P

LRU_SCALE = 8.0
NORM_EPS = 1e-06
MESH = pl.DeviceIdType.MESH
F32 = jnp.float32
BF16 = jnp.bfloat16

NF = 8
NX = 4
ROWS = 384
CH = 256
D = 2048
BLK = 48
HID = 704
WL = 2176
LANES = {"DA": slice(0, 768), "GA": slice(768, 1152), "GB1": slice(1152, 1664), "GB2": slice(1664, 2176)}
LA, LB = slice(0, 1152), slice(1152, WL)
GROUPS = ((0,), (1, 2), (3, 4), (5, 6), (7,))
NRECV = 111
NSEND = 21

ORDER = (
    ("GB1", 0, 0), ("GA", 0, 0), ("GB2", 0, 0), ("DA", 0, 0), ("scan1", 0, 0), ("SB", 1, 0), ("GB1", 0, 1),
    ("SA", 1, 0), ("scan2", 0, 0), ("GA", 0, 1), ("scan3", 0, 0), ("GB1", 1, 0), ("GA", 1, 0), ("GB2", 0, 1),
    ("DA", 0, 1), ("GB2", 1, 0), ("SB", 2, 0), ("GB1", 0, 2), ("GB1", 1, 1), ("SA", 2, 0), ("GA", 0, 2),
    ("GA", 1, 1), ("GB1", 2, 0), ("GA", 2, 0), ("row", 0, 0), ("DA", 0, 2), ("SB", 3, 0), ("GB1", 0, 3),
    ("GA", 1, 2), ("GB1", 1, 2), ("GA", 2, 1), ("GB1", 2, 1), ("GA", 3, 0), ("DA", 1, 0), ("SA", 3, 0),
    ("GA", 0, 3), ("GB1", 3, 0), ("SB", 4, 0), ("GB1", 0, 4), ("col", 0, 0), ("DA", 0, 3), ("GB1", 1, 3),
    ("mix", 0, 0), ("GB1", 2, 2), ("GA", 2, 2), ("mix2", 0, 0), ("GA", 3, 1), ("GB1", 3, 1), ("DA", 1, 1),
    ("SA", 4, 0), ("GB2", 0, 2), ("GB1", 1, 4), ("GA", 0, 4), ("GA", 1, 3), ("GB2", 0, 3), ("GB1", 2, 3),
    ("DA", 0, 4), ("relay", 0, 0), ("GA", 3, 2), ("DA", 1, 2), ("GB1", 3, 2), ("GB2", 0, 4), ("GB2", 1, 1),
    ("GA", 1, 4), ("GB1", 2, 4), ("DA", 1, 3), ("send", 0, 0), ("GB2", 1, 2), ("GA", 2, 3), ("GB1", 3, 3),
    ("GB2", 1, 3), ("DA", 1, 4), ("DA", 2, 0), ("GB2", 1, 4), ("GA", 2, 4), ("ag", 0, 0), ("GB2", 2, 0),
    ("DA", 2, 1), ("GB1", 3, 4), ("GB2", 2, 1), ("ag2", 0, 0), ("GB2", 2, 2), ("GA", 3, 3), ("DA", 2, 2),
    ("GB2", 2, 3), ("agend", 0, 0), ("GB2", 2, 4), ("GA", 3, 4), ("DA", 2, 3), ("GB2", 3, 0), ("agp", 0, 0),
    ("GB1", 4, 0), ("GB1", 4, 1), ("GB1", 4, 2), ("GB1", 4, 3), ("GB1", 4, 4), ("u1", 0, 0), ("GB2", 3, 1),
    ("DA", 2, 4), ("GB2", 3, 2), ("DA", 3, 0), ("DA", 3, 1), ("GB2", 3, 3), ("GA", 4, 0), ("GA", 4, 1),
    ("GA", 4, 2), ("GA", 4, 3), ("GA", 4, 4), ("u0", 0, 0), ("DA", 3, 2), ("GB2", 3, 4), ("e0", 0, 0),
    ("DA", 3, 3), ("DA", 3, 4), ("GB2", 4, 0), ("GB2", 4, 1), ("GB2", 4, 2), ("GB2", 4, 3), ("GB2", 4, 4),
    ("u2p", 0, 0), ("f0p", 0, 0), ("h0", 0, 0), ("e1", 0, 0), ("f1p", 0, 0), ("h1", 0, 0), ("u2o", 0, 0),
    ("f0o", 0, 0), ("f1o", 0, 0), ("g0s", 0, 0), ("DA", 4, 0), ("DA", 4, 1), ("DA", 4, 2), ("DA", 4, 3),
    ("DA", 4, 4), ("e2", 0, 0), ("f2p", 0, 0), ("h2", 0, 0), ("g1s", 0, 0), ("f2o", 0, 0), ("g0r", 0, 0),
    ("g2s", 0, 0), ("g1r", 0, 0),
)


def dot(a, b):
    return jnp.dot(a, b, preferred_element_type=F32)


def dot_nt(a, b):
    return lax.dot_general(a, b, (((1,), (1,)), ((), ())), preferred_element_type=F32)


def sigmoid(v):
    return 1.0 / (1.0 + jnp.exp(-v))


def gelu(v):
    inner = 0.7978845608028654 * (v + 0.044715 * (v * v * v))
    return 0.5 * v * (1.0 + jnp.tanh(inner))


def one_minus_exp(w):
    series = 1.0 + w * (1.0 / 6.0)
    for n in (5.0, 4.0, 3.0, 2.0):
        series = 1.0 + w * (1.0 / n) * series
    return jnp.where(w > -0.25, -w * series, 1.0 - jnp.exp(w))


def rms_scale(values, gains):
    mean = jnp.sum(values * values, axis=-1, keepdims=True) * (1.0 / D)
    return values * lax.rsqrt(mean + NORM_EPS) * gains


def kernel(
    resid, x_in, g_in, conv_w, ga_in, gx_in, rate, extra, wp_in, mixg, preg, wg_in, wu_in, wd_in, outg,
    out,
    W, wp, xb, xp, gb, eb, cw, ga, gx, rt, mg, pg, og, wg, wu, wd, rs_b,
    halo, bd, cout, gates, acum, bcum, geb, tot, rowbuf, rtot, colbuf,
    mixa, mixs, mixb, parts, stream, sb, rl, rr, fl, fr, nb, hid,
    parts2, psend, pbuf, sb0, rl0, rr0, fl0, fr0, sb1, rl1, rr1, fl1, fr1, sb2, rb2, ffn,
    local_sem, send_sem, recv_sem,
):
    sp = lax.axis_index("sp")
    tp = lax.axis_index("tp")
    z, y = sp // NF, sp % NF
    x, c = tp // 2, tp % 2

    def at_zy(zz, yy):
        return {"sp": zz * NF + yy, "tp": tp}

    def at_x(step):
        return {"sp": sp, "tp": ((x + step) % NX) * 2 + c}

    partner = {"sp": sp, "tp": x * 2 + (1 - c)}
    behind = {"sp": (sp + NF * NF - 1) % (NF * NF), "tp": tp}
    ahead = {"sp": (sp + 1) % (NF * NF), "tp": tp}

    barrier = pltpu.get_barrier_semaphore()
    peers = [at_zy(z, (y + k) % NF) for k in range(1, NF)]
    peers += [at_zy((z + k) % NF, y) for k in range(1, NF)]
    peers += [at_x(1), at_x(2), at_x(NX - 1), partner, behind, ahead]
    for peer in peers:
        pl.semaphore_signal(barrier, inc=1, device_id=peer, device_id_type=MESH)

    loads = {}

    def load(name, src, dst):
        copy = pltpu.make_async_copy(src, dst, local_sem.at[len(loads)])
        copy.start()
        loads[name] = copy

    load("wg", wg_in, wg)
    load("wu", wu_in, wu)
    load("wd", wd_in, wd)
    load("x", x_in, xb)
    load("ga", ga_in, ga)
    load("gx", gx_in, gx)
    load("g", g_in, gb)
    load("cw", conv_w, cw)
    load("rt", rate, rt)
    load("e", extra, eb)
    load("wp", wp_in, wp.at[0])
    load("rs", resid.at[pl.ds(pl.multiple_of(tp * BLK, 16), BLK), :], rs_b)
    load("mg", mixg, mg)
    load("pg", preg, pg)
    load("og", outg, og)

    for name in ("wg", "wu", "wd"):
        loads[name].wait()
    mine = W.at[z, y]
    mine[:, 0:640] = wd[:, 0:640]
    mine[:, 640:768] = jnp.concatenate([wd[:, 640:704], jnp.zeros((32, 64), BF16)], axis=1)
    mine[:, 768:896] = wg[:, 512:640]
    mine[:, 896:1024] = wu[:, 512:640]
    mine[:, 1024:1152] = jnp.concatenate([wg[:, 640:704], wu[:, 640:704]], axis=1)
    for n in range(2):
        mine[:, 512 * n + 1152 : 512 * n + 1408] = wg[:, 256 * n : 256 * n + 256]
        mine[:, 512 * n + 1408 : 512 * n + 1664] = wu[:, 256 * n : 256 * n + 256]

    send_ids, recv_ids = {}, {}

    def send(src, dst, device, to, out):
        copy = pltpu.make_async_remote_copy(
            src_ref=src,
            dst_ref=dst,
            send_sem=send_sem.at[send_ids.setdefault(out, len(send_ids))],
            recv_sem=recv_sem.at[recv_ids.setdefault(to, len(recv_ids))],
            device_id=device,
            device_id_type=MESH,
        )
        copy.start()

    def arrived(to, like):
        pltpu.make_async_copy(like, like, recv_sem.at[recv_ids[to]]).wait()

    def sent(out, like):
        pltpu.make_async_copy(like, like, send_sem.at[send_ids[out]]).wait()

    def mod(v):
        return (v + NF) % NF

    def piece(fam, first, second, lanes):
        return W.at[second, first, :, lanes] if fam == "A" else W.at[first, second, :, lanes]

    def some(n, lanes):
        return W.at[0, 0:n, :, lanes]

    first = {"A": y, "B": z}
    second = {"A": z, "B": y}

    def along_y(step):
        return at_zy(z, (y + step) % NF)

    def along_z(step):
        return at_zy((z + step) % NF, y)

    along_first = {"A": along_y, "B": along_z}
    along_second = {"A": along_z, "B": along_y}
    WAYS = ((1, -1), (NF - 1, 1))

    def hop1(fam, k):
        whole = LA if fam == "A" else LB
        cut = whole.start + (640 if fam == "A" else 512)
        for d, (step, sign) in enumerate(WAYS):
            lanes = whole if k < 4 else (slice(whole.start, cut) if d == 0 else slice(cut, whole.stop))
            ref = piece(fam, mod(first[fam] + sign * (k - 1)), second[fam], lanes)
            send(ref, ref, along_first[fam](step), ("S" + fam, k), "S" + fam)

    def hop1_done(fam, k):
        whole = LA if fam == "A" else LB
        arrived(("S" + fam, k), some(2 if k < 4 else 1, whole))

    def offset(j):
        return (j + 1) // 2 * (-1 if j % 2 == 1 else 1)

    def hop2(name, t, q):
        fam, lanes = name[1], LANES[name]
        for d, (step, sign) in enumerate(WAYS):
            for j in GROUPS[q]:
                if t == 4 and (j < 4) != (d == 0):
                    continue
                ref = piece(fam, mod(first[fam] + offset(j)), mod(second[fam] + sign * (t - 1)), lanes)
                send(ref, ref, along_second[fam](step), (name, t, q), name)

    def hop2_done(name, t, q):
        n = len(GROUPS[q])
        arrived((name, t, q), some(2 * n if t < 4 else n, LANES[name]))

    loads["x"].wait()
    pl.semaphore_wait(barrier, len(peers))
    send(xb.at[pl.ds(ROWS - 16, 16), :], halo, ahead, "halo", "halo")
    hop1("A", 1)
    hop1("B", 1)
    loads["wp"].wait()
    send(wp.at[0], wp.at[1], partner, "wp", "wp")
    for name in ("ga", "gx", "g", "cw", "rt", "e"):
        loads[name].wait()
    bd[...] = jnp.zeros_like(bd)
    for n in range(4):
        s = slice(64 * n, 64 * n + 64)
        bd[s, 64 * n : 64 * n + 64] = ga[n]
        bd[s, CH + 64 * n : CH + 64 * n + 64] = gx[n]
    xp[16:, :] = xb[...].astype(F32)
    geb[...] = gelu(gb[...].astype(F32))

    def scan1():
        arrived("halo", halo)
        xp[0:16, :] = jnp.where(sp > 0, halo[...].astype(F32), 0.0)
        conv = xp[13 : 13 + ROWS, :] * cw[0:1, :]
        for tap in range(1, 4):
            conv = conv + xp[13 + tap : 13 + tap + ROWS, :] * cw[tap : tap + 1, :]
        cout[...] = conv.astype(BF16)
        gates[...] = dot(cout[...], bd[...])

    held = {}

    def scan_rows(lo, hi, start):
        in_group = lax.broadcasted_iota(jnp.int32, (4, 8, CH), 1)

        def chunk(i, carry):
            rows = pl.ds(pl.multiple_of(i * 32, 32), 32)
            recur = sigmoid(gates[rows, 0:CH])
            inject = sigmoid(gates[rows, CH:])
            log_decay = (-LRU_SCALE * recur) * rt[...] + eb[rows, :]
            decay = jnp.exp(log_decay)
            grown = one_minus_exp(2.0 * log_decay)
            root = jnp.where(grown > 0.0, grown * lax.rsqrt(jnp.maximum(grown, 1e-37)), 0.0)
            drive = root * inject * cout[rows, :].astype(F32)
            a = decay.reshape(4, 8, CH)
            b = drive.reshape(4, 8, CH)
            for step in (1, 2, 4):
                keep = in_group >= step
                a_prev = jnp.where(keep, pltpu.roll(a, step, 1), 1.0)
                b_prev = jnp.where(keep, pltpu.roll(b, step, 1), 0.0)
                b = a * b_prev + b
                a = a * a_prev
            a_in, b_in = carry
            a_all, b_all = [], []
            for n in range(4):
                a_n = a[n] * a_in
                b_n = a[n] * b_in + b[n]
                a_in, b_in = a_n[7:8, :], b_n[7:8, :]
                a_all.append(a_n)
                b_all.append(b_n)
            acum[rows, :] = jnp.concatenate(a_all, axis=0)
            bcum[rows, :] = jnp.concatenate(b_all, axis=0)
            return a_in, b_in

        return lax.fori_loop(lo, hi, chunk, start)

    def scan2():
        held["half"] = scan_rows(0, 6, (jnp.ones((1, CH), F32), jnp.zeros((1, CH), F32)))

    def scan3():
        a_end, b_end = scan_rows(6, ROWS // 32, held["half"])
        tot[:, 0:CH] = a_end
        tot[:, CH:] = b_end
        for k in range(1, NF):
            send(tot, rowbuf.at[k - 1], along_y(k), "row", "row")

    def composed(own, buf, me):
        pa, pb = jnp.ones((1, CH), F32), jnp.zeros((1, CH), F32)
        ea, eb_ = pa, pb
        for place in range(NF):
            slot = (me - place + NF) % NF
            got = buf[jnp.maximum(slot - 1, 0)]
            is_me = slot == 0
            va = jnp.where(is_me, own[:, 0:CH], got[:, 0:CH])
            vb = jnp.where(is_me, own[:, CH:], got[:, CH:])
            ea = jnp.where(is_me, pa, ea)
            eb_ = jnp.where(is_me, pb, eb_)
            pa, pb = pa * va, va * pb + vb
        return (pa, pb), (ea, eb_)

    def row():
        arrived("row", rowbuf)
        (ra, rb_), held["in"] = composed(tot[...], rowbuf, y)
        rtot[:, 0:CH] = ra
        rtot[:, CH:] = rb_
        for k in range(1, NF):
            send(rtot, colbuf.at[k - 1], along_z(k), "col", "col")

    def col():
        arrived("col", colbuf)
        _, (col_a, col_b) = composed(rtot[...], colbuf, z)
        in_a, in_b = held["in"]
        held["carried"] = in_a * col_b + in_b

    def mixer_block(core, rel):
        block = ((x + rel) % NX) * 2 + core
        rows = pl.ds(pl.multiple_of(block * BLK, 16), BLK)
        return ((bcum[rows, :] + acum[rows, :] * held["carried"]) * geb[rows, :]).astype(BF16)

    def mix():
        for rel in range(NX):
            mixs[BLK * rel : BLK * rel + BLK, :] = mixer_block(1 - c, rel)
        send(mixs, mixb, partner, "mix", "mix")
        for rel in range(NX):
            mixa[BLK * rel : BLK * rel + BLK, :] = mixer_block(c, rel)
        arrived("wp", wp.at[1])
        parts[...] = dot(mixa[...], wp[0])

    def scatter_start(u, take, sbuf, bufs):
        rl_, rr_, fl_, fr_ = bufs
        for half in range(2):
            sbuf[half] = take(2, half).astype(BF16)
        send(sbuf.at[0], rl_, at_x(1), ("rl", u), ("sb", u))
        send(sbuf.at[1], rr_, at_x(NX - 1), ("rr", u), ("sb", u))
        sbuf[2] = take(1, 1).astype(BF16)
        send(sbuf.at[2], fl_.at[1], at_x(1), ("f", u), ("sb", u))
        sbuf[3] = take(3, 0).astype(BF16)
        send(sbuf.at[3], fr_.at[0], at_x(NX - 1), ("f", u), ("sb", u))

    def scatter_relay(u, take, sbuf, bufs):
        rl_, rr_, fl_, fr_ = bufs
        arrived(("rl", u), rl_)
        sbuf[4] = (take(1, 0) + rl_[...].astype(F32)).astype(BF16)
        send(sbuf.at[4], fl_.at[0], at_x(1), ("f", u), ("sb", u))
        arrived(("rr", u), rr_)
        sbuf[5] = (take(3, 1) + rr_[...].astype(F32)).astype(BF16)
        send(sbuf.at[5], fr_.at[1], at_x(NX - 1), ("f", u), ("sb", u))

    bufs = (rl, rr, fl, fr)

    def take(rel, half):
        return parts[BLK * rel : BLK * rel + BLK, 1024 * half : 1024 * half + 1024]

    def mix2():
        arrived("mix", mixb)
        parts[...] += dot(mixb[...], wp[1])
        scatter_start(0, take, sb, bufs)

    def relay():
        scatter_relay(0, take, sb, bufs)

    def norm_and_send():
        arrived(("f", 0), sb.at[0:4])
        for name in ("rs", "mg", "pg", "og"):
            loads[name].wait()
        halves = [take(0, half) + fl[half].astype(F32) + fr[half].astype(F32) for half in range(2)]
        mixed = jnp.concatenate(halves, axis=1)
        after_mix = rs_b[...].astype(F32) + rms_scale(mixed, mg[...])
        stream[...] = after_mix
        normed = rms_scale(after_mix, pg[...]).astype(BF16)
        nb[0, 0] = normed[:, 0:1024]
        nb[1, 0] = normed[:, 1024:]
        send(nb.at[0, 0], nb.at[0, 3], at_x(1), "al", "nb")
        send(nb.at[1, 0], nb.at[1, 1], at_x(NX - 1), "ar", "nb")
        send(nb.at[1, 0], nb.at[1, 3], at_x(1), "an", "nb")
        send(nb.at[0, 0], nb.at[0, 1], at_x(NX - 1), "an", "nb")
        for half in range(2):
            to_partner(half, 0)

    def to_partner(half, rel):
        send(nb.at[half, rel], nb.at[half, NX + rel], partner, "nbp", "nbp")

    def ag():
        arrived("al", nb.at[0, 3])
        send(nb.at[0, 3], nb.at[0, 2], at_x(1), "ab", "nb")
        to_partner(0, 3)
        arrived("ar", nb.at[1, 1])
        send(nb.at[1, 1], nb.at[1, 2], at_x(NX - 1), "ab", "nb")
        to_partner(1, 1)

    def ag2():
        arrived("an", nb.at[0, 0:2])
        to_partner(1, 3)
        to_partner(0, 1)

    def agend():
        arrived("ab", nb.at[0, 0:2])
        to_partner(0, 2)
        to_partner(1, 2)

    def agp():
        arrived("nbp", nb.at[0])

    HALF = NX * BLK
    mine_rows, other_rows, all_rows = slice(0, HALF), slice(HALF, 2 * HALF), slice(0, 2 * HALF)

    def gate_up(n, span):
        w = W[:, :, :, LANES[("GA", "GB1", "GB2")[n]]]
        w = w.reshape(D, w.shape[-1])
        rows = span.stop - span.start
        at = slice(span.start // BLK, span.stop // BLK)
        both = dot(nb[0, at].reshape(rows, 1024), w[0:1024]) + dot(nb[1, at].reshape(rows, 1024), w[1024:])
        if n > 0:
            g, u = both[:, 0:256], both[:, 256:512]
            hid[span, 256 * n - 256 : 256 * n] = (g * sigmoid(g) * u).astype(BF16)
        else:
            g, u = both[:, 0:128], both[:, 128:256]
            hid[span, 512:640] = (g * sigmoid(g) * u).astype(BF16)
            g = both[:, 256:384]
            u = pltpu.roll(g, 64, 1)
            lane = lax.broadcasted_iota(jnp.int32, g.shape, 1)
            hid[span, 640:768] = jnp.where(lane < 64, g * sigmoid(g) * u, 0.0).astype(BF16)

    def place(i):
        return (z + NF + (i + 1) // 2 * (1 - 2 * (i % 2))) % NF

    def down(i, rows, lanes):
        w = W[place(i), :, :, lanes]
        return dot_nt(hid[rows, lanes], w.reshape(256, lanes.stop - lanes.start))

    def down_first(lo, hi):
        for i in range(lo, hi):
            parts2[i] = down(i, all_rows, slice(0, 256)) + down(i, all_rows, slice(512, 768))

    def down_last(u, rows):
        for i in range(*SPANS[u]):
            parts2[i, rows] += down(i, rows, slice(256, 512))

    SPANS = ((0, 4), (4, 7), (7, 8))

    def pair_start(u):
        span = slice(*SPANS[u])
        psend[span] = parts2[span, other_rows, :].astype(BF16)
        send(psend.at[span], pbuf.at[span], partner, ("h", u), ("h", u))

    def pair_end(u):
        span = slice(*SPANS[u])
        arrived(("h", u), pbuf.at[span])
        parts2[span, mine_rows, :] += pbuf[span].astype(F32)

    bufs0 = (rl0, rr0, fl0, fr0)
    bufs1 = (rl1, rr1, fl1, fr1)

    def take0(rel, half):
        return parts2[0:4, BLK * rel : BLK * rel + BLK, 128 * half : 128 * half + 128]

    def take1(rel, half):
        return parts2[4:7, BLK * rel : BLK * rel + BLK, 128 * half : 128 * half + 128]

    def g0s():
        pair_end(0)
        scatter_start(1, take0, sb0, bufs0)

    def g0r():
        scatter_relay(1, take0, sb0, bufs0)

    def g1s():
        pair_end(1)
        scatter_start(2, take1, sb1, bufs1)

    def g1r():
        scatter_relay(2, take1, sb1, bufs1)

    def g2s():
        pair_end(2)
        for k, (rel, step) in enumerate(((2, 2), (1, 1), (3, NX - 1))):
            sb2[k] = parts2[7, BLK * rel : BLK * rel + BLK, :].astype(BF16)
            send(sb2.at[k], rb2.at[k], at_x(step), "d", "d")

    steps = {
        "scan1": scan1, "scan2": scan2, "scan3": scan3, "row": row, "col": col, "mix": mix, "mix2": mix2,
        "relay": relay, "send": norm_and_send, "ag": ag, "agend": agend, "g0s": g0s, "g0r": g0r, "g1s": g1s,
        "g1r": g1r, "g2s": g2s, "agp": agp, "ag2": ag2,
    }
    for n in range(2):
        steps["u%d" % n] = functools.partial(gate_up, n, all_rows)
    for n, span in enumerate(((0, 5), (5, 7), (7, 8))):
        steps["e%d" % n] = functools.partial(down_first, *span)
        steps["h%d" % n] = functools.partial(pair_start, n)
    for name, rows in (("p", other_rows), ("o", mine_rows)):
        steps["u2" + name] = functools.partial(gate_up, 2, rows)
        for n in range(3):
            steps["f%d" % n + name] = functools.partial(down_last, n, rows)

    for name, t, q in ORDER:
        if name in steps:
            steps[name]()
        elif name[0] == "S":
            fam = name[1]
            hop1_done(fam, t)
            if t < 4:
                hop1(fam, t + 1)
        else:
            if t > 0:
                hop2_done(name, t, q)
            if t < 4:
                hop2(name, t + 1, q)

    def put(i, lane, value):
        ffn[:, pl.ds(pl.multiple_of(place(i) * 256 + lane, 128), value.shape[-1])] = value

    for u, lo, hi, take_, sbuf, (_, _, fl_, fr_) in ((1, 0, 4, take0, sb0, bufs0), (2, 4, 7, take1, sb1, bufs1)):
        arrived(("f", u), sbuf.at[0:4])
        for half in range(2):
            got = take_(0, half) + fl_[half].astype(F32) + fr_[half].astype(F32)
            for i in range(lo, hi):
                put(i, 128 * half, got[i - lo])
    arrived("d", rb2)
    put(7, 0, parts2[7, 0:BLK, :] + sum(rb2[k].astype(F32) for k in range(3)))
    out[...] = (stream[...] + 0.5 * rms_scale(ffn[...], og[...])).astype(BF16)

    for fam, lanes in (("A", LA), ("B", LB)):
        sent("S" + fam, W.at[0, 0:7, :, lanes])
    for name in LANES:
        sent(name, W.at[0:7, :, :, LANES[name]])
    for u, span in enumerate(SPANS):
        sent(("h", u), psend.at[slice(*span)])
    for out_, ref in (
        ("halo", halo), ("wp", wp.at[1]), ("row", rowbuf), ("col", colbuf), ("mix", mixb), (("sb", 0), sb),
        ("nb", sb), ("nbp", nb.at[0]), (("sb", 1), sb0), (("sb", 2), sb1), ("d", sb2),
    ):
        sent(out_, ref)
    assert len(recv_ids) <= NRECV and len(send_ids) <= NSEND, (len(recv_ids), len(send_ids))


def shards(
    resid, x_branch, gate_branch, conv_w, gate_a_w, gate_x_w, decay_rate, decay_extra, w_proj, mix_gain,
    pre_gain, w_gate, w_up, w_down, out_gain,
):
    vmem = pltpu.VMEM
    return pl.pallas_call(
        kernel,
        out_shape=jax.ShapeDtypeStruct((BLK, D), BF16),
        in_specs=[pl.BlockSpec(memory_space=pl.ANY)] * 15,
        out_specs=pl.BlockSpec(memory_space=pltpu.VMEM),
        scratch_shapes=[
            vmem((NF, NF, 32, WL), BF16),
            vmem((2, CH, D), BF16),
            vmem((ROWS, CH), BF16),
            vmem((ROWS + 16, CH), F32),
            vmem((ROWS, CH), BF16),
            vmem((ROWS, CH), F32),
            vmem((4, CH), F32),
            vmem((4, 64, 64), BF16),
            vmem((4, 64, 64), BF16),
            vmem((1, CH), F32),
            vmem((1, D), F32),
            vmem((1, D), F32),
            vmem((1, D), F32),
            vmem((32, HID), BF16),
            vmem((32, HID), BF16),
            vmem((32, HID), BF16),
            vmem((BLK, D), BF16),
            vmem((16, CH), BF16),
            vmem((CH, 2 * CH), BF16),
            vmem((ROWS, CH), BF16),
            vmem((ROWS, 2 * CH), F32),
            vmem((ROWS, CH), F32),
            vmem((ROWS, CH), F32),
            vmem((ROWS, CH), F32),
            vmem((1, 2 * CH), F32),
            vmem((NF - 1, 1, 2 * CH), F32),
            vmem((1, 2 * CH), F32),
            vmem((NF - 1, 1, 2 * CH), F32),
            vmem((NX * BLK, CH), BF16),
            vmem((NX * BLK, CH), BF16),
            vmem((NX * BLK, CH), BF16),
            vmem((NX * BLK, D), F32),
            vmem((BLK, D), F32),
            vmem((6, BLK, 1024), BF16),
            vmem((BLK, 1024), BF16),
            vmem((BLK, 1024), BF16),
            vmem((2, BLK, 1024), BF16),
            vmem((2, BLK, 1024), BF16),
            vmem((2, 2 * NX, BLK, 1024), BF16),
            vmem((2 * NX * BLK, 768), BF16),
            vmem((NF, 2 * NX * BLK, 256), F32),
            vmem((NF, NX * BLK, 256), BF16),
            vmem((NF, NX * BLK, 256), BF16),
            vmem((6, 4, BLK, 128), BF16),
            vmem((4, BLK, 128), BF16),
            vmem((4, BLK, 128), BF16),
            vmem((2, 4, BLK, 128), BF16),
            vmem((2, 4, BLK, 128), BF16),
            vmem((6, 3, BLK, 128), BF16),
            vmem((3, BLK, 128), BF16),
            vmem((3, BLK, 128), BF16),
            vmem((2, 3, BLK, 128), BF16),
            vmem((2, 3, BLK, 128), BF16),
            vmem((3, BLK, 256), BF16),
            vmem((3, BLK, 256), BF16),
            vmem((BLK, D), F32),
            pltpu.SemaphoreType.DMA((15,)),
            pltpu.SemaphoreType.DMA((NSEND,)),
            pltpu.SemaphoreType.DMA((NRECV,)),
        ],
        compiler_params=pltpu.CompilerParams(
            collective_id=0, has_side_effects=True, vmem_limit_bytes=58 * 1024 * 1024
        ),
        name="layer",
    )(
        resid, x_branch, gate_branch, conv_w, gate_a_w, gate_x_w, decay_rate.reshape(1, CH), decay_extra,
        w_proj, mix_gain.reshape(1, D), pre_gain.reshape(1, D), w_gate, w_up, w_down.T, out_gain.reshape(1, D),
    )


def solution(mesh):
    return jax.shard_map(
        shards,
        mesh=mesh,
        in_specs=(
            P("sp", None),
            P("sp", "tp"),
            P("sp", "tp"),
            P(None, "tp"),
            P("tp", None, None),
            P("tp", None, None),
            P("tp"),
            P("sp", "tp"),
            P("tp", None),
            P(),
            P(),
            P("sp", "tp"),
            P("sp", "tp"),
            P("tp", "sp"),
            P(),
        ),
        out_specs=P(("sp", "tp"), None),
        check_vma=False,
    )
```
